256 devices in a mesh: sp: 64 (over z, x, core), tp: 4 (over y).
Axes of the slice: x: 4, y: 4, z: 8, core: 2. Of those that a mesh axis runs over, the one named last changes fastest.
Arguments:
- queries: bfloat16 [8192, 2048], P('sp', 'tp'), may hold values from -6 to 6
- keys: bfloat16 [8192, 512], P('sp', 'tp'), may hold values from -6 to 6
- values: bfloat16 [8192, 512], P('sp', 'tp'), may hold values from -6 to 6
- break_bias: float32 [16], P('tp'), as said below
- residual: bfloat16 [8192, 4096], P(('sp', 'tp')), may hold values from -6 to 6
- w_out: bfloat16 [2048, 4096], P('tp'), may hold values from -0.125 to 0.125
- ffn_gain: float32 [4096], replicated, may hold values from 0.1 to 1.9
- pick_ids: int32 [8192, 2], P('sp'), may hold values from 0 to 63, as said below
- pair_logit: float32 [8192], P('sp'), may hold values from -8 to 8
- w_gate: bfloat16 [64, 4096, 1024], P('sp', None, 'tp'), may hold values from -0.09375 to 0.09375
- w_up: bfloat16 [64, 4096, 1024], P('sp', None, 'tp'), may hold values from -0.09375 to 0.09375
- w_down: bfloat16 [64, 1024, 4096], P('sp', 'tp'), may hold values from -0.1875 to 0.1875
- out_gain: float32 [4096], replicated, may hold values from 0.1 to 1.9
Outputs:
- new_stream: bfloat16 [8192, 4096], P(('sp', 'tp'))
The draws below stay inside these ranges and needn't reach their ends.
Inputs may be any that keep to these rules, and one draw needn't show every extreme that they name: `break_bias`: the logarithm of a break rate per position: between ln(0.02 / 8192) and ln(8 / 128). `pick_ids`: A row's 2 experts differ and lie in one group of 16 consecutive experts. In each aligned block of 32 rows no expert is named more than 2 times, and some expert exactly 2 times.
All inputs are finite; a program needn't handle non-finite values.
Results may differ from the reference program's by a relative error of at most 0.017.
Values may be sent and summed in bfloat16 or wider, within the bound.
No kernel may reach another device: no remote copies, remote signals or barrier semaphores. Data moves between devices by JAX's collectives and lax.ppermute only.
A program may use at most 64 MiB of HBM per device.

```python
import jax
import jax.numpy as jnp
from jax import lax

D = 4096
HEAD = 128
HEADS = 16
KV_HEADS = 4
FF = 1024
GROUPS = 4
TOP = 2
TOK_DEV = 128
TOKENS = 8192
EXPERTS = 64
PER = 16
ROWS_DEV = 32
CAP = 2
N_SP = 64
N_TP = 4


def draw_break_bias(key, part):
    key_kind, key_fast, key_slow = jax.random.split(key, 3)
    fast_share = 0.5
    fast = jax.random.uniform(key_kind, (HEADS,), jnp.float32) < fast_share
    fast_rate = jax.random.uniform(key_fast, (HEADS,), jnp.float32, 3.0, 8.0) / TOK_DEV
    slow_rate = jax.random.uniform(key_slow, (HEADS,), jnp.float32, 0.02, 0.2) / TOKENS
    return jnp.log(jnp.where(fast, fast_rate, slow_rate)).astype(jnp.float32)


def pick_block(key):
    pairs = EXPERTS * CAP // 2
    half_group = PER // 2
    key_label, key_force, key_rank, key_rows = jax.random.split(key, 4)
    rounds = GROUPS * CAP
    labels = jax.vmap(lambda sub_key: jax.random.permutation(sub_key, PER))(jax.random.split(key_label, rounds))
    index = jnp.arange(pairs, dtype=jnp.int32)
    round_id = index // half_group
    inside = index % half_group
    group_id = round_id // CAP
    leading = group_id * PER + labels[round_id, 2 * inside]
    trailing = group_id * PER + labels[round_id, 2 * inside + 1]
    forced = jax.random.randint(key_force, (), 0, EXPERTS)
    hit = ((leading == forced) | (trailing == forced)).astype(jnp.int32)
    ranks = jax.random.permutation(key_rank, pairs).astype(jnp.int32)
    chosen = jnp.argsort(ranks - pairs * hit, stable=True)[:ROWS_DEV]
    chosen = chosen[jax.random.permutation(key_rows, ROWS_DEV)]
    return jnp.stack([leading[chosen], trailing[chosen]], axis=1).astype(jnp.int32)


def draw_pick_ids(key, part):
    blocks = TOKENS // ROWS_DEV
    return jax.vmap(pick_block)(jax.random.split(key, blocks)).reshape(TOKENS, TOP).astype(jnp.int32)


def block_levels(key, shape, cuts, least, largest):
    loudness, own = 1.0, jax.random.fold_in(key, 6)
    for axis_at, blocks in cuts:
        heights = jnp.exp(jax.random.uniform(jax.random.fold_in(own, axis_at), (blocks,), jnp.float32, least / len(cuts), largest / len(cuts)))
        loudness = loudness * jnp.repeat(heights, shape[axis_at] // blocks).reshape([-1 if axis == axis_at else 1 for axis in range(len(shape))])
    return loudness


def centred(rng, dims, scale, most, cuts=(), kind=jnp.bfloat16):
    factor_of = block_levels(rng, dims, cuts, -0.22, 0.18) if cuts else 1.0
    drawn = jax.random.normal(rng, dims, jnp.float32) * scale * factor_of
    return jnp.minimum(jnp.maximum(drawn, -most), most).astype(kind)


def setup_inputs(seed: int = 0) -> dict:
    key_list = jax.random.split(jax.random.key(seed), 14)
    queries = centred(key_list[0], (TOKENS, HEADS * HEAD), 1.0, 6.0, ((0, 64), (1, 4)))
    keys = centred(key_list[1], (TOKENS, KV_HEADS * HEAD), 1.0, 6.0, ((0, 64), (1, 4)))
    values = centred(key_list[2], (TOKENS, KV_HEADS * HEAD), 1.0, 6.0, ((0, 64), (1, 4)))
    break_bias = draw_break_bias(jax.random.fold_in(key_list[13], 71), 0)
    residual = centred(key_list[4], (TOKENS, D), 1.0, 6.0, ((0, 256),))
    w_out = centred(key_list[5], (HEADS * HEAD, D), (HEADS * HEAD) ** -0.5, 0.125, ((0, 4),))
    ffn_gain = jnp.clip(1.0 + 0.18 * jax.random.normal(key_list[6], (D,), jnp.float32), 0.1, 1.9)
    pick_ids = draw_pick_ids(jax.random.fold_in(key_list[13], 71), 0)
    pair_logit = centred(key_list[8], (TOKENS,), 1.5, 8.0, ((0, 64),), jnp.float32)
    w_gate = centred(key_list[9], (EXPERTS, D, FF), D ** -0.5, 0.09375, ((0, 64), (2, 4)))
    w_up = centred(key_list[10], (EXPERTS, D, FF), D ** -0.5, 0.09375, ((0, 64), (2, 4)))
    w_down = centred(key_list[11], (EXPERTS, FF, D), FF ** -0.5, 0.1875, ((0, 64), (1, 4)))
    out_gain = jnp.clip(1.0 + 0.18 * jax.random.normal(key_list[12], (D,), jnp.float32), 0.1, 1.9)
    return {"queries": queries, "keys": keys, "values": values, "break_bias": break_bias, "residual": residual, "w_out": w_out, "ffn_gain": ffn_gain, "pick_ids": pick_ids, "pair_logit": pair_logit, "w_gate": w_gate, "w_up": w_up, "w_down": w_down, "out_gain": out_gain}


epsilon = 1e-06

def rounded(values_in):
    return lax.optimization_barrier(values_in.astype(jnp.bfloat16)).astype(jnp.float32)

def stick_block(carried, query_rows, key_block, value_block, head_bias, query_pos, key_pos):
    output, used_up = carried
    scores = jnp.einsum('qcgd,scd->qcgs', query_rows.astype(jnp.float32), key_block.astype(jnp.float32))
    scores = scores * query_rows.shape[-1] ** (-0.5) + head_bias[None, :, :, None]
    before = (key_pos[None, :] < query_pos[:, None])[:, None, None, :]
    breaks = jnp.where(before, jax.nn.softplus(scores), 0.0)
    behind = lax.cumsum(breaks, axis=3, reverse=True) - breaks
    weights = jnp.where(before, jnp.exp(jax.nn.log_sigmoid(scores) - behind - used_up[..., None]), 0.0)
    output = output + jnp.einsum('qcgs,scd->qcgd', rounded(weights), value_block.astype(jnp.float32))
    return (output, used_up + lax.optimization_barrier(jnp.sum(breaks, axis=3)))

def reference(queries, keys, values, break_bias, residual, w_out, ffn_gain, pick_ids, pair_logit, w_gate, w_up, w_down, out_gain):
    extent = queries.shape[0]
    per_key = HEADS // KV_HEADS
    window = min(512, extent)
    blocks = extent // window
    query_all = queries.reshape(blocks, window, KV_HEADS, per_key, HEAD)
    key_all = keys.reshape(extent, KV_HEADS, HEAD)
    value_all = values.reshape(extent, KV_HEADS, HEAD)
    head_bias = break_bias.reshape(KV_HEADS, per_key)

    def one_block(block_index):
        query_rows = lax.dynamic_index_in_dim(query_all, block_index, 0, keepdims=False)
        query_pos = block_index * window + jnp.arange(window, dtype=jnp.int32)
        initial = (jnp.zeros((window, KV_HEADS, per_key, HEAD), jnp.float32), jnp.zeros((window, KV_HEADS, per_key), jnp.float32))

        def visit(step_index, carried):
            first_key = ((block_index - step_index) * window).astype(jnp.int32)
            key_block = lax.dynamic_slice_in_dim(key_all, first_key, window, 0)
            value_block = lax.dynamic_slice_in_dim(value_all, first_key, window, 0)
            key_pos = first_key + jnp.arange(window, dtype=jnp.int32)
            return stick_block(carried, query_rows, key_block, value_block, head_bias, query_pos, key_pos)
        return lax.fori_loop(jnp.int32(0), block_index + 1, visit, initial)[0]
    attended = lax.map(one_block, jnp.arange(blocks, dtype=jnp.int32)).reshape(extent, HEADS, HEAD)
    scaled = attended * lax.rsqrt(lax.optimization_barrier(jnp.mean(attended * attended, axis=-1, keepdims=True)) + epsilon)
    head_out = scaled.astype(jnp.bfloat16).reshape(extent, HEADS * HEAD)
    set_width = HEADS * HEAD // N_TP
    mixed = jnp.zeros((extent, D), jnp.float32)
    for member in range(N_TP):
        col_start = member * set_width
        mixed = mixed + rounded(jnp.dot(head_out[:, col_start:col_start + set_width], w_out[col_start:col_start + set_width], preferred_element_type=jnp.float32))
    stream = (residual.astype(jnp.float32) + mixed).astype(jnp.bfloat16)
    stream_float = stream.astype(jnp.float32)
    ffn_in = (stream_float * lax.rsqrt(lax.optimization_barrier(jnp.mean(stream_float * stream_float, axis=-1, keepdims=True)) + epsilon) * ffn_gain).astype(jnp.bfloat16)
    picks_flat = pick_ids.reshape(-1).astype(jnp.int32)
    total_picks = picks_flat.shape[0]
    ordering = jnp.argsort(picks_flat, stable=True).astype(jnp.int32)
    sorted_ids = picks_flat[ordering]
    tallies = lax.optimization_barrier(jnp.sum((picks_flat[None, :] == jnp.arange(EXPERTS, dtype=jnp.int32)[:, None]).astype(jnp.int32), axis=1)).astype(jnp.int32)
    offsets = (jnp.cumsum(tallies) - tallies).astype(jnp.int32)
    within = (jnp.arange(total_picks, dtype=jnp.int32) - offsets[sorted_ids]).astype(jnp.int32)
    room = N_SP * N_TP * CAP
    table = jnp.full((EXPERTS, room), total_picks, jnp.int32).at[sorted_ids, within].set(ordering)
    padded = jnp.concatenate([ffn_in, jnp.zeros((1, D), jnp.bfloat16)], axis=0)
    unit_width = FF // N_TP

    def run_expert(operands):
        row_ids, gate_matrix, up_matrix, down_matrix = operands
        inputs = padded[row_ids // TOP]
        hidden = (jax.nn.silu(jnp.dot(inputs, gate_matrix, preferred_element_type=jnp.float32)) * jnp.dot(inputs, up_matrix, preferred_element_type=jnp.float32)).astype(jnp.bfloat16)
        summed = jnp.zeros((room, D), jnp.float32)
        for member in range(N_TP):
            unit_start = member * unit_width
            summed = summed + rounded(jnp.dot(hidden[:, unit_start:unit_start + unit_width], down_matrix[unit_start:unit_start + unit_width], preferred_element_type=jnp.float32))
        return summed.astype(jnp.bfloat16)
    results = lax.map(run_expert, (table, w_gate, w_up, w_down))
    per_pick = jnp.zeros((total_picks + 1, D), jnp.bfloat16).at[table.reshape(-1)].set(results.reshape(-1, D))
    per_pick = per_pick[:total_picks].astype(jnp.float32).reshape(extent, TOP, D)
    blended = jax.nn.sigmoid(pair_logit)[:, None] * per_pick[:, 0] + jax.nn.sigmoid(-pair_logit)[:, None] * per_pick[:, 1]
    blend_scale = lax.rsqrt(lax.optimization_barrier(jnp.mean(blended * blended, axis=-1, keepdims=True)) + epsilon)
    return (stream_float + blended * blend_scale * out_gain).astype(jnp.bfloat16)
```

```python
import jax
import jax.numpy as jnp
from jax import lax
from jax.experimental import pallas as pl
from jax.experimental.pallas import tpu as pltpu
from jax.sharding import PartitionSpec as P

HEAD = 128
TOP = 2


epsilon = 1e-06


def split_up(shard, dim, peers):
    before, after = (shard.shape[:dim], shard.shape[dim + 1 :])
    return jnp.moveaxis(shard.reshape(*before, peers, -1, *after), dim, 0)


def summed_on_arrival(shard, axis, dim):
    parts = split_up(shard, dim, lax.axis_size(axis))
    arrived = lax.all_to_all(parts, axis, split_axis=0, concat_axis=0, tiled=True)
    return arrived.astype(jnp.float32).sum(axis=0)


LOG2E = 1.4426950408889634
KEY_BLOCK = 256
ROWS = 128


def attention_kernel(place_ref, bias_ref, query_ref, kv_ref, out_ref, stacked, outputs, used):
    place = place_ref[0]
    heads = query_ref.shape[1] // HEAD
    rows = query_ref.shape[0]
    for head in range(heads):
        stacked[head * rows : (head + 1) * rows] = query_ref[:, head * HEAD : (head + 1) * HEAD]
    outputs[...] = jnp.zeros_like(outputs)
    used[...] = jnp.zeros_like(used)
    later = (
        lax.broadcasted_iota(jnp.int32, (KEY_BLOCK, KEY_BLOCK), 0)
        > lax.broadcasted_iota(jnp.int32, (KEY_BLOCK, KEY_BLOCK), 1)
    ).astype(jnp.float32).astype(jnp.bfloat16)
    factor = HEAD ** (-0.5) * LOG2E
    needed = (place * rows + rows + KEY_BLOCK - 1) // KEY_BLOCK

    def visit(block, masked):
        keys = kv_ref[pl.ds(pl.multiple_of(block * KEY_BLOCK, KEY_BLOCK), KEY_BLOCK), :HEAD]
        values = kv_ref[pl.ds(pl.multiple_of(block * KEY_BLOCK, KEY_BLOCK), KEY_BLOCK), HEAD:]
        scores = lax.dot_general(
            stacked[...], keys, (((1,), (1,)), ((), ())), preferred_element_type=jnp.float32
        )
        breaks, leads = [], []
        if masked:
            query_pos = place * rows + lax.broadcasted_iota(jnp.int32, (rows, KEY_BLOCK), 0)
            key_pos = block * KEY_BLOCK + lax.broadcasted_iota(jnp.int32, (rows, KEY_BLOCK), 1)
            before = key_pos < query_pos
        for head in range(heads):
            z = scores[head * rows : (head + 1) * rows] * factor + bias_ref[head] * LOG2E
            log_term = jnp.log2(1.0 + jnp.exp2(-jnp.abs(z)))
            softplus = jnp.maximum(z, 0.0) + log_term
            if masked:
                softplus = jnp.where(before, softplus, 0.0)
            breaks.append(softplus)
            leads.append(jnp.minimum(z, 0.0) - log_term)
        behind = jnp.dot(
            jnp.concatenate([b.astype(jnp.bfloat16) for b in breaks], axis=0),
            later,
            preferred_element_type=jnp.float32,
        )
        weights = []
        for head in range(heads):
            at = slice(head * rows, (head + 1) * rows)
            past = behind[at]
            gone = used[at]
            weight = jnp.exp2(leads[head] - past - jnp.concatenate([gone, gone], axis=1))
            if masked:
                weight = jnp.where(before, weight, 0.0)
            weights.append(weight.astype(jnp.bfloat16))
            used[at] = gone + jnp.broadcast_to(past[:, :1] + breaks[head][:, :1], gone.shape)
        outputs[...] += jnp.dot(
            jnp.concatenate(weights, axis=0), values, preferred_element_type=jnp.float32
        )

    visit(needed - 1, True)

    def step(index, carried):
        visit(needed - 2 - index, False)
        return carried

    lax.fori_loop(0, needed - 1, step, 0)
    for head in range(heads):
        output = outputs[head * rows : (head + 1) * rows]
        scaled = output * lax.rsqrt(jnp.mean(output * output, axis=-1, keepdims=True) + epsilon)
        out_ref[:, head * HEAD : (head + 1) * HEAD] = scaled.astype(jnp.bfloat16)


def attend(queries, key_values, break_bias, position):
    rows, width = queries.shape
    stack = rows * (width // HEAD)
    return pl.pallas_call(
        attention_kernel,
        name="stick_attention",
        out_shape=jax.ShapeDtypeStruct((rows, width), jnp.bfloat16),
        in_specs=[
            pl.BlockSpec(memory_space=pltpu.SMEM),
            pl.BlockSpec(memory_space=pltpu.SMEM),
            pl.BlockSpec(memory_space=pltpu.VMEM),
            pl.BlockSpec(memory_space=pltpu.VMEM),
        ],
        out_specs=pl.BlockSpec(memory_space=pltpu.VMEM),
        scratch_shapes=[
            pltpu.VMEM((stack, HEAD), jnp.bfloat16),
            pltpu.VMEM((stack, HEAD), jnp.float32),
            pltpu.VMEM((stack, HEAD), jnp.float32),
        ],
        compiler_params=pltpu.CompilerParams(vmem_limit_bytes=40 * 1024 * 1024),
    )(position, break_bias, queries, key_values)


def on_device(
    queries,
    keys,
    values,
    break_bias,
    residual,
    w_out,
    ffn_gain,
    pick_ids,
    pair_logit,
    w_gate,
    w_up,
    w_down,
    out_gain,
):
    length = queries.shape[0]
    position = lax.axis_index("sp")
    own = jnp.concatenate([keys, values], axis=1)
    key_values = lax.all_gather(own, "sp", axis=0, tiled=True)
    head_out = attend(queries, key_values, break_bias, position.reshape(1).astype(jnp.int32))
    quarters = lax.axis_size("tp")
    quarter = lax.axis_index("tp")
    slice_rows = length // quarters
    width = w_out.shape[1]
    experts = lax.axis_size("sp")
    capacity = max(2, (3 * slice_rows + experts - 1) // experts)
    mixed = summed_on_arrival(
        jnp.dot(head_out, w_out, preferred_element_type=jnp.float32).astype(jnp.bfloat16), "tp", 0
    )
    stream = (residual.astype(jnp.float32) + mixed).astype(jnp.bfloat16)
    routed = lax.dynamic_slice_in_dim(pick_ids, quarter * slice_rows, slice_rows, 0)[None]
    stream_float = stream.astype(jnp.float32)
    ffn_in = (
        stream_float
        * lax.rsqrt(jnp.mean(stream_float * stream_float, axis=-1, keepdims=True) + epsilon)
        * ffn_gain
    ).astype(jnp.bfloat16)
    blocks = routed.shape[0]
    entries = ffn_in.reshape(blocks, slice_rows, width)
    flat_ids = routed.reshape(blocks, slice_rows * TOP)
    places = jnp.arange(slice_rows * TOP, dtype=jnp.int32)
    earlier = places[None, :] < places[:, None]
    matches = (flat_ids[:, :, None] == flat_ids[:, None, :]) & earlier[None]
    ranks = jnp.sum(matches.astype(jnp.int32), axis=2)
    targets = (flat_ids * capacity + ranks).reshape(blocks, slice_rows, TOP)
    block_ids = jnp.arange(blocks, dtype=jnp.int32)[:, None]
    outgoing = jnp.zeros((blocks, experts * capacity, width), jnp.bfloat16)
    for pick_index in range(TOP):
        outgoing = outgoing.at[block_ids, targets[:, :, pick_index]].set(entries)
    arrived = lax.all_to_all(outgoing, "sp", split_axis=1, concat_axis=1, tiled=True).reshape(
        -1, width
    )
    piece = lax.all_gather(arrived, "tp", axis=0, tiled=True)
    gated = jax.nn.silu(jnp.dot(piece, w_gate[0], preferred_element_type=jnp.float32))
    hidden = (gated * jnp.dot(piece, w_up[0], preferred_element_type=jnp.float32)).astype(
        jnp.bfloat16
    )
    results = summed_on_arrival(
        jnp.dot(hidden, w_down[0], preferred_element_type=jnp.float32).astype(jnp.bfloat16), "tp", 0
    ).astype(jnp.bfloat16)
    returned = lax.all_to_all(results, "sp", split_axis=0, concat_axis=0, tiled=True)
    own_targets = targets[0]
    logits = lax.dynamic_slice_in_dim(pair_logit, quarter * slice_rows, slice_rows, 0)
    leading = returned[own_targets[:, 0]].astype(jnp.float32)
    trailing = returned[own_targets[:, 1]].astype(jnp.float32)
    blended = (
        jax.nn.sigmoid(logits)[:, None] * leading + jax.nn.sigmoid(-logits)[:, None] * trailing
    )
    blend_scale = lax.rsqrt(jnp.mean(blended * blended, axis=-1, keepdims=True) + epsilon)
    return (stream_float + blended * blend_scale * out_gain).astype(jnp.bfloat16)


def solution(mesh):
    placed = (
        P("sp", "tp"),
        P("sp", "tp"),
        P("sp", "tp"),
        P("tp"),
        P(("sp", "tp"), None),
        P("tp", None),
        P(),
        P("sp", None),
        P("sp"),
        P("sp", None, "tp"),
        P("sp", None, "tp"),
        P("sp", "tp", None),
        P(),
    )
    return jax.shard_map(
        on_device, mesh=mesh, in_specs=placed, out_specs=P(("sp", "tp"), None), check_vma=False
    )
```

```python
import functools

import jax
import jax.numpy as jnp
from jax import lax
from jax.experimental import pallas as pl
from jax.experimental.pallas import tpu as pltpu
from jax.sharding import PartitionSpec as P

HEAD = 128
TOP = 2
Z_SIZE = 8
X_SIZE = 4
CORES = 2
Z_PLANE = X_SIZE * CORES

epsilon = 1e-06


def split_up(shard, dim, peers):
    before, after = (shard.shape[:dim], shard.shape[dim + 1 :])
    return jnp.moveaxis(shard.reshape(*before, peers, -1, *after), dim, 0)


LOG2E = 1.4426950408889634
KEY_BLOCK = 256


def causal_visit(state, query_ref, kv_ref, bias_ref, later, block, first_query):
    outputs, used = state
    rows = query_ref.shape[0] // bias_ref.shape[0]
    heads = bias_ref.shape[0]
    factor = HEAD ** (-0.5) * LOG2E
    at_block = pl.ds(pl.multiple_of(block * KEY_BLOCK, KEY_BLOCK), KEY_BLOCK)
    keys = kv_ref[at_block, :HEAD]
    values = kv_ref[at_block, HEAD:]
    scores = lax.dot_general(
        query_ref[...], keys, (((1,), (1,)), ((), ())), preferred_element_type=jnp.float32
    )
    if first_query is not None:
        query_pos = first_query + lax.broadcasted_iota(jnp.int32, (rows, KEY_BLOCK), 0)
        key_pos = block * KEY_BLOCK + lax.broadcasted_iota(jnp.int32, (rows, KEY_BLOCK), 1)
        before = key_pos < query_pos
    breaks, leads = [], []
    for head in range(heads):
        z = scores[head * rows : (head + 1) * rows] * factor + bias_ref[head] * LOG2E
        log_term = jnp.log2(1.0 + jnp.exp2(-jnp.abs(z)))
        softplus = jnp.maximum(z, 0.0) + log_term
        if first_query is not None:
            softplus = jnp.where(before, softplus, 0.0)
        breaks.append(softplus)
        leads.append(jnp.minimum(z, 0.0) - log_term)
    behind = jnp.dot(
        jnp.concatenate([b.astype(jnp.bfloat16) for b in breaks], axis=0),
        later,
        preferred_element_type=jnp.float32,
    )
    weights = []
    for head in range(heads):
        at = slice(head * rows, (head + 1) * rows)
        past = behind[at]
        gone = used[at]
        weight = jnp.exp2(leads[head] - past - jnp.concatenate([gone, gone], axis=1))
        if first_query is not None:
            weight = jnp.where(before, weight, 0.0)
        weights.append(weight.astype(jnp.bfloat16))
        used[at] = gone + jnp.broadcast_to(past[:, :1] + breaks[head][:, :1], gone.shape)
    outputs[...] += jnp.dot(
        jnp.concatenate(weights, axis=0), values, preferred_element_type=jnp.float32
    )


def later_keys():
    return (
        lax.broadcasted_iota(jnp.int32, (KEY_BLOCK, KEY_BLOCK), 0)
        > lax.broadcasted_iota(jnp.int32, (KEY_BLOCK, KEY_BLOCK), 1)
    ).astype(jnp.float32).astype(jnp.bfloat16)


def lay_out(own_ref, twin_ref, plane, place):
    lanes = (place // CORES) % X_SIZE
    core = place % CORES
    length = own_ref.shape[1]
    for shift in range(X_SIZE):
        source = ((lanes + X_SIZE - shift) % X_SIZE) * CORES
        plane[pl.ds(pl.multiple_of((source + core) * length, length), length)] = own_ref[shift]
        plane[pl.ds(pl.multiple_of((source + 1 - core) * length, length), length)] = twin_ref[shift]


def own_plane_kernel(place_ref, bias_ref, query_ref, own_ref, twin_ref, near, near_used, far, plane):
    place = place_ref[0]
    lay_out(own_ref, twin_ref, plane, place)
    for ref in (near, near_used, far):
        ref[...] = jnp.zeros_like(ref)
    later = later_keys()
    rows = query_ref.shape[0] // bias_ref.shape[0]
    first_query = (place % (X_SIZE * CORES)) * rows
    last = (first_query + rows - 1) // KEY_BLOCK
    causal_visit((near, near_used), query_ref, plane, bias_ref, later, last, first_query)

    def step(index, carried):
        causal_visit((near, near_used), query_ref, plane, bias_ref, later, last - 1 - index, None)
        return carried

    lax.fori_loop(0, last, step, 0)


def whole_plane(state, query_ref, plane, bias_ref):
    later = later_keys()
    blocks = plane.shape[0] // KEY_BLOCK

    def step(index, carried):
        causal_visit(state, query_ref, plane, bias_ref, later, blocks - 1 - index, None)
        return carried

    lax.fori_loop(0, blocks, step, 0)


def two_planes_kernel(distance, place_ref, bias_ref, query_ref, below, below_twin, above, above_twin,
                      near_in, near_used_in, far_in, near, near_used, far, plane, found, found_used):
    place = place_ref[0]
    level = place // (X_SIZE * CORES)

    @pl.when(level >= distance)
    def _():
        lay_out(below, below_twin, plane, place)
        whole_plane((near, near_used), query_ref, plane, bias_ref)

    @pl.when(level + distance >= Z_SIZE)
    def _():
        lay_out(above, above_twin, plane, place)
        found[...] = jnp.zeros_like(found)
        found_used[...] = jnp.zeros_like(found_used)
        whole_plane((found, found_used), query_ref, plane, bias_ref)
        far[...] = found[...] + jnp.exp2(-found_used[...]) * far[...]


def last_plane_kernel(distance, place_ref, bias_ref, query_ref, below, below_twin,
                      near_in, near_used_in, far_in, out_ref, plane, near, near_used):
    place = place_ref[0]
    near[...] = near_in[...]
    near_used[...] = near_used_in[...]

    @pl.when(place // (X_SIZE * CORES) >= distance)
    def _():
        lay_out(below, below_twin, plane, place)
        whole_plane((near, near_used), query_ref, plane, bias_ref)

    rows = out_ref.shape[0]
    for head in range(bias_ref.shape[0]):
        at = slice(head * rows, (head + 1) * rows)
        output = near[at] + jnp.exp2(-near_used[at]) * far_in[at]
        scaled = output * lax.rsqrt(jnp.mean(output * output, axis=-1, keepdims=True) + epsilon)
        out_ref[:, head * HEAD : (head + 1) * HEAD] = scaled.astype(jnp.bfloat16)


def attention_call(kernel, name, planes, position, break_bias, stacked, key_values, state, rows):
    stack = stacked.shape[0]
    in_vmem = pl.BlockSpec(memory_space=pltpu.VMEM)
    in_smem = pl.BlockSpec(memory_space=pltpu.SMEM)
    plane = pltpu.VMEM((Z_PLANE * rows, 2 * HEAD), jnp.bfloat16)
    running = pltpu.VMEM((stack, HEAD), jnp.float32)
    kept = jax.ShapeDtypeStruct((stack, HEAD), jnp.float32)
    last = name == "attend_last"
    keys = planes * Z_PLANE * rows
    first_state = 3 + len(key_values)
    return pl.pallas_call(
        kernel,
        name=name,
        out_shape=jax.ShapeDtypeStruct((rows, stack // rows * HEAD), jnp.bfloat16) if last else (kept,) * 3,
        in_specs=[in_smem, in_smem] + [in_vmem] * (1 + len(key_values) + len(state)),
        out_specs=in_vmem if last else (in_vmem,) * 3,
        scratch_shapes=[plane] + ([] if not state else [running, running]),
        input_output_aliases={} if last or not state else {first_state + i: i for i in range(3)},
        cost_estimate=pl.CostEstimate(
            flops=2 * stack * keys * (2 * HEAD + KEY_BLOCK), transcendentals=3 * stack * keys, bytes_accessed=0
        ),
        compiler_params=pltpu.CompilerParams(vmem_limit_bytes=24 * 1024 * 1024),
    )(position, break_bias, stacked, *key_values, *state)


def moved(shard, step_z, step_x, swap):
    pairs = []
    for place in range(Z_SIZE * Z_PLANE):
        z, x, core = place // Z_PLANE, place // CORES % X_SIZE, place % CORES
        target = ((z + step_z) % Z_SIZE * X_SIZE + (x + step_x) % X_SIZE) * CORES + (core ^ swap)
        pairs.append((place, target))
    return lax.ppermute(shard, "sp", pairs)


def attend(queries, keys, values, break_bias, position):
    rows = queries.shape[0]
    heads = queries.shape[1] // HEAD
    stacked = jnp.concatenate([queries[:, h * HEAD : (h + 1) * HEAD] for h in range(heads)], axis=0)
    block = jnp.concatenate([keys, values], axis=1)
    own = jnp.stack([block] + [moved(block, 0, step, 0) for step in range(1, X_SIZE)])
    twin = moved(own, 0, 0, 1)
    common = (position, break_bias, stacked)
    below, above = own, own
    arrived = []
    for distance in range(1, Z_SIZE // 2 + 1):
        below = moved(below, 1, 0, 0)
        pieces = [below]
        if distance < Z_SIZE // 2:
            above = moved(above, -1, 0, 0)
            pieces.append(above)
        arrived.append([part for piece in pieces for part in (piece, moved(piece, 0, 0, 1))])
    state = attention_call(own_plane_kernel, "attend_own", 1, *common, (own, twin), (), rows)
    for distance in range(1, Z_SIZE // 2):
        kernel = functools.partial(two_planes_kernel, distance)
        state = attention_call(kernel, "attend_two", 2, *common, arrived[distance - 1], state, rows)
    kernel = functools.partial(last_plane_kernel, Z_SIZE // 2)
    return attention_call(kernel, "attend_last", 1, *common, arrived[-1], state, rows)


COLUMNS = 1024


def in_kernel(kernel, name, out_shapes, megabytes, flops, *operands, scratch=()):
    spec = pl.BlockSpec(memory_space=pltpu.VMEM)
    several = isinstance(out_shapes, tuple)
    return pl.pallas_call(
        kernel,
        name=name,
        out_shape=out_shapes,
        in_specs=[spec] * len(operands),
        out_specs=(spec,) * len(out_shapes) if several else spec,
        scratch_shapes=list(scratch),
        cost_estimate=pl.CostEstimate(flops=flops, transcendentals=0, bytes_accessed=0),
        compiler_params=pltpu.CompilerParams(vmem_limit_bytes=megabytes * 1024 * 1024),
    )(*operands)


def dispatch_kernel(mixed_ref, residual_ref, gain_ref, targets_ref, stream_ref, outgoing_ref):
    rows, width = residual_ref.shape
    slots = outgoing_ref.shape[0] * outgoing_ref.shape[1]
    total = jnp.zeros((rows, 1), jnp.float32)
    for start in range(0, width, COLUMNS):
        at = slice(start, start + COLUMNS)
        mixed = mixed_ref[0, :, at].astype(jnp.float32)
        for member in range(1, mixed_ref.shape[0]):
            mixed = mixed + mixed_ref[member, :, at].astype(jnp.float32)
        stream = (residual_ref[:, at].astype(jnp.float32) + mixed).astype(jnp.bfloat16)
        stream_ref[:, at] = stream
        wide = stream.astype(jnp.float32)
        total = total + jnp.sum(wide * wide, axis=1, keepdims=True)
    scale = lax.rsqrt(total / width + epsilon)
    slot = lax.broadcasted_iota(jnp.int32, (slots, rows), 0)
    chosen = (slot == targets_ref[0:1, :]) | (slot == targets_ref[1:2, :])
    chosen = chosen.astype(jnp.float32).astype(jnp.bfloat16)
    for start in range(0, width, COLUMNS):
        at = slice(start, start + COLUMNS)
        normed = (stream_ref[:, at].astype(jnp.float32) * scale * gain_ref[:, at]).astype(jnp.bfloat16)
        sent = jnp.dot(chosen, normed, preferred_element_type=jnp.float32).astype(jnp.bfloat16)
        outgoing_ref[:, :, at] = sent.reshape(outgoing_ref.shape[0], outgoing_ref.shape[1], COLUMNS)


def expert_kernel(*refs):
    count = (len(refs) - 3) // 2
    inputs, outs = refs[:count], refs[count + 3 :]
    gate_ref, up_ref, down_ref = refs[count : count + 3]
    for source, out in zip(inputs, outs):
        slots = source.shape[0] * source.shape[1]
        width = source.shape[2]
        entries = source[...].reshape(slots, width)
        gate = jnp.dot(entries, gate_ref[...], preferred_element_type=jnp.float32)
        up = jnp.dot(entries, up_ref[...], preferred_element_type=jnp.float32)
        hidden = (gate / (1.0 + jnp.exp(-gate)) * up).astype(jnp.bfloat16)
        for start in range(0, width, COLUMNS):
            at = slice(start, start + COLUMNS)
            share = jnp.dot(hidden, down_ref[:, at], preferred_element_type=jnp.float32)
            out[:, :, at] = share.astype(jnp.bfloat16).reshape(source.shape[0], source.shape[1], COLUMNS)


def run_experts(pieces, weights, name):
    shapes = tuple(jax.ShapeDtypeStruct(piece.shape, jnp.bfloat16) for piece in pieces)
    slots = sum(piece.shape[0] * piece.shape[1] for piece in pieces)
    flops = 6 * slots * weights[0].shape[0] * weights[0].shape[1]
    return in_kernel(expert_kernel, name, shapes, 32, flops, *pieces, *weights)


def final_kernel(returned_ref, targets_ref, logits_ref, stream_ref, gain_ref, out_ref, blended):
    rows, width = stream_ref.shape
    slots = returned_ref.shape[0] * returned_ref.shape[1]
    slot = lax.broadcasted_iota(jnp.int32, (rows, slots), 1)
    picks = [
        (slot == targets_ref[:, pick : pick + 1]).astype(jnp.float32).astype(jnp.bfloat16) for pick in range(TOP)
    ]
    logits = logits_ref[...]
    shares = (1.0 / (1.0 + jnp.exp(-logits)), 1.0 / (1.0 + jnp.exp(logits)))
    total = jnp.zeros((rows, 1), jnp.float32)
    for start in range(0, width, COLUMNS):
        at = slice(start, start + COLUMNS)
        entries = returned_ref[:, :, at].reshape(slots, COLUMNS)
        mix = shares[0] * jnp.dot(picks[0], entries, preferred_element_type=jnp.float32)
        mix = mix + shares[1] * jnp.dot(picks[1], entries, preferred_element_type=jnp.float32)
        blended[:, at] = mix
        total = total + jnp.sum(mix * mix, axis=1, keepdims=True)
    scale = lax.rsqrt(total / width + epsilon)
    for start in range(0, width, COLUMNS):
        at = slice(start, start + COLUMNS)
        wide = stream_ref[:, at].astype(jnp.float32)
        out_ref[:, at] = (wide + blended[:, at] * scale * gain_ref[:, at]).astype(jnp.bfloat16)


def along_tp(shard, step):
    size = lax.axis_size("tp")
    return lax.ppermute(shard, "tp", [(member, (member + step) % size) for member in range(size)])


def expert_outputs(own, weights):
    half = own.shape[0] // 2
    from_below = along_tp(own, 1)
    from_above = along_tp(own, -1)
    (share_own,) = run_experts((own,), weights, "experts_own")
    far_first = along_tp(from_below[:half], 1)
    far_second = along_tp(from_above[half:], -1)
    share_below, share_above = run_experts((from_below, from_above), weights, "experts_near")
    direct_up = along_tp(share_above[half:], 1)
    direct_down = along_tp(share_below[:half], -1)
    far_share_first, far_share_second = run_experts((far_first, far_second), weights, "experts_far")
    relay_up = along_tp(far_share_first, 1)
    relay_down = along_tp(far_share_second, -1)
    both_up = along_tp(added(share_above[:half], relay_up), 1)
    both_down = along_tp(added(share_below[half:], relay_down), -1)
    first = added(share_own[:half], both_up, direct_down)
    second = added(share_own[half:], direct_up, both_down)
    return jnp.concatenate([first, second], axis=0)


def added(*parts):
    total = parts[0].astype(jnp.float32)
    for part in parts[1:]:
        total = total + part.astype(jnp.float32)
    return total.astype(jnp.bfloat16)


def on_device(
    queries,
    keys,
    values,
    break_bias,
    residual,
    w_out,
    ffn_gain,
    pick_ids,
    pair_logit,
    w_gate,
    w_up,
    w_down,
    out_gain,
):
    position = lax.axis_index("sp")
    quarters = lax.axis_size("tp")
    quarter = lax.axis_index("tp")
    slice_rows = queries.shape[0] // quarters
    width = w_out.shape[1]
    experts = lax.axis_size("sp")
    capacity = max(2, (3 * slice_rows + experts - 1) // experts)
    routed = lax.dynamic_slice_in_dim(pick_ids, quarter * slice_rows, slice_rows, 0)
    flat_ids = routed.reshape(slice_rows * TOP)
    places = jnp.arange(slice_rows * TOP, dtype=jnp.int32)
    matches = (flat_ids[:, None] == flat_ids[None, :]) & (places[None, :] < places[:, None])
    ranks = jnp.sum(matches.astype(jnp.int32), axis=1)
    targets = (flat_ids * capacity + ranks).reshape(slice_rows, TOP)
    logits = lax.dynamic_slice_in_dim(pair_logit, quarter * slice_rows, slice_rows, 0)[:, None]

    head_out = attend(queries, keys, values, break_bias, position.reshape(1).astype(jnp.int32))
    partial = jnp.dot(head_out, w_out, preferred_element_type=jnp.float32).astype(jnp.bfloat16)
    parts = split_up(partial, 0, quarters)
    mixed = lax.all_to_all(parts, "tp", split_axis=0, concat_axis=0, tiled=True)
    slots = jax.ShapeDtypeStruct((experts, capacity, width), jnp.bfloat16)
    rows = jax.ShapeDtypeStruct((slice_rows, width), jnp.bfloat16)
    dispatch_flops = 2 * experts * capacity * slice_rows * width
    stream, outgoing = in_kernel(
        dispatch_kernel, "dispatch", (rows, slots), 16, dispatch_flops,
        mixed, residual, ffn_gain[None], targets.T,
    )
    arrived = lax.all_to_all(outgoing, "sp", split_axis=0, concat_axis=0, tiled=True)
    results = expert_outputs(arrived, (w_gate[0], w_up[0], w_down[0]))
    returned = lax.all_to_all(results, "sp", split_axis=0, concat_axis=0, tiled=True)
    return in_kernel(
        final_kernel, "blend", rows, 16, 2 * dispatch_flops,
        returned, targets, logits, stream, out_gain[None],
        scratch=[pltpu.VMEM((slice_rows, width), jnp.float32)],
    )


def solution(mesh):
    placed = (
        P("sp", "tp"),
        P("sp", "tp"),
        P("sp", "tp"),
        P("tp"),
        P(("sp", "tp"), None),
        P("tp", None),
        P(),
        P("sp", None),
        P("sp"),
        P("sp", None, "tp"),
        P("sp", None, "tp"),
        P("sp", "tp", None),
        P(),
    )
    return jax.shard_map(
        on_device, mesh=mesh, in_specs=placed, out_specs=P(("sp", "tp"), None), check_vma=False
    )
```

```python
import functools

import jax
import jax.numpy as jnp
from jax import lax
from jax.experimental import pallas as pl
from jax.experimental.pallas import tpu as pltpu
from jax.sharding import PartitionSpec as P


HEAD = 128
TOP = 2
Z_SIZE = 8
X_SIZE = 4
CORES = 2
Z_PLANE = X_SIZE * CORES

epsilon = 1e-06


def split_up(shard, dim, peers):
    before, after = (shard.shape[:dim], shard.shape[dim + 1 :])
    return jnp.moveaxis(shard.reshape(*before, peers, -1, *after), dim, 0)


LOG2E = 1.4426950408889634
KEY_BLOCK = 256
PICK_ROWS = 8


def causal_visit(state, query_ref, kv_ref, bias_ref, later, block, first_query):
    outputs, used = state
    rows = query_ref.shape[0] // bias_ref.shape[0]
    heads = bias_ref.shape[0]
    factor = HEAD ** (-0.5) * LOG2E
    at_block = pl.ds(pl.multiple_of(block * KEY_BLOCK, KEY_BLOCK), KEY_BLOCK)
    keys = kv_ref[at_block, :HEAD]
    values = kv_ref[at_block, HEAD:]
    scores = lax.dot_general(
        query_ref[...], keys, (((1,), (1,)), ((), ())), preferred_element_type=jnp.float32
    )
    if first_query is not None:
        query_pos = first_query + lax.broadcasted_iota(jnp.int32, (rows, KEY_BLOCK), 0)
        key_pos = block * KEY_BLOCK + lax.broadcasted_iota(jnp.int32, (rows, KEY_BLOCK), 1)
        before = key_pos < query_pos
    breaks, leads = [], []
    for head in range(heads):
        z = scores[head * rows : (head + 1) * rows] * factor + bias_ref[head] * LOG2E
        log_term = jnp.log2(1.0 + jnp.exp2(-jnp.abs(z)))
        softplus = jnp.maximum(z, 0.0) + log_term
        leads.append(z - softplus)
        breaks.append(softplus if first_query is None else jnp.where(before, softplus, 0.0))
    behind = jnp.dot(
        jnp.concatenate([b.astype(jnp.bfloat16) for b in breaks], axis=0),
        later,
        preferred_element_type=jnp.float32,
    )
    weights = []
    for head in range(heads):
        at = slice(head * rows, (head + 1) * rows)
        past = behind[at]
        gone = used[at]
        weight = jnp.exp2(leads[head] - past - jnp.concatenate([gone, gone], axis=1))
        if first_query is not None:
            weight = jnp.where(before, weight, 0.0)
        weights.append(weight.astype(jnp.bfloat16))
        used[at] = gone + jnp.broadcast_to(past[:, :1] + breaks[head][:, :1], gone.shape)
    outputs[...] += jnp.dot(
        jnp.concatenate(weights, axis=0), values, preferred_element_type=jnp.float32
    )


def later_keys():
    return (
        lax.broadcasted_iota(jnp.int32, (KEY_BLOCK, KEY_BLOCK), 0)
        > lax.broadcasted_iota(jnp.int32, (KEY_BLOCK, KEY_BLOCK), 1)
    ).astype(jnp.float32).astype(jnp.bfloat16)


def lay_out(own_ref, twin_ref, plane, place):
    lanes = (place // CORES) % X_SIZE
    core = place % CORES
    length = own_ref.shape[1] - PICK_ROWS
    for shift in range(X_SIZE):
        source = ((lanes + X_SIZE - shift) % X_SIZE) * CORES
        plane[pl.ds(pl.multiple_of((source + core) * length, length), length)] = own_ref[shift, :length]
        plane[pl.ds(pl.multiple_of((source + 1 - core) * length, length), length)] = twin_ref[shift, :length]


def tally(counts, *pieces):
    expert = lax.broadcasted_iota(jnp.int32, counts.shape, 0).astype(jnp.float32)
    found = counts[...]
    for piece in pieces:
        length = piece.shape[1] - PICK_ROWS
        for shift in range(X_SIZE):
            picks = piece[shift, length:].astype(jnp.float32)[0:1]
            found = found + (picks == expert).astype(jnp.float32)
    counts[...] = found


def own_plane_kernel(place_ref, bias_ref, query_ref, own_ref, twin_ref, near, near_used, far, counts, plane):
    place = place_ref[0]
    lay_out(own_ref, twin_ref, plane, place)
    for ref in (near, near_used, far, counts):
        ref[...] = jnp.zeros_like(ref)
    tally(counts, own_ref, twin_ref)
    later = later_keys()
    rows = query_ref.shape[0] // bias_ref.shape[0]
    first_query = (place % (X_SIZE * CORES)) * rows
    last = (first_query + rows - 1) // KEY_BLOCK

    def step(index, carried):
        causal_visit((near, near_used), query_ref, plane, bias_ref, later, last - index, first_query)
        return carried

    lax.fori_loop(0, last + 1, step, 0)


def whole_plane(state, query_ref, plane, bias_ref):
    later = later_keys()
    blocks = plane.shape[0] // KEY_BLOCK

    def step(index, carried):
        causal_visit(state, query_ref, plane, bias_ref, later, blocks - 1 - 2 * index, None)
        causal_visit(state, query_ref, plane, bias_ref, later, blocks - 2 - 2 * index, None)
        return carried

    lax.fori_loop(0, blocks // 2, step, 0)


def two_planes_kernel(distance, place_ref, bias_ref, query_ref, below, below_twin, above, above_twin,
                      near_in, near_used_in, far_in, counts_in, near, near_used, far, counts,
                      planes, found, found_used):
    place = place_ref[0]
    tally(counts, below, below_twin, above, above_twin)
    level = place // (X_SIZE * CORES)
    lay_out(below, below_twin, planes.at[0], place)
    lay_out(above, above_twin, planes.at[1], place)

    def visit(side, carried):
        found[...] = jnp.zeros_like(found)
        found_used[...] = jnp.zeros_like(found_used)
        whole_plane((found, found_used), query_ref, planes.at[side], bias_ref)

        @pl.when(side == 0)
        def _():
            near[...] += jnp.exp2(-near_used[...]) * found[...]
            near_used[...] += found_used[...]

        @pl.when(side == 1)
        def _():
            far[...] = found[...] + jnp.exp2(-found_used[...]) * far[...]

        return carried

    first = jnp.where(level >= distance, 0, 1)
    past = jnp.where(level + distance >= Z_SIZE, 2, 1)
    lax.fori_loop(first, past, visit, 0)


def last_plane_kernel(distance, place_ref, bias_ref, query_ref, below, below_twin,
                      near_in, near_used_in, far_in, counts_in, out_ref, most_ref, plane, near, near_used, counts):
    place = place_ref[0]
    counts[...] = counts_in[...]
    tally(counts, below, below_twin)
    quarter = counts.shape[1] // 4
    lane = lax.broadcasted_iota(jnp.int32, counts.shape, 1) // quarter
    most = jnp.zeros((counts.shape[0], 1), jnp.float32)
    for member in range(4):
        named = jnp.sum(jnp.where(lane == member, counts[...], 0.0), axis=1, keepdims=True)
        most = jnp.maximum(most, named)
    most_ref[0] = jnp.max(most).astype(jnp.int32)
    near[...] = near_in[...]
    near_used[...] = near_used_in[...]

    @pl.when(place // (X_SIZE * CORES) >= distance)
    def _():
        lay_out(below, below_twin, plane, place)
        whole_plane((near, near_used), query_ref, plane, bias_ref)

    rows = out_ref.shape[0]
    for head in range(bias_ref.shape[0]):
        at = slice(head * rows, (head + 1) * rows)
        output = near[at] + jnp.exp2(-near_used[at]) * far_in[at]
        scaled = output * lax.rsqrt(jnp.mean(output * output, axis=-1, keepdims=True) + epsilon)
        out_ref[:, head * HEAD : (head + 1) * HEAD] = scaled.astype(jnp.bfloat16)


def attention_call(kernel, name, planes, position, break_bias, stacked, key_values, state, rows):
    stack = stacked.shape[0]
    in_vmem = pl.BlockSpec(memory_space=pltpu.VMEM)
    in_smem = pl.BlockSpec(memory_space=pltpu.SMEM)
    plane = (Z_PLANE * rows, 2 * HEAD)
    running = pltpu.VMEM((stack, HEAD), jnp.float32)
    kept = jax.ShapeDtypeStruct((stack, HEAD), jnp.float32)
    counts = (Z_SIZE * Z_PLANE, rows * TOP)
    last = name == "attend_last"
    keys = planes * Z_PLANE * rows
    first_state = 3 + len(key_values)
    heads = jax.ShapeDtypeStruct((rows, stack // rows * HEAD), jnp.bfloat16)
    return pl.pallas_call(
        kernel,
        out_shape=(heads, jax.ShapeDtypeStruct((1,), jnp.int32))
        if last
        else (kept,) * 3 + (jax.ShapeDtypeStruct(counts, jnp.float32),),
        in_specs=[in_smem, in_smem] + [in_vmem] * (1 + len(key_values) + len(state)),
        out_specs=(in_vmem, in_smem) if last else (in_vmem,) * 4,
        scratch_shapes=[pltpu.VMEM(plane if planes == 1 else (planes, *plane), jnp.bfloat16)]
        + ([running, running] if state else [])
        + ([pltpu.VMEM(counts, jnp.float32)] if last else []),
        input_output_aliases={} if last or not state else {first_state + i: i for i in range(4)},
        cost_estimate=pl.CostEstimate(
            flops=2 * stack * keys * (2 * HEAD + KEY_BLOCK), transcendentals=3 * stack * keys, bytes_accessed=0
        ),
        compiler_params=pltpu.CompilerParams(vmem_limit_bytes=24 * 1024 * 1024),
    )(position, break_bias, stacked, *key_values, *state)


def moved(shard, step_z, step_x, swap):
    pairs = []
    for place in range(Z_SIZE * Z_PLANE):
        z, x, core = place // Z_PLANE, place // CORES % X_SIZE, place % CORES
        target = ((z + step_z) % Z_SIZE * X_SIZE + (x + step_x) % X_SIZE) * CORES + (core ^ swap)
        pairs.append((place, target))
    return lax.ppermute(shard, "sp", pairs)


def attend(queries, keys, values, break_bias, pick_ids, position):
    rows = queries.shape[0]
    heads = queries.shape[1] // HEAD
    stacked = jnp.concatenate([queries[:, h * HEAD : (h + 1) * HEAD] for h in range(heads)], axis=0)
    picks = pick_ids.astype(jnp.bfloat16).reshape(1, rows * TOP)
    picks = jnp.concatenate([picks, jnp.zeros((PICK_ROWS - 1, rows * TOP), jnp.bfloat16)], axis=0)
    block = jnp.concatenate([jnp.concatenate([keys, values], axis=1), picks], axis=0)
    own = jnp.stack([block] + [moved(block, 0, step, 0) for step in range(1, X_SIZE)])
    twin = moved(own, 0, 0, 1)
    common = (position, break_bias, stacked)
    below, above = own, own
    arrived = []
    for distance in range(1, Z_SIZE // 2 + 1):
        below = moved(below, 1, 0, 0)
        pieces = [below, moved(below, 0, 0, 1)]
        if distance < Z_SIZE // 2:
            above = moved(above, -1, 0, 0)
            pieces += [above, moved(above, 0, 0, 1)]
        arrived.append(pieces)
    state = attention_call(own_plane_kernel, "attend_0", 1, *common, (own, twin), (), rows)
    for distance in range(1, Z_SIZE // 2):
        kernel = functools.partial(two_planes_kernel, distance)
        name = f"attend_{distance}"
        state = attention_call(kernel, name, 2, *common, arrived[distance - 1], state, rows)
    kernel = functools.partial(last_plane_kernel, Z_SIZE // 2)
    return attention_call(kernel, "attend_last", 1, *common, arrived[-1], state, rows)


COLUMNS = 1024
PACKED = 48


def in_kernel(kernel, out_shapes, megabytes, flops, *operands, scratch=()):
    spec = pl.BlockSpec(memory_space=pltpu.VMEM)
    several = isinstance(out_shapes, tuple)
    return pl.pallas_call(
        kernel,
        out_shape=out_shapes,
        in_specs=[spec] * len(operands),
        out_specs=(spec,) * len(out_shapes) if several else spec,
        scratch_shapes=list(scratch),
        cost_estimate=pl.CostEstimate(flops=flops, transcendentals=0, bytes_accessed=0),
        compiler_params=pltpu.CompilerParams(vmem_limit_bytes=megabytes * 1024 * 1024),
    )(*operands)


def over_columns(width, step, carried):
    def at_column(index, carried):
        return step(pl.ds(pl.multiple_of(index * COLUMNS, COLUMNS), COLUMNS), carried)

    return lax.fori_loop(0, width // COLUMNS, at_column, carried)


def dispatch_kernel(mixed_ref, residual_ref, gain_ref, targets_ref, stream_ref, outgoing_ref):
    rows, width = residual_ref.shape
    experts, capacity = outgoing_ref.shape[:2]

    def add(at, total):
        mixed = mixed_ref[0, :, at].astype(jnp.float32)
        for member in range(1, mixed_ref.shape[0]):
            mixed = mixed + mixed_ref[member, :, at].astype(jnp.float32)
        stream = (residual_ref[:, at].astype(jnp.float32) + mixed).astype(jnp.bfloat16)
        stream_ref[:, at] = stream
        wide = stream.astype(jnp.float32)
        return total + jnp.sum(wide * wide, axis=1, keepdims=True)

    total = over_columns(width, add, jnp.zeros((rows, 1), jnp.float32))
    scale = lax.rsqrt(total / width + epsilon)
    slot = lax.broadcasted_iota(jnp.int32, (experts * capacity, rows), 0)
    chosen = (slot == targets_ref[0:1, :]) | (slot == targets_ref[1:2, :])
    chosen = chosen.astype(jnp.float32).astype(jnp.bfloat16)

    def send(at, carried):
        normed = (stream_ref[:, at].astype(jnp.float32) * scale * gain_ref[:, at]).astype(jnp.bfloat16)
        sent = jnp.dot(chosen, normed, preferred_element_type=jnp.float32).astype(jnp.bfloat16)
        outgoing_ref[:, :, at] = sent.reshape(experts, capacity, COLUMNS)
        return carried

    over_columns(width, send, 0)


def pack_kernel(arrived_ref, first_ref, second_ref, rest_ref, back_ref, entries):
    slots = arrived_ref.shape[0] * arrived_ref.shape[1]
    width = arrived_ref.shape[2]

    def read(at, largest):
        part = arrived_ref[:, :, at].reshape(slots, COLUMNS)
        entries[:, at] = part
        size = jnp.abs(part.astype(jnp.float32))
        for lane in range(0, COLUMNS, 128):
            largest = jnp.maximum(largest, size[:, lane : lane + 128])
        return largest

    largest = over_columns(width, read, jnp.zeros((slots, 128), jnp.float32))
    held = (jnp.max(largest, axis=1, keepdims=True) > 0).astype(jnp.float32)
    row = lax.broadcasted_iota(jnp.int32, (slots, slots), 0)
    column = lax.broadcasted_iota(jnp.int32, (slots, slots), 1)

    def product(left, right):
        left, right = left.astype(jnp.float32), right.astype(jnp.float32)
        return jnp.dot(
            left.astype(jnp.bfloat16), right.astype(jnp.bfloat16), preferred_element_type=jnp.float32
        )

    held_rows = jnp.broadcast_to(held, (slots, slots))
    held_columns = product(jnp.ones((slots, slots), jnp.float32), jnp.where(row == column, held_rows, 0.0))
    place_rows = product(column < row, held_rows)
    place_columns = product(held_columns, row < column)
    back = ((place_rows == column.astype(jnp.float32)) & (held_rows > 0)).astype(jnp.float32)
    back_ref[...] = back.astype(jnp.bfloat16)
    forth = ((place_columns == row.astype(jnp.float32)) & (held_columns > 0)).astype(jnp.float32)
    forth = forth.astype(jnp.bfloat16)
    half = first_ref.shape[0]

    def write(at, carried):
        packed = jnp.dot(forth, entries[:, at], preferred_element_type=jnp.float32).astype(jnp.bfloat16)
        first_ref[:, at] = packed[:half]
        second_ref[:, at] = packed[half : 2 * half]
        rest_ref[:, at] = packed[2 * half :]
        return carried

    over_columns(width, write, 0)


def expert_kernel(*refs):
    count = (len(refs) - 6) // 2
    inputs, outs = refs[:count], refs[count + 3 : -3]
    gate_ref, up_ref, down_ref = refs[count : count + 3]
    entries, gate, up = refs[-3:]
    half, width = inputs[0].shape
    for index, source in enumerate(inputs):
        entries[index * half : (index + 1) * half] = source[...]
    gate[...] = jnp.zeros_like(gate)
    up[...] = jnp.zeros_like(up)

    def rise(index, carried):
        at = pl.ds(pl.multiple_of(index * COLUMNS, COLUMNS), COLUMNS)
        part = entries[:, at]
        gate[...] += jnp.dot(part, gate_ref[at, :], preferred_element_type=jnp.float32)
        up[...] += jnp.dot(part, up_ref[at, :], preferred_element_type=jnp.float32)
        return carried

    lax.fori_loop(0, width // COLUMNS, rise, 0)
    hidden = (gate[...] / (1.0 + jnp.exp(-gate[...])) * up[...]).astype(jnp.bfloat16)

    def fall(index, carried):
        at = pl.ds(pl.multiple_of(index * COLUMNS, COLUMNS), COLUMNS)
        share = jnp.dot(hidden, down_ref[:, at], preferred_element_type=jnp.float32).astype(jnp.bfloat16)
        for place, out in enumerate(outs):
            out[:, at] = share[place * half : (place + 1) * half]
        return carried

    lax.fori_loop(0, width // COLUMNS, fall, 0)


def run_experts(pieces, weights):
    shapes = tuple(jax.ShapeDtypeStruct(piece.shape, jnp.bfloat16) for piece in pieces)
    slots = sum(piece.shape[0] for piece in pieces)
    width, units = weights[0].shape
    flops = 6 * slots * width * units
    scratch = [pltpu.VMEM((slots, width), jnp.bfloat16)] + [pltpu.VMEM((slots, units), jnp.float32)] * 2
    return in_kernel(expert_kernel, shapes, 32, flops, *pieces, *weights, scratch=scratch)


def final_kernel(returned_ref, targets_ref, logits_ref, stream_ref, gain_ref, out_ref, blended):
    rows, width = stream_ref.shape
    slots = returned_ref.shape[0] * returned_ref.shape[1]
    slot = lax.broadcasted_iota(jnp.int32, (rows, slots), 1)
    picks = [
        (slot == targets_ref[:, pick : pick + 1]).astype(jnp.float32).astype(jnp.bfloat16) for pick in range(TOP)
    ]
    logits = logits_ref[...]
    shares = (1.0 / (1.0 + jnp.exp(-logits)), 1.0 / (1.0 + jnp.exp(logits)))

    def mix(at, total):
        entries = returned_ref[:, :, at].reshape(slots, COLUMNS)
        both = shares[0] * jnp.dot(picks[0], entries, preferred_element_type=jnp.float32)
        both = both + shares[1] * jnp.dot(picks[1], entries, preferred_element_type=jnp.float32)
        blended[:, at] = both
        return total + jnp.sum(both * both, axis=1, keepdims=True)

    total = over_columns(width, mix, jnp.zeros((rows, 1), jnp.float32))
    scale = lax.rsqrt(total / width + epsilon)

    def add(at, carried):
        wide = stream_ref[:, at].astype(jnp.float32)
        out_ref[:, at] = (wide + blended[:, at] * scale * gain_ref[:, at]).astype(jnp.bfloat16)
        return carried

    over_columns(width, add, 0)


def along_tp(shard, step):
    size = lax.axis_size("tp")
    return lax.ppermute(shard, "tp", [(member, (member + step) % size) for member in range(size)])


def relay_kernel(own_up, far_up, own_down, far_down, up_ref, down_ref):
    for own, far, out in ((own_up, far_up, up_ref), (own_down, far_down, down_ref)):

        def step(index, carried):
            at = pl.ds(pl.multiple_of(index * COLUMNS, COLUMNS), COLUMNS)
            out[:, at] = (own[:, at].astype(jnp.float32) + far[:, at].astype(jnp.float32)).astype(jnp.bfloat16)
            return carried

        lax.fori_loop(0, out.shape[1] // COLUMNS, step, 0)


def unpack_kernel(back_ref, rest_ref, *refs):
    firsts, seconds, results_ref = refs[:3], refs[3:6], refs[6]
    _, width = firsts[0].shape

    def step(index, carried):
        at = pl.ds(pl.multiple_of(index * COLUMNS, COLUMNS), COLUMNS)
        sums = []
        for parts in (firsts, seconds):
            total = parts[0][:, at].astype(jnp.float32)
            for part in parts[1:]:
                total = total + part[:, at].astype(jnp.float32)
            sums.append(total.astype(jnp.bfloat16))
        packed = jnp.concatenate(sums + [rest_ref[:, at]], axis=0)
        spread = jnp.dot(back_ref[...], packed, preferred_element_type=jnp.float32).astype(jnp.bfloat16)
        results_ref[:, :, at] = spread.reshape(results_ref.shape[0], results_ref.shape[1], COLUMNS)
        return carried

    lax.fori_loop(0, width // COLUMNS, step, 0)


def rest_outputs(rest, weights):
    half = rest.shape[0] // 2
    members = lax.axis_size("tp")
    gathered = [
        lax.all_gather(rest[start : start + half], "tp", axis=0, tiled=False) for start in (0, half)
    ]
    rows = jnp.concatenate(gathered, axis=1).reshape(members * rest.shape[0], rest.shape[1])
    (share,) = run_experts((rows,), weights)
    parts = lax.all_to_all(split_up(share, 0, members), "tp", split_axis=0, concat_axis=0, tiled=True)
    return jnp.sum(parts.astype(jnp.float32), axis=0).astype(jnp.bfloat16)


def expert_outputs(arrived, most, weights):
    experts, capacity, width = arrived.shape
    slots = experts * capacity
    half = jax.ShapeDtypeStruct((PACKED, width), jnp.bfloat16)
    rest_shape = jax.ShapeDtypeStruct((slots - 2 * PACKED, width), jnp.bfloat16)
    square = jax.ShapeDtypeStruct((slots, slots), jnp.bfloat16)
    first, second, rest, back = in_kernel(
        pack_kernel, (half, half, rest_shape, square), 16, 2 * slots * slots * width, arrived,
        scratch=[pltpu.VMEM((slots, width), jnp.bfloat16)],
    )
    below_first = along_tp(first, 1)
    above_second = along_tp(second, -1)
    below_second = along_tp(second, 1)
    above_first = along_tp(first, -1)
    far_first = along_tp(below_first, 1)
    far_second = along_tp(above_second, -1)
    own = run_experts((first, second), weights)
    near = run_experts((below_first, below_second, above_first, above_second), weights)
    direct_up = along_tp(near[3], 1)
    direct_down = along_tp(near[0], -1)
    far = run_experts((far_first, far_second), weights)
    relay_up = along_tp(far[0], 1)
    relay_down = along_tp(far[1], -1)
    both_up, both_down = in_kernel(
        relay_kernel, (half, half), 8, 4 * PACKED * width, near[2], relay_up, near[1], relay_down
    )
    both_up = along_tp(both_up, 1)
    both_down = along_tp(both_down, -1)
    rest_out = lax.cond(most > 2 * PACKED, lambda: rest_outputs(rest, weights), lambda: jnp.zeros_like(rest))
    return in_kernel(
        unpack_kernel, jax.ShapeDtypeStruct(arrived.shape, jnp.bfloat16), 16,
        2 * slots * slots * width, back, rest_out, own[0], both_up, direct_down, own[1], direct_up, both_down,
    )


def on_device(
    queries,
    keys,
    values,
    break_bias,
    residual,
    w_out,
    ffn_gain,
    pick_ids,
    pair_logit,
    w_gate,
    w_up,
    w_down,
    out_gain,
):
    position = lax.axis_index("sp")
    quarters = lax.axis_size("tp")
    quarter = lax.axis_index("tp")
    slice_rows = queries.shape[0] // quarters
    width = w_out.shape[1]
    experts = lax.axis_size("sp")
    capacity = max(2, (3 * slice_rows + experts - 1) // experts)
    routed = lax.dynamic_slice_in_dim(pick_ids, quarter * slice_rows, slice_rows, 0)
    flat_ids = routed.reshape(slice_rows * TOP)
    places = jnp.arange(slice_rows * TOP, dtype=jnp.int32)
    matches = (flat_ids[:, None] == flat_ids[None, :]) & (places[None, :] < places[:, None])
    ranks = jnp.sum(matches.astype(jnp.int32), axis=1)
    targets = (flat_ids * capacity + ranks).reshape(slice_rows, TOP)
    logits = lax.dynamic_slice_in_dim(pair_logit, quarter * slice_rows, slice_rows, 0)[:, None]

    place = position.reshape(1).astype(jnp.int32)
    head_out, most = attend(queries, keys, values, break_bias, pick_ids, place)
    partial = jnp.dot(head_out, w_out, preferred_element_type=jnp.float32).astype(jnp.bfloat16)
    parts = split_up(partial, 0, quarters)
    mixed = lax.all_to_all(parts, "tp", split_axis=0, concat_axis=0, tiled=True)
    slots = jax.ShapeDtypeStruct((experts, capacity, width), jnp.bfloat16)
    rows = jax.ShapeDtypeStruct((slice_rows, width), jnp.bfloat16)
    dispatch_flops = 2 * experts * capacity * slice_rows * width
    stream, outgoing = in_kernel(
        dispatch_kernel, (rows, slots), 16, dispatch_flops,
        mixed, residual, ffn_gain[None], targets.T,
    )
    arrived = lax.all_to_all(outgoing, "sp", split_axis=0, concat_axis=0, tiled=True)
    results = expert_outputs(arrived, most[0], (w_gate[0], w_up[0], w_down[0]))
    returned = lax.all_to_all(results, "sp", split_axis=0, concat_axis=0, tiled=True)
    return in_kernel(
        final_kernel, rows, 16, 2 * dispatch_flops,
        returned, targets, logits, stream, out_gain[None],
        scratch=[pltpu.VMEM((slice_rows, width), jnp.float32)],
    )


def solution(mesh):
    placed = (
        P("sp", "tp"),
        P("sp", "tp"),
        P("sp", "tp"),
        P("tp"),
        P(("sp", "tp"), None),
        P("tp", None),
        P(),
        P("sp", None),
        P("sp"),
        P("sp", None, "tp"),
        P("sp", None, "tp"),
        P("sp", "tp", None),
        P(),
    )

    return jax.shard_map(on_device, mesh=mesh, in_specs=placed, out_specs=P(("sp", "tp"), None), check_vma=False)
```

```python
import functools
import itertools

import jax
import jax.numpy as jnp
from jax import lax
from jax.experimental import pallas as pl
from jax.experimental.pallas import tpu as pltpu
from jax.sharding import PartitionSpec as P


HEAD = 128
TOP = 2
Z_SIZE = 8
X_SIZE = 4
CORES = 2
Z_PLANE = X_SIZE * CORES

epsilon = 1e-06


def split_up(shard, dim, peers):
    before, after = (shard.shape[:dim], shard.shape[dim + 1 :])
    return jnp.moveaxis(shard.reshape(*before, peers, -1, *after), dim, 0)


LOG2E = 1.4426950408889634
KEY_BLOCK = 256
PICK_ROWS = 8


def causal_visit(state, query_ref, kv_ref, bias_ref, later, block, first_query):
    outputs, used = state
    rows = query_ref.shape[0] // bias_ref.shape[0]
    heads = bias_ref.shape[0]
    factor = HEAD ** (-0.5) * LOG2E
    at_block = pl.ds(pl.multiple_of(block * KEY_BLOCK, KEY_BLOCK), KEY_BLOCK)
    keys = kv_ref[at_block, :HEAD]
    values = kv_ref[at_block, HEAD:]
    scores = lax.dot_general(
        query_ref[...], keys, (((1,), (1,)), ((), ())), preferred_element_type=jnp.float32
    )
    if first_query is not None:
        query_pos = first_query + lax.broadcasted_iota(jnp.int32, (rows, KEY_BLOCK), 0)
        key_pos = block * KEY_BLOCK + lax.broadcasted_iota(jnp.int32, (rows, KEY_BLOCK), 1)
        before = key_pos < query_pos
    breaks, leads = [], []
    for head in range(heads):
        z = scores[head * rows : (head + 1) * rows] * factor + bias_ref[head] * LOG2E
        log_term = jnp.log2(1.0 + jnp.exp2(-jnp.abs(z)))
        softplus = jnp.maximum(z, 0.0) + log_term
        leads.append(z - softplus)
        breaks.append(softplus if first_query is None else jnp.where(before, softplus, 0.0))
    behind = jnp.dot(
        jnp.concatenate([b.astype(jnp.bfloat16) for b in breaks], axis=0),
        later,
        preferred_element_type=jnp.float32,
    )
    weights = []
    for head in range(heads):
        at = slice(head * rows, (head + 1) * rows)
        past = behind[at]
        gone = used[at]
        weight = jnp.exp2(leads[head] - past - jnp.concatenate([gone, gone], axis=1))
        if first_query is not None:
            weight = jnp.where(before, weight, 0.0)
        weights.append(weight.astype(jnp.bfloat16))
        used[at] = gone + jnp.broadcast_to(past[:, :1] + breaks[head][:, :1], gone.shape)
    outputs[...] += jnp.dot(
        jnp.concatenate(weights, axis=0), values, preferred_element_type=jnp.float32
    )


def later_keys():
    return (
        lax.broadcasted_iota(jnp.int32, (KEY_BLOCK, KEY_BLOCK), 0)
        > lax.broadcasted_iota(jnp.int32, (KEY_BLOCK, KEY_BLOCK), 1)
    ).astype(jnp.float32).astype(jnp.bfloat16)


def lay_out(own_ref, twin_ref, plane, place):
    core = place % CORES
    length = own_ref.shape[1] - PICK_ROWS
    for lane in range(X_SIZE):
        first = lane * CORES * length
        plane[pl.ds(pl.multiple_of(first + core * length, length), length)] = own_ref[lane, :length]
        plane[pl.ds(pl.multiple_of(first + (1 - core) * length, length), length)] = twin_ref[lane, :length]


def tally(counts, *pieces):
    expert = lax.broadcasted_iota(jnp.int32, counts.shape, 0).astype(jnp.float32)
    found = counts[...]
    for piece in pieces:
        length = piece.shape[1] - PICK_ROWS
        for block in range(piece.shape[0]):
            picks = piece[block, length:].astype(jnp.float32)[0:1]
            found = found + (picks == expert).astype(jnp.float32)
    counts[...] = found


def own_plane_kernel(place_ref, bias_ref, query_ref, blocks_ref, near, near_used, far, counts, plane):
    place = place_ref[0]
    rows = query_ref.shape[0] // bias_ref.shape[0]
    for block in range(Z_PLANE):
        plane[block * rows : (block + 1) * rows] = blocks_ref[block, :rows]
    for ref in (near, near_used, far, counts):
        ref[...] = jnp.zeros_like(ref)
    tally(counts, blocks_ref)
    later = later_keys()
    first_query = (place % (X_SIZE * CORES)) * rows
    last = (first_query + rows - 1) // KEY_BLOCK

    def step(index, carried):
        causal_visit((near, near_used), query_ref, plane, bias_ref, later, last - index, first_query)
        return carried

    lax.fori_loop(0, last + 1, step, 0)


def whole_plane(state, query_ref, plane, bias_ref):
    later = later_keys()
    blocks = plane.shape[0] // KEY_BLOCK

    def step(index, carried):
        causal_visit(state, query_ref, plane, bias_ref, later, blocks - 1 - 2 * index, None)
        causal_visit(state, query_ref, plane, bias_ref, later, blocks - 2 - 2 * index, None)
        return carried

    lax.fori_loop(0, blocks // 2, step, 0)


def two_planes_kernel(distance, place_ref, bias_ref, query_ref, below, above, twins,
                      near_in, near_used_in, far_in, counts_in, near, near_used, far, counts,
                      planes, found, found_used):
    place = place_ref[0]
    tally(counts, below, above, twins)
    level = place // (X_SIZE * CORES)
    lay_out(below, twins.at[:X_SIZE], planes.at[0], place)
    lay_out(above, twins.at[X_SIZE:], planes.at[1], place)

    def visit(side, carried):
        found[...] = jnp.zeros_like(found)
        found_used[...] = jnp.zeros_like(found_used)
        whole_plane((found, found_used), query_ref, planes.at[side], bias_ref)

        @pl.when(side == 0)
        def _():
            near[...] += jnp.exp2(-near_used[...]) * found[...]
            near_used[...] += found_used[...]

        @pl.when(side == 1)
        def _():
            far[...] = found[...] + jnp.exp2(-found_used[...]) * far[...]

        return carried

    first = jnp.where(level >= distance, 0, 1)
    past = jnp.where(level + distance >= Z_SIZE, 2, 1)
    lax.fori_loop(first, past, visit, 0)


def last_plane_kernel(distance, place_ref, bias_ref, query_ref, below, below_twin,
                      near_in, near_used_in, far_in, counts_in, out_ref, most_ref, plane, near, near_used, counts):
    place = place_ref[0]
    counts[...] = counts_in[...]
    tally(counts, below, below_twin)
    quarter = counts.shape[1] // 4
    lane = lax.broadcasted_iota(jnp.int32, counts.shape, 1) // quarter
    most = jnp.zeros((counts.shape[0], 1), jnp.float32)
    for member in range(4):
        named = jnp.sum(jnp.where(lane == member, counts[...], 0.0), axis=1, keepdims=True)
        most = jnp.maximum(most, named)
    most_ref[0] = jnp.max(most).astype(jnp.int32)
    near[...] = near_in[...]
    near_used[...] = near_used_in[...]

    @pl.when(place // (X_SIZE * CORES) >= distance)
    def _():
        lay_out(below, below_twin, plane, place)
        whole_plane((near, near_used), query_ref, plane, bias_ref)

    rows = out_ref.shape[0]
    for head in range(bias_ref.shape[0]):
        at = slice(head * rows, (head + 1) * rows)
        output = near[at] + jnp.exp2(-near_used[at]) * far_in[at]
        scaled = output * lax.rsqrt(jnp.mean(output * output, axis=-1, keepdims=True) + epsilon)
        out_ref[:, head * HEAD : (head + 1) * HEAD] = scaled.astype(jnp.bfloat16)


def attention_call(kernel, name, planes, position, break_bias, stacked, key_values, state, rows):
    stack = stacked.shape[0]
    in_vmem = pl.BlockSpec(memory_space=pltpu.VMEM)
    in_smem = pl.BlockSpec(memory_space=pltpu.SMEM)
    plane = (Z_PLANE * rows, 2 * HEAD)
    running = pltpu.VMEM((stack, HEAD), jnp.float32)
    kept = jax.ShapeDtypeStruct((stack, HEAD), jnp.float32)
    counts = (Z_SIZE * Z_PLANE, rows * TOP)
    last = name == "attend_last"
    keys = planes * Z_PLANE * rows
    first_state = 3 + len(key_values)
    heads = jax.ShapeDtypeStruct((rows, stack // rows * HEAD), jnp.bfloat16)
    return pl.pallas_call(
        kernel,
        out_shape=(heads, jax.ShapeDtypeStruct((1,), jnp.int32))
        if last
        else (kept,) * 3 + (jax.ShapeDtypeStruct(counts, jnp.float32),),
        in_specs=[in_smem, in_smem] + [in_vmem] * (1 + len(key_values) + len(state)),
        out_specs=(in_vmem, in_smem) if last else (in_vmem,) * 4,
        scratch_shapes=[pltpu.VMEM(plane if planes == 1 else (planes, *plane), jnp.bfloat16)]
        + ([running, running] if state else [])
        + ([pltpu.VMEM(counts, jnp.float32)] if last else []),
        input_output_aliases={} if last or not state else {first_state + i: i for i in range(4)},
        cost_estimate=pl.CostEstimate(
            flops=2 * stack * keys * (2 * HEAD + KEY_BLOCK), transcendentals=3 * stack * keys, bytes_accessed=0
        ),
        compiler_params=pltpu.CompilerParams(vmem_limit_bytes=24 * 1024 * 1024),
    )(position, break_bias, stacked, *key_values, *state)


def moved(shard, step_z, step_x, swap):
    pairs = []
    for place in range(Z_SIZE * Z_PLANE):
        z, x, core = place // Z_PLANE, place // CORES % X_SIZE, place % CORES
        target = ((z + step_z) % Z_SIZE * X_SIZE + (x + step_x) % X_SIZE) * CORES + (core ^ swap)
        pairs.append((place, target))
    return lax.ppermute(shard, "sp", pairs)


def attend(queries, keys, values, break_bias, pick_ids, position):
    rows = queries.shape[0]
    heads = queries.shape[1] // HEAD
    stacked = jnp.concatenate([queries[:, h * HEAD : (h + 1) * HEAD] for h in range(heads)], axis=0)
    picks = pick_ids.astype(jnp.bfloat16).reshape(1, rows * TOP)
    picks = jnp.concatenate([picks, jnp.zeros((PICK_ROWS - 1, rows * TOP), jnp.bfloat16)], axis=0)
    block = jnp.concatenate([jnp.concatenate([keys, values], axis=1), picks], axis=0)
    groups = [[z * Z_PLANE + w for w in range(Z_PLANE)] for z in range(Z_SIZE)]
    copies = jnp.broadcast_to(block[None], (Z_PLANE, *block.shape))
    blocks = lax.all_to_all(copies, "sp", 0, 0, axis_index_groups=groups, tiled=True)
    by_core = blocks.reshape(X_SIZE, CORES, *block.shape)
    own = lax.dynamic_index_in_dim(by_core, position[0] % CORES, 1, keepdims=False)
    common = (position, break_bias, stacked)
    below, above = own, own
    arrived = []
    for distance in range(1, Z_SIZE // 2 + 1):
        below = moved(below, 1, 0, 0)
        if distance < Z_SIZE // 2:
            above = moved(above, -1, 0, 0)
            both = jnp.concatenate([below, above], axis=0)
            arrived.append((below, above, moved(both, 0, 0, 1)))
        else:
            arrived.append((below, moved(below, 0, 0, 1)))
    state = attention_call(own_plane_kernel, "attend_0", 1, *common, (blocks,), (), rows)
    for distance in range(1, Z_SIZE // 2):
        kernel = functools.partial(two_planes_kernel, distance)
        name = f"attend_{distance}"
        state = attention_call(kernel, name, 2, *common, arrived[distance - 1], state, rows)
    kernel = functools.partial(last_plane_kernel, Z_SIZE // 2)
    return attention_call(kernel, "attend_last", 1, *common, arrived[-1], state, rows)


COLUMNS = 1024
PACKED = (48, 40)


def in_kernel(kernel, out_shapes, megabytes, flops, *operands, scratch=()):
    spec = pl.BlockSpec(memory_space=pltpu.VMEM)
    several = isinstance(out_shapes, tuple)
    return pl.pallas_call(
        kernel,
        out_shape=out_shapes,
        in_specs=[spec] * len(operands),
        out_specs=(spec,) * len(out_shapes) if several else spec,
        scratch_shapes=list(scratch),
        cost_estimate=pl.CostEstimate(flops=flops, transcendentals=0, bytes_accessed=0),
        compiler_params=pltpu.CompilerParams(vmem_limit_bytes=megabytes * 1024 * 1024),
    )(*operands)


def over_columns(width, step, carried, unrolled=False):
    if unrolled:
        for start in range(0, width, COLUMNS):
            carried = step(slice(start, start + COLUMNS), carried)
        return carried

    def at_column(index, carried):
        return step(pl.ds(pl.multiple_of(index * COLUMNS, COLUMNS), COLUMNS), carried)

    return lax.fori_loop(0, width // COLUMNS, at_column, carried)


def dispatch_kernel(mixed_ref, residual_ref, gain_ref, targets_ref, stream_ref, outgoing_ref):
    rows, width = residual_ref.shape
    experts, capacity = outgoing_ref.shape[:2]

    def add(at, total):
        mixed = mixed_ref[0, :, at].astype(jnp.float32)
        for member in range(1, mixed_ref.shape[0]):
            mixed = mixed + mixed_ref[member, :, at].astype(jnp.float32)
        stream = (residual_ref[:, at].astype(jnp.float32) + mixed).astype(jnp.bfloat16)
        stream_ref[:, at] = stream
        wide = stream.astype(jnp.float32)
        return total + jnp.sum(wide * wide, axis=1, keepdims=True)

    total = over_columns(width, add, jnp.zeros((rows, 1), jnp.float32), True)
    scale = lax.rsqrt(total / width + epsilon)
    slot = lax.broadcasted_iota(jnp.int32, (experts * capacity, rows), 0)
    chosen = (slot == targets_ref[0:1, :]) | (slot == targets_ref[1:2, :])
    chosen = chosen.astype(jnp.float32).astype(jnp.bfloat16)

    def send(at, carried):
        normed = (stream_ref[:, at].astype(jnp.float32) * scale * gain_ref[:, at]).astype(jnp.bfloat16)
        sent = jnp.dot(chosen, normed, preferred_element_type=jnp.float32).astype(jnp.bfloat16)
        outgoing_ref[:, :, at] = sent.reshape(experts, capacity, COLUMNS)
        return carried

    over_columns(width, send, 0, True)


def pack_kernel(arrived_ref, first_ref, second_ref, rest_ref, back_ref, entries):
    slots = arrived_ref.shape[0] * arrived_ref.shape[1]
    width = arrived_ref.shape[2]

    def read(at, largest):
        part = arrived_ref[:, :, at].reshape(slots, COLUMNS)
        entries[:, at] = part
        size = jnp.abs(part.astype(jnp.float32))
        for lane in range(0, COLUMNS, 128):
            largest = jnp.maximum(largest, size[:, lane : lane + 128])
        return largest

    largest = over_columns(width, read, jnp.zeros((slots, 128), jnp.float32))
    held = (jnp.max(largest, axis=1, keepdims=True) > 0).astype(jnp.float32)
    row = lax.broadcasted_iota(jnp.int32, (slots, slots), 0)
    column = lax.broadcasted_iota(jnp.int32, (slots, slots), 1)

    def product(left, right):
        left, right = left.astype(jnp.float32), right.astype(jnp.float32)
        return jnp.dot(
            left.astype(jnp.bfloat16), right.astype(jnp.bfloat16), preferred_element_type=jnp.float32
        )

    held_rows = jnp.broadcast_to(held, (slots, slots))
    held_columns = product(jnp.ones((slots, slots), jnp.float32), jnp.where(row == column, held_rows, 0.0))
    place_rows = product(column < row, held_rows)
    place_columns = product(held_columns, row < column)
    back = ((place_rows == column.astype(jnp.float32)) & (held_rows > 0)).astype(jnp.float32)
    back_ref[...] = back.astype(jnp.bfloat16)
    forth = ((place_columns == row.astype(jnp.float32)) & (held_columns > 0)).astype(jnp.float32)
    forth = forth.astype(jnp.bfloat16)
    half, both = first_ref.shape[0], first_ref.shape[0] + second_ref.shape[0]

    def write(at, carried):
        packed = jnp.dot(forth, entries[:, at], preferred_element_type=jnp.float32).astype(jnp.bfloat16)
        first_ref[:, at] = packed[:half]
        second_ref[:, at] = packed[half:both]
        rest_ref[:, at] = packed[both:]
        return carried

    over_columns(width, write, 0)


def expert_kernel(*refs):
    count = (len(refs) - 6) // 2
    inputs, outs = refs[:count], refs[count + 3 : -3]
    gate_ref, up_ref, down_ref = refs[count : count + 3]
    entries, gate, up = refs[-3:]
    width = inputs[0].shape[1]
    ends = list(itertools.accumulate(source.shape[0] for source in inputs))
    for source, end in zip(inputs, ends):
        entries[end - source.shape[0] : end] = source[...]
    gate[...] = jnp.zeros_like(gate)
    up[...] = jnp.zeros_like(up)

    def rise(index, carried):
        at = pl.ds(pl.multiple_of(index * COLUMNS, COLUMNS), COLUMNS)
        part = entries[:, at]
        gate[...] += jnp.dot(part, gate_ref[at, :], preferred_element_type=jnp.float32)
        up[...] += jnp.dot(part, up_ref[at, :], preferred_element_type=jnp.float32)
        return carried

    lax.fori_loop(0, width // COLUMNS, rise, 0)
    hidden = (gate[...] / (1.0 + jnp.exp(-gate[...])) * up[...]).astype(jnp.bfloat16)

    def fall(index, carried):
        at = pl.ds(pl.multiple_of(index * COLUMNS, COLUMNS), COLUMNS)
        share = jnp.dot(hidden, down_ref[:, at], preferred_element_type=jnp.float32).astype(jnp.bfloat16)
        for out, end in zip(outs, ends):
            out[:, at] = share[end - out.shape[0] : end]
        return carried

    lax.fori_loop(0, width // COLUMNS, fall, 0)


def run_experts(pieces, weights):
    shapes = tuple(jax.ShapeDtypeStruct(piece.shape, jnp.bfloat16) for piece in pieces)
    slots = sum(piece.shape[0] for piece in pieces)
    width, units = weights[0].shape
    flops = 6 * slots * width * units
    scratch = [pltpu.VMEM((slots, width), jnp.bfloat16)] + [pltpu.VMEM((slots, units), jnp.float32)] * 2
    return in_kernel(expert_kernel, shapes, 32, flops, *pieces, *weights, scratch=scratch)


def final_kernel(returned_ref, targets_ref, logits_ref, stream_ref, gain_ref, out_ref, blended):
    rows, width = stream_ref.shape
    slots = returned_ref.shape[0] * returned_ref.shape[1]
    slot = lax.broadcasted_iota(jnp.int32, (rows, slots), 1)
    picks = [
        (slot == targets_ref[:, pick : pick + 1]).astype(jnp.float32).astype(jnp.bfloat16) for pick in range(TOP)
    ]
    logits = logits_ref[...]
    shares = (1.0 / (1.0 + jnp.exp(-logits)), 1.0 / (1.0 + jnp.exp(logits)))

    def mix(at, total):
        entries = returned_ref[:, :, at].reshape(slots, COLUMNS)
        both = shares[0] * jnp.dot(picks[0], entries, preferred_element_type=jnp.float32)
        both = both + shares[1] * jnp.dot(picks[1], entries, preferred_element_type=jnp.float32)
        blended[:, at] = both
        return total + jnp.sum(both * both, axis=1, keepdims=True)

    total = over_columns(width, mix, jnp.zeros((rows, 1), jnp.float32), True)
    scale = lax.rsqrt(total / width + epsilon)

    def add(at, carried):
        wide = stream_ref[:, at].astype(jnp.float32)
        out_ref[:, at] = (wide + blended[:, at] * scale * gain_ref[:, at]).astype(jnp.bfloat16)
        return carried

    over_columns(width, add, 0, True)


def along_tp(shard, step):
    size = lax.axis_size("tp")
    return lax.ppermute(shard, "tp", [(member, (member + step) % size) for member in range(size)])


def relay_kernel(own_up, far_up, own_down, far_down, up_ref, down_ref):
    for own, far, out in ((own_up, far_up, up_ref), (own_down, far_down, down_ref)):

        def step(index, carried):
            at = pl.ds(pl.multiple_of(index * COLUMNS, COLUMNS), COLUMNS)
            out[:, at] = (own[:, at].astype(jnp.float32) + far[:, at].astype(jnp.float32)).astype(jnp.bfloat16)
            return carried

        lax.fori_loop(0, out.shape[1] // COLUMNS, step, 0)


def unpack_kernel(back_ref, rest_ref, *refs):
    firsts, seconds, results_ref = refs[:3], refs[3:6], refs[6]
    width = firsts[0].shape[1]

    def step(index, carried):
        at = pl.ds(pl.multiple_of(index * COLUMNS, COLUMNS), COLUMNS)
        sums = []
        for parts in (firsts, seconds):
            total = parts[0][:, at].astype(jnp.float32)
            for part in parts[1:]:
                total = total + part[:, at].astype(jnp.float32)
            sums.append(total.astype(jnp.bfloat16))
        packed = jnp.concatenate(sums + [rest_ref[:, at]], axis=0)
        spread = jnp.dot(back_ref[...], packed, preferred_element_type=jnp.float32).astype(jnp.bfloat16)
        results_ref[:, :, at] = spread.reshape(results_ref.shape[0], results_ref.shape[1], COLUMNS)
        return carried

    lax.fori_loop(0, width // COLUMNS, step, 0)


def rest_outputs(rest, weights):
    members = lax.axis_size("tp")
    copies = jnp.broadcast_to(rest[None], (members, *rest.shape))
    rows = lax.all_to_all(copies, "tp", split_axis=0, concat_axis=0, tiled=True).reshape(-1, rest.shape[1])
    (share,) = run_experts((rows,), weights)
    parts = lax.all_to_all(split_up(share, 0, members), "tp", split_axis=0, concat_axis=0, tiled=True)
    return jnp.sum(parts.astype(jnp.float32), axis=0).astype(jnp.bfloat16)


def expert_outputs(arrived, most, weights):
    experts, capacity, width = arrived.shape
    slots = experts * capacity
    half, other = (jax.ShapeDtypeStruct((count, width), jnp.bfloat16) for count in PACKED)
    rest_shape = jax.ShapeDtypeStruct((slots - sum(PACKED), width), jnp.bfloat16)
    square = jax.ShapeDtypeStruct((slots, slots), jnp.bfloat16)
    first, second, rest, back = in_kernel(
        pack_kernel, (half, other, rest_shape, square), 16, 2 * slots * slots * width, arrived,
        scratch=[pltpu.VMEM((slots, width), jnp.bfloat16)],
    )
    below_first = along_tp(first, 1)
    above_second = along_tp(second, -1)
    below_second = along_tp(second, 1)
    above_first = along_tp(first, -1)
    far_first = along_tp(below_first, 1)
    far_second = along_tp(above_second, -1)
    own = run_experts((first, second), weights)
    near = run_experts((below_first, below_second, above_first, above_second), weights)
    direct_up = along_tp(near[3], 1)
    direct_down = along_tp(near[0], -1)
    far = run_experts((far_first, far_second), weights)
    relay_up = along_tp(far[0], 1)
    relay_down = along_tp(far[1], -1)
    both_up, both_down = in_kernel(
        relay_kernel, (half, other), 8, 2 * sum(PACKED) * width, near[2], relay_up, near[1], relay_down
    )
    both_up = along_tp(both_up, 1)
    both_down = along_tp(both_down, -1)
    rest_out = lax.cond(most > sum(PACKED), lambda: rest_outputs(rest, weights), lambda: jnp.zeros_like(rest))
    return in_kernel(
        unpack_kernel, jax.ShapeDtypeStruct(arrived.shape, jnp.bfloat16), 16,
        2 * slots * slots * width, back, rest_out, own[0], both_up, direct_down, own[1], direct_up, both_down,
    )


def on_device(
    queries,
    keys,
    values,
    break_bias,
    residual,
    w_out,
    ffn_gain,
    pick_ids,
    pair_logit,
    w_gate,
    w_up,
    w_down,
    out_gain,
):
    position = lax.axis_index("sp")
    quarters = lax.axis_size("tp")
    quarter = lax.axis_index("tp")
    slice_rows = queries.shape[0] // quarters
    width = w_out.shape[1]
    experts = lax.axis_size("sp")
    capacity = max(2, (3 * slice_rows + experts - 1) // experts)
    routed = lax.dynamic_slice_in_dim(pick_ids, quarter * slice_rows, slice_rows, 0)
    flat_ids = routed.reshape(slice_rows * TOP)
    places = jnp.arange(slice_rows * TOP, dtype=jnp.int32)
    matches = (flat_ids[:, None] == flat_ids[None, :]) & (places[None, :] < places[:, None])
    ranks = jnp.sum(matches.astype(jnp.int32), axis=1)
    targets = (flat_ids * capacity + ranks).reshape(slice_rows, TOP)
    logits = lax.dynamic_slice_in_dim(pair_logit, quarter * slice_rows, slice_rows, 0)[:, None]

    place = position.reshape(1).astype(jnp.int32)
    head_out, most = attend(queries, keys, values, break_bias, pick_ids, place)
    partial = jnp.dot(head_out, w_out, preferred_element_type=jnp.float32).astype(jnp.bfloat16)
    parts = split_up(partial, 0, quarters)
    mixed = lax.all_to_all(parts, "tp", split_axis=0, concat_axis=0, tiled=True)
    slots = jax.ShapeDtypeStruct((experts, capacity, width), jnp.bfloat16)
    rows = jax.ShapeDtypeStruct((slice_rows, width), jnp.bfloat16)
    dispatch_flops = 2 * experts * capacity * slice_rows * width
    stream, outgoing = in_kernel(
        dispatch_kernel, (rows, slots), 16, dispatch_flops,
        mixed, residual, ffn_gain[None], targets.T,
    )
    arrived = lax.all_to_all(outgoing, "sp", split_axis=0, concat_axis=0, tiled=True)
    results = expert_outputs(arrived, most[0], (w_gate[0], w_up[0], w_down[0]))
    returned = lax.all_to_all(results, "sp", split_axis=0, concat_axis=0, tiled=True)
    return in_kernel(
        final_kernel, rows, 16, 2 * dispatch_flops,
        returned, targets, logits, stream, out_gain[None],
        scratch=[pltpu.VMEM((slice_rows, width), jnp.float32)],
    )


def solution(mesh):
    placed = (
        P("sp", "tp"),
        P("sp", "tp"),
        P("sp", "tp"),
        P("tp"),
        P(("sp", "tp"), None),
        P("tp", None),
        P(),
        P("sp", None),
        P("sp"),
        P("sp", None, "tp"),
        P("sp", None, "tp"),
        P("sp", "tp", None),
        P(),
    )

    return jax.shard_map(on_device, mesh=mesh, in_specs=placed, out_specs=P(("sp", "tp"), None), check_vma=False)
```

```python
import functools
import itertools

import jax
import jax.numpy as jnp
from jax import lax
from jax.experimental import pallas as pl
from jax.experimental.pallas import tpu as pltpu
from jax.sharding import PartitionSpec as P


HEAD = 128
TOP = 2
Z_SIZE = 8
X_SIZE = 4
CORES = 2
Z_PLANE = X_SIZE * CORES

epsilon = 1e-06


def split_up(shard, dim, peers):
    before, after = (shard.shape[:dim], shard.shape[dim + 1 :])
    return jnp.moveaxis(shard.reshape(*before, peers, -1, *after), dim, 0)


LOG2E = 1.4426950408889634
KEY_BLOCK = 256
MOST = 100.0
PICK_ROWS = 8


def causal_visit(state, query_ref, kv_ref, bias_ref, later, block, first_query):
    outputs, used = state
    rows = query_ref.shape[0] // bias_ref.shape[0]
    heads = bias_ref.shape[0]
    factor = HEAD ** (-0.5) * LOG2E
    at_block = pl.ds(pl.multiple_of(block * KEY_BLOCK, KEY_BLOCK), KEY_BLOCK)
    keys = kv_ref[at_block, :HEAD]
    values = kv_ref[at_block, HEAD:]
    scores = lax.dot_general(
        query_ref[...], keys, (((1,), (1,)), ((), ())), preferred_element_type=jnp.float32
    )
    if first_query is not None:
        query_pos = first_query + lax.broadcasted_iota(jnp.int32, (rows, KEY_BLOCK), 0)
        key_pos = block * KEY_BLOCK + lax.broadcasted_iota(jnp.int32, (rows, KEY_BLOCK), 1)
        before = key_pos < query_pos
    breaks, leads = [], []
    for head in range(heads):
        z = scores[head * rows : (head + 1) * rows] * factor + bias_ref[head] * LOG2E
        softplus = jnp.maximum(jnp.log2(1.0 + jnp.exp2(jnp.minimum(z, MOST))), z)
        leads.append(z - softplus)
        breaks.append(softplus if first_query is None else jnp.where(before, softplus, 0.0))
    behind = jnp.dot(
        jnp.concatenate([b.astype(jnp.bfloat16) for b in breaks], axis=0),
        later,
        preferred_element_type=jnp.float32,
    )
    weights = []
    for head in range(heads):
        at = slice(head * rows, (head + 1) * rows)
        past = behind[at]
        gone = used[at]
        weight = jnp.exp2(leads[head] - past - jnp.concatenate([gone, gone], axis=1))
        if first_query is not None:
            weight = jnp.where(before, weight, 0.0)
        weights.append(weight.astype(jnp.bfloat16))
        used[at] = gone + jnp.broadcast_to(past[:, :1] + breaks[head][:, :1], gone.shape)
    outputs[...] += jnp.dot(
        jnp.concatenate(weights, axis=0), values, preferred_element_type=jnp.float32
    )


def later_keys():
    return (
        lax.broadcasted_iota(jnp.int32, (KEY_BLOCK, KEY_BLOCK), 0)
        > lax.broadcasted_iota(jnp.int32, (KEY_BLOCK, KEY_BLOCK), 1)
    ).astype(jnp.float32).astype(jnp.bfloat16)


def lay_out(own_ref, twin_ref, plane, place):
    lanes = (place // CORES) % X_SIZE
    core = place % CORES
    length = own_ref.shape[1] - PICK_ROWS
    for shift in range(X_SIZE):
        source = ((lanes + X_SIZE - shift) % X_SIZE) * CORES
        plane[pl.ds(pl.multiple_of((source + core) * length, length), length)] = own_ref[shift, :length]
        plane[pl.ds(pl.multiple_of((source + 1 - core) * length, length), length)] = twin_ref[shift, :length]


def tally(counts, *pieces):
    expert = lax.broadcasted_iota(jnp.int32, counts.shape, 0).astype(jnp.float32)
    found = counts[...]
    for piece in pieces:
        length = piece.shape[1] - PICK_ROWS
        for block in range(piece.shape[0]):
            picks = piece[block, length:].astype(jnp.float32)[0:1]
            found = found + (picks == expert).astype(jnp.float32)
    counts[...] = found


def own_plane_kernel(place_ref, bias_ref, query_ref, own_ref, twin_ref, near, near_used, far, counts, plane):
    place = place_ref[0]
    lay_out(own_ref, twin_ref, plane, place)
    for ref in (near, near_used, far, counts):
        ref[...] = jnp.zeros_like(ref)
    tally(counts, own_ref, twin_ref)
    later = later_keys()
    rows = query_ref.shape[0] // bias_ref.shape[0]
    first_query = (place % (X_SIZE * CORES)) * rows
    last = (first_query + rows - 1) // KEY_BLOCK

    def step(index, carried):
        causal_visit((near, near_used), query_ref, plane, bias_ref, later, last - index, first_query)
        return carried

    lax.fori_loop(0, last + 1, step, 0)


def whole_plane(state, query_ref, plane, bias_ref):
    later = later_keys()
    blocks = plane.shape[0] // KEY_BLOCK

    def step(index, carried):
        causal_visit(state, query_ref, plane, bias_ref, later, blocks - 1 - 2 * index, None)
        causal_visit(state, query_ref, plane, bias_ref, later, blocks - 2 - 2 * index, None)
        return carried

    lax.fori_loop(0, blocks // 2, step, 0)


def two_planes_kernel(distance, place_ref, bias_ref, query_ref, below, above, twins,
                      near_in, near_used_in, far_in, counts_in, near, near_used, far, counts,
                      planes, found, found_used):
    place = place_ref[0]
    tally(counts, below, above, twins)
    level = place // (X_SIZE * CORES)
    lay_out(below, twins.at[:X_SIZE], planes.at[0], place)
    lay_out(above, twins.at[X_SIZE:], planes.at[1], place)

    def visit(side, carried):
        found[...] = jnp.zeros_like(found)
        found_used[...] = jnp.zeros_like(found_used)
        whole_plane((found, found_used), query_ref, planes.at[side], bias_ref)

        @pl.when(side == 0)
        def _():
            near[...] += jnp.exp2(-near_used[...]) * found[...]
            near_used[...] += found_used[...]

        @pl.when(side == 1)
        def _():
            far[...] = found[...] + jnp.exp2(-found_used[...]) * far[...]

        return carried

    first = jnp.where(level >= distance, 0, 1)
    past = jnp.where(level + distance >= Z_SIZE, 2, 1)
    lax.fori_loop(first, past, visit, 0)


def last_plane_kernel(distance, place_ref, bias_ref, query_ref, below, below_twin,
                      near_in, near_used_in, far_in, counts_in, out_ref, most_ref, plane, near, near_used, counts):
    place = place_ref[0]
    counts[...] = counts_in[...]
    tally(counts, below, below_twin)
    quarter = counts.shape[1] // 4
    lane = lax.broadcasted_iota(jnp.int32, counts.shape, 1) // quarter
    most = jnp.zeros((counts.shape[0], 1), jnp.float32)
    for member in range(4):
        named = jnp.sum(jnp.where(lane == member, counts[...], 0.0), axis=1, keepdims=True)
        most = jnp.maximum(most, named)
    most_ref[0] = jnp.max(most).astype(jnp.int32)
    near[...] = near_in[...]
    near_used[...] = near_used_in[...]

    @pl.when(place // (X_SIZE * CORES) >= distance)
    def _():
        lay_out(below, below_twin, plane, place)
        whole_plane((near, near_used), query_ref, plane, bias_ref)

    rows = out_ref.shape[0]
    for head in range(bias_ref.shape[0]):
        at = slice(head * rows, (head + 1) * rows)
        output = near[at] + jnp.exp2(-near_used[at]) * far_in[at]
        scaled = output * lax.rsqrt(jnp.mean(output * output, axis=-1, keepdims=True) + epsilon)
        out_ref[:, head * HEAD : (head + 1) * HEAD] = scaled.astype(jnp.bfloat16)


def attention_call(kernel, name, planes, position, break_bias, stacked, key_values, state, rows):
    stack = stacked.shape[0]
    in_vmem = pl.BlockSpec(memory_space=pltpu.VMEM)
    in_smem = pl.BlockSpec(memory_space=pltpu.SMEM)
    plane = (Z_PLANE * rows, 2 * HEAD)
    running = pltpu.VMEM((stack, HEAD), jnp.float32)
    kept = jax.ShapeDtypeStruct((stack, HEAD), jnp.float32)
    counts = (Z_SIZE * Z_PLANE, rows * TOP)
    last = name == "attend_last"
    keys = planes * Z_PLANE * rows
    first_state = 3 + len(key_values)
    heads = jax.ShapeDtypeStruct((rows, stack // rows * HEAD), jnp.bfloat16)
    return pl.pallas_call(
        kernel,
        out_shape=(heads, jax.ShapeDtypeStruct((1,), jnp.int32))
        if last
        else (kept,) * 3 + (jax.ShapeDtypeStruct(counts, jnp.float32),),
        in_specs=[in_smem, in_smem] + [in_vmem] * (1 + len(key_values) + len(state)),
        out_specs=(in_vmem, in_smem) if last else (in_vmem,) * 4,
        scratch_shapes=[pltpu.VMEM(plane if planes == 1 else (planes, *plane), jnp.bfloat16)]
        + ([running, running] if state else [])
        + ([pltpu.VMEM(counts, jnp.float32)] if last else []),
        input_output_aliases={} if last or not state else {first_state + i: i for i in range(4)},
        cost_estimate=pl.CostEstimate(
            flops=2 * stack * keys * (2 * HEAD + KEY_BLOCK), transcendentals=3 * stack * keys, bytes_accessed=0
        ),
        compiler_params=pltpu.CompilerParams(vmem_limit_bytes=24 * 1024 * 1024),
    )(position, break_bias, stacked, *key_values, *state)


def moved(shard, step_z, step_x, swap):
    pairs = []
    for place in range(Z_SIZE * Z_PLANE):
        z, x, core = place // Z_PLANE, place // CORES % X_SIZE, place % CORES
        target = ((z + step_z) % Z_SIZE * X_SIZE + (x + step_x) % X_SIZE) * CORES + (core ^ swap)
        pairs.append((place, target))
    return lax.ppermute(shard, "sp", pairs)


def attend(queries, keys, values, break_bias, pick_ids, position):
    rows = queries.shape[0]
    heads = queries.shape[1] // HEAD
    stacked = jnp.concatenate([queries[:, h * HEAD : (h + 1) * HEAD] for h in range(heads)], axis=0)
    picks = pick_ids.astype(jnp.bfloat16).reshape(1, rows * TOP)
    picks = jnp.concatenate([picks, jnp.zeros((PICK_ROWS - 1, rows * TOP), jnp.bfloat16)], axis=0)
    block = jnp.concatenate([jnp.concatenate([keys, values], axis=1), picks], axis=0)
    own = jnp.stack([block] + [moved(block, 0, step, 0) for step in range(1, X_SIZE)])
    twin = moved(own, 0, 0, 1)
    common = (position, break_bias, stacked)
    below, above = own, own
    arrived = []
    for distance in range(1, Z_SIZE // 2 + 1):
        below = moved(below, 1, 0, 0)
        if distance < Z_SIZE // 2:
            above = moved(above, -1, 0, 0)
            both = jnp.concatenate([below, above], axis=0)
            arrived.append((below, above, moved(both, 0, 0, 1)))
        else:
            arrived.append((below, moved(below, 0, 0, 1)))
    state = attention_call(own_plane_kernel, "attend_0", 1, *common, (own, twin), (), rows)
    for distance in range(1, Z_SIZE // 2):
        kernel = functools.partial(two_planes_kernel, distance)
        name = f"attend_{distance}"
        state = attention_call(kernel, name, 2, *common, arrived[distance - 1], state, rows)
    kernel = functools.partial(last_plane_kernel, Z_SIZE // 2)
    return attention_call(kernel, "attend_last", 1, *common, arrived[-1], state, rows)


COLUMNS = 1024
PACKED = (48, 40)


def in_kernel(kernel, out_shapes, megabytes, flops, *operands, scratch=()):
    spec = pl.BlockSpec(memory_space=pltpu.VMEM)
    several = isinstance(out_shapes, tuple)
    return pl.pallas_call(
        kernel,
        out_shape=out_shapes,
        in_specs=[spec] * len(operands),
        out_specs=(spec,) * len(out_shapes) if several else spec,
        scratch_shapes=list(scratch),
        cost_estimate=pl.CostEstimate(flops=flops, transcendentals=0, bytes_accessed=0),
        compiler_params=pltpu.CompilerParams(vmem_limit_bytes=megabytes * 1024 * 1024),
    )(*operands)


def over_columns(width, step, carried, unrolled=False):
    if unrolled:
        for start in range(0, width, COLUMNS):
            carried = step(slice(start, start + COLUMNS), carried)
        return carried

    def at_column(index, carried):
        return step(pl.ds(pl.multiple_of(index * COLUMNS, COLUMNS), COLUMNS), carried)

    return lax.fori_loop(0, width // COLUMNS, at_column, carried)


def dispatch_kernel(mixed_ref, residual_ref, gain_ref, targets_ref, stream_ref, outgoing_ref):
    rows, width = residual_ref.shape
    experts, capacity = outgoing_ref.shape[:2]

    def add(at, total):
        mixed = mixed_ref[0, :, at].astype(jnp.float32)
        for member in range(1, mixed_ref.shape[0]):
            mixed = mixed + mixed_ref[member, :, at].astype(jnp.float32)
        stream = (residual_ref[:, at].astype(jnp.float32) + mixed).astype(jnp.bfloat16)
        stream_ref[:, at] = stream
        wide = stream.astype(jnp.float32)
        return total + jnp.sum(wide * wide, axis=1, keepdims=True)

    total = over_columns(width, add, jnp.zeros((rows, 1), jnp.float32), True)
    scale = lax.rsqrt(total / width + epsilon)
    slot = lax.broadcasted_iota(jnp.int32, (experts * capacity, rows), 0)
    chosen = (slot == targets_ref[0:1, :]) | (slot == targets_ref[1:2, :])
    chosen = chosen.astype(jnp.float32).astype(jnp.bfloat16)

    def send(at, carried):
        normed = (stream_ref[:, at].astype(jnp.float32) * scale * gain_ref[:, at]).astype(jnp.bfloat16)
        sent = jnp.dot(chosen, normed, preferred_element_type=jnp.float32).astype(jnp.bfloat16)
        outgoing_ref[:, :, at] = sent.reshape(experts, capacity, COLUMNS)
        return carried

    over_columns(width, send, 0, True)


def pack_kernel(arrived_ref, first_ref, second_ref, rest_ref, back_ref, entries):
    slots = arrived_ref.shape[0] * arrived_ref.shape[1]
    width = arrived_ref.shape[2]

    def read(at, largest):
        part = arrived_ref[:, :, at].reshape(slots, COLUMNS)
        entries[:, at] = part
        size = jnp.abs(part.astype(jnp.float32))
        for lane in range(0, COLUMNS, 128):
            largest = jnp.maximum(largest, size[:, lane : lane + 128])
        return largest

    largest = over_columns(width, read, jnp.zeros((slots, 128), jnp.float32))
    held = (jnp.max(largest, axis=1, keepdims=True) > 0).astype(jnp.float32)
    row = lax.broadcasted_iota(jnp.int32, (slots, slots), 0)
    column = lax.broadcasted_iota(jnp.int32, (slots, slots), 1)

    def product(left, right):
        left, right = left.astype(jnp.float32), right.astype(jnp.float32)
        return jnp.dot(
            left.astype(jnp.bfloat16), right.astype(jnp.bfloat16), preferred_element_type=jnp.float32
        )

    held_rows = jnp.broadcast_to(held, (slots, slots))
    held_columns = product(jnp.ones((slots, slots), jnp.float32), jnp.where(row == column, held_rows, 0.0))
    place_rows = product(column < row, held_rows)
    place_columns = product(held_columns, row < column)
    back = ((place_rows == column.astype(jnp.float32)) & (held_rows > 0)).astype(jnp.float32)
    back_ref[...] = back.astype(jnp.bfloat16)
    forth = ((place_columns == row.astype(jnp.float32)) & (held_columns > 0)).astype(jnp.float32)
    forth = forth.astype(jnp.bfloat16)
    half, both = first_ref.shape[0], first_ref.shape[0] + second_ref.shape[0]

    def write(at, carried):
        packed = jnp.dot(forth, entries[:, at], preferred_element_type=jnp.float32).astype(jnp.bfloat16)
        first_ref[:, at] = packed[:half]
        second_ref[:, at] = packed[half:both]
        rest_ref[:, at] = packed[both:]
        return carried

    over_columns(width, write, 0)


def expert_kernel(*refs):
    count = (len(refs) - 6) // 2
    inputs, outs = refs[:count], refs[count + 3 : -3]
    gate_ref, up_ref, down_ref = refs[count : count + 3]
    entries, gate, up = refs[-3:]
    width = inputs[0].shape[1]
    ends = list(itertools.accumulate(source.shape[0] for source in inputs))
    for source, end in zip(inputs, ends):
        entries[end - source.shape[0] : end] = source[...]
    gate[...] = jnp.zeros_like(gate)
    up[...] = jnp.zeros_like(up)

    def rise(index, carried):
        at = pl.ds(pl.multiple_of(index * COLUMNS, COLUMNS), COLUMNS)
        part = entries[:, at]
        gate[...] += jnp.dot(part, gate_ref[at, :], preferred_element_type=jnp.float32)
        up[...] += jnp.dot(part, up_ref[at, :], preferred_element_type=jnp.float32)
        return carried

    lax.fori_loop(0, width // COLUMNS, rise, 0)
    hidden = (gate[...] / (1.0 + jnp.exp(-gate[...])) * up[...]).astype(jnp.bfloat16)

    def fall(index, carried):
        at = pl.ds(pl.multiple_of(index * COLUMNS, COLUMNS), COLUMNS)
        share = jnp.dot(hidden, down_ref[:, at], preferred_element_type=jnp.float32).astype(jnp.bfloat16)
        for out, end in zip(outs, ends):
            out[:, at] = share[end - out.shape[0] : end]
        return carried

    lax.fori_loop(0, width // COLUMNS, fall, 0)


def run_experts(pieces, weights):
    shapes = tuple(jax.ShapeDtypeStruct(piece.shape, jnp.bfloat16) for piece in pieces)
    slots = sum(piece.shape[0] for piece in pieces)
    width, units = weights[0].shape
    flops = 6 * slots * width * units
    scratch = [pltpu.VMEM((slots, width), jnp.bfloat16)] + [pltpu.VMEM((slots, units), jnp.float32)] * 2
    return in_kernel(expert_kernel, shapes, 32, flops, *pieces, *weights, scratch=scratch)


def final_kernel(returned_ref, targets_ref, logits_ref, stream_ref, gain_ref, out_ref, blended):
    rows, width = stream_ref.shape
    slots = returned_ref.shape[0] * returned_ref.shape[1]
    slot = lax.broadcasted_iota(jnp.int32, (rows, slots), 1)
    picks = [
        (slot == targets_ref[:, pick : pick + 1]).astype(jnp.float32).astype(jnp.bfloat16) for pick in range(TOP)
    ]
    logits = logits_ref[...]
    shares = (1.0 / (1.0 + jnp.exp(-logits)), 1.0 / (1.0 + jnp.exp(logits)))

    def mix(at, total):
        entries = returned_ref[:, :, at].reshape(slots, COLUMNS)
        both = shares[0] * jnp.dot(picks[0], entries, preferred_element_type=jnp.float32)
        both = both + shares[1] * jnp.dot(picks[1], entries, preferred_element_type=jnp.float32)
        blended[:, at] = both
        return total + jnp.sum(both * both, axis=1, keepdims=True)

    total = over_columns(width, mix, jnp.zeros((rows, 1), jnp.float32), True)
    scale = lax.rsqrt(total / width + epsilon)

    def add(at, carried):
        wide = stream_ref[:, at].astype(jnp.float32)
        out_ref[:, at] = (wide + blended[:, at] * scale * gain_ref[:, at]).astype(jnp.bfloat16)
        return carried

    over_columns(width, add, 0, True)


def along_tp(shard, step):
    size = lax.axis_size("tp")
    return lax.ppermute(shard, "tp", [(member, (member + step) % size) for member in range(size)])


def relay_kernel(own_up, far_up, own_down, far_down, up_ref, down_ref):
    for own, far, out in ((own_up, far_up, up_ref), (own_down, far_down, down_ref)):

        def step(index, carried):
            at = pl.ds(pl.multiple_of(index * COLUMNS, COLUMNS), COLUMNS)
            out[:, at] = (own[:, at].astype(jnp.float32) + far[:, at].astype(jnp.float32)).astype(jnp.bfloat16)
            return carried

        lax.fori_loop(0, out.shape[1] // COLUMNS, step, 0)


def unpack_kernel(back_ref, rest_ref, *refs):
    firsts, seconds, results_ref = refs[:3], refs[3:6], refs[6]
    width = firsts[0].shape[1]

    def step(index, carried):
        at = pl.ds(pl.multiple_of(index * COLUMNS, COLUMNS), COLUMNS)
        sums = []
        for parts in (firsts, seconds):
            total = parts[0][:, at].astype(jnp.float32)
            for part in parts[1:]:
                total = total + part[:, at].astype(jnp.float32)
            sums.append(total.astype(jnp.bfloat16))
        packed = jnp.concatenate(sums + [rest_ref[:, at]], axis=0)
        spread = jnp.dot(back_ref[...], packed, preferred_element_type=jnp.float32).astype(jnp.bfloat16)
        results_ref[:, :, at] = spread.reshape(results_ref.shape[0], results_ref.shape[1], COLUMNS)
        return carried

    lax.fori_loop(0, width // COLUMNS, step, 0)


def rest_outputs(rest, weights):
    members = lax.axis_size("tp")
    copies = jnp.broadcast_to(rest[None], (members, *rest.shape))
    rows = lax.all_to_all(copies, "tp", split_axis=0, concat_axis=0, tiled=True).reshape(-1, rest.shape[1])
    (share,) = run_experts((rows,), weights)
    parts = lax.all_to_all(split_up(share, 0, members), "tp", split_axis=0, concat_axis=0, tiled=True)
    return jnp.sum(parts.astype(jnp.float32), axis=0).astype(jnp.bfloat16)


def expert_outputs(arrived, most, weights):
    experts, capacity, width = arrived.shape
    slots = experts * capacity
    half, other = (jax.ShapeDtypeStruct((count, width), jnp.bfloat16) for count in PACKED)
    rest_shape = jax.ShapeDtypeStruct((slots - sum(PACKED), width), jnp.bfloat16)
    square = jax.ShapeDtypeStruct((slots, slots), jnp.bfloat16)
    first, second, rest, back = in_kernel(
        pack_kernel, (half, other, rest_shape, square), 16, 2 * slots * slots * width, arrived,
        scratch=[pltpu.VMEM((slots, width), jnp.bfloat16)],
    )
    below_first = along_tp(first, 1)
    above_second = along_tp(second, -1)
    below_second = along_tp(second, 1)
    above_first = along_tp(first, -1)
    far_first = along_tp(below_first, 1)
    far_second = along_tp(above_second, -1)
    own = run_experts((first, second), weights)
    near = run_experts((below_first, below_second, above_first, above_second), weights)
    direct_up = along_tp(near[3], 1)
    direct_down = along_tp(near[0], -1)
    far = run_experts((far_first, far_second), weights)
    relay_up = along_tp(far[0], 1)
    relay_down = along_tp(far[1], -1)
    both_up, both_down = in_kernel(
        relay_kernel, (half, other), 8, 2 * sum(PACKED) * width, near[2], relay_up, near[1], relay_down
    )
    both_up = along_tp(both_up, 1)
    both_down = along_tp(both_down, -1)
    rest_out = lax.cond(most > sum(PACKED), lambda: rest_outputs(rest, weights), lambda: jnp.zeros_like(rest))
    return in_kernel(
        unpack_kernel, jax.ShapeDtypeStruct(arrived.shape, jnp.bfloat16), 16,
        2 * slots * slots * width, back, rest_out, own[0], both_up, direct_down, own[1], direct_up, both_down,
    )


def on_device(
    queries,
    keys,
    values,
    break_bias,
    residual,
    w_out,
    ffn_gain,
    pick_ids,
    pair_logit,
    w_gate,
    w_up,
    w_down,
    out_gain,
):
    position = lax.axis_index("sp")
    quarters = lax.axis_size("tp")
    quarter = lax.axis_index("tp")
    slice_rows = queries.shape[0] // quarters
    width = w_out.shape[1]
    experts = lax.axis_size("sp")
    capacity = max(2, (3 * slice_rows + experts - 1) // experts)
    routed = lax.dynamic_slice_in_dim(pick_ids, quarter * slice_rows, slice_rows, 0)
    flat_ids = routed.reshape(slice_rows * TOP)
    places = jnp.arange(slice_rows * TOP, dtype=jnp.int32)
    matches = (flat_ids[:, None] == flat_ids[None, :]) & (places[None, :] < places[:, None])
    ranks = jnp.sum(matches.astype(jnp.int32), axis=1)
    targets = (flat_ids * capacity + ranks).reshape(slice_rows, TOP)
    logits = lax.dynamic_slice_in_dim(pair_logit, quarter * slice_rows, slice_rows, 0)[:, None]

    place = position.reshape(1).astype(jnp.int32)
    head_out, most = attend(queries, keys, values, break_bias, pick_ids, place)
    partial = jnp.dot(head_out, w_out, preferred_element_type=jnp.float32).astype(jnp.bfloat16)
    parts = split_up(partial, 0, quarters)
    mixed = lax.all_to_all(parts, "tp", split_axis=0, concat_axis=0, tiled=True)
    slots = jax.ShapeDtypeStruct((experts, capacity, width), jnp.bfloat16)
    rows = jax.ShapeDtypeStruct((slice_rows, width), jnp.bfloat16)
    dispatch_flops = 2 * experts * capacity * slice_rows * width
    stream, outgoing = in_kernel(
        dispatch_kernel, (rows, slots), 16, dispatch_flops,
        mixed, residual, ffn_gain[None], targets.T,
    )
    arrived = lax.all_to_all(outgoing, "sp", split_axis=0, concat_axis=0, tiled=True)
    results = expert_outputs(arrived, most[0], (w_gate[0], w_up[0], w_down[0]))
    returned = lax.all_to_all(results, "sp", split_axis=0, concat_axis=0, tiled=True)
    return in_kernel(
        final_kernel, rows, 16, 2 * dispatch_flops,
        returned, targets, logits, stream, out_gain[None],
        scratch=[pltpu.VMEM((slice_rows, width), jnp.float32)],
    )


def solution(mesh):
    placed = (
        P("sp", "tp"),
        P("sp", "tp"),
        P("sp", "tp"),
        P("tp"),
        P(("sp", "tp"), None),
        P("tp", None),
        P(),
        P("sp", None),
        P("sp"),
        P("sp", None, "tp"),
        P("sp", None, "tp"),
        P("sp", "tp", None),
        P(),
    )

    return jax.shard_map(on_device, mesh=mesh, in_specs=placed, out_specs=P(("sp", "tp"), None), check_vma=False)
```

```python
import functools
import itertools

import jax
import jax.numpy as jnp
from jax import lax
from jax.experimental import pallas as pl
from jax.experimental.pallas import tpu as pltpu
from jax.sharding import PartitionSpec as P


HEAD = 128
TOP = 2
Z_SIZE = 8
X_SIZE = 4
CORES = 2
Z_PLANE = X_SIZE * CORES

epsilon = 1e-06


def split_up(shard, dim, peers):
    before, after = (shard.shape[:dim], shard.shape[dim + 1 :])
    return jnp.moveaxis(shard.reshape(*before, peers, -1, *after), dim, 0)


LOG2E = 1.4426950408889634
KEY_BLOCK = 256
MOST = 100.0
PICK_ROWS = 8


def causal_visit(state, query_ref, kv_ref, bias_ref, later, block, first_query):
    outputs, used = state
    rows = query_ref.shape[0] // bias_ref.shape[0]
    heads = bias_ref.shape[0]
    factor = HEAD ** (-0.5) * LOG2E
    at_block = pl.ds(pl.multiple_of(block * KEY_BLOCK, KEY_BLOCK), KEY_BLOCK)
    keys = kv_ref[at_block, :HEAD]
    values = kv_ref[at_block, HEAD:]
    scores = lax.dot_general(
        query_ref[...], keys, (((1,), (1,)), ((), ())), preferred_element_type=jnp.float32
    )
    if first_query is not None:
        query_pos = first_query + lax.broadcasted_iota(jnp.int32, (rows, KEY_BLOCK), 0)
        key_pos = block * KEY_BLOCK + lax.broadcasted_iota(jnp.int32, (rows, KEY_BLOCK), 1)
        before = key_pos < query_pos
    breaks, leads = [], []
    for head in range(heads):
        z = scores[head * rows : (head + 1) * rows] * factor + bias_ref[head] * LOG2E
        softplus = jnp.maximum(jnp.log2(1.0 + jnp.exp2(jnp.minimum(z, MOST))), z)
        leads.append(z - softplus)
        breaks.append(softplus if first_query is None else jnp.where(before, softplus, 0.0))
    behind = jnp.dot(
        jnp.concatenate([b.astype(jnp.bfloat16) for b in breaks], axis=0),
        later,
        preferred_element_type=jnp.float32,
    )
    weights = []
    for head in range(heads):
        at = slice(head * rows, (head + 1) * rows)
        past = behind[at]
        gone = used[at]
        weight = jnp.exp2(leads[head] - past - jnp.concatenate([gone, gone], axis=1))
        if first_query is not None:
            weight = jnp.where(before, weight, 0.0)
        weights.append(weight.astype(jnp.bfloat16))
        used[at] = gone + jnp.broadcast_to(past[:, :1] + breaks[head][:, :1], gone.shape)
    outputs[...] += jnp.dot(
        jnp.concatenate(weights, axis=0), values, preferred_element_type=jnp.float32
    )


def later_keys():
    return (
        lax.broadcasted_iota(jnp.int32, (KEY_BLOCK, KEY_BLOCK), 0)
        > lax.broadcasted_iota(jnp.int32, (KEY_BLOCK, KEY_BLOCK), 1)
    ).astype(jnp.float32).astype(jnp.bfloat16)


def lay_out(own_ref, twin_ref, plane, place):
    lanes = (place // CORES) % X_SIZE
    core = place % CORES
    length = own_ref.shape[1] - PICK_ROWS
    for shift in range(X_SIZE):
        source = ((lanes + X_SIZE - shift) % X_SIZE) * CORES
        plane[pl.ds(pl.multiple_of((source + core) * length, length), length)] = own_ref[shift, :length]
        plane[pl.ds(pl.multiple_of((source + 1 - core) * length, length), length)] = twin_ref[shift, :length]


def tally(counts, *pieces):
    expert = lax.broadcasted_iota(jnp.int32, counts.shape, 0).astype(jnp.float32)
    found = counts[...]
    for piece in pieces:
        length = piece.shape[1] - PICK_ROWS
        for shift in range(X_SIZE):
            picks = piece[shift, length:].astype(jnp.float32)[0:1]
            found = found + (picks == expert).astype(jnp.float32)
    counts[...] = found


def own_plane_kernel(place_ref, bias_ref, query_ref, own_ref, twin_ref, near, near_used, far, counts, plane):
    place = place_ref[0]
    lay_out(own_ref, twin_ref, plane, place)
    for ref in (near, near_used, far, counts):
        ref[...] = jnp.zeros_like(ref)
    tally(counts, own_ref, twin_ref)
    later = later_keys()
    rows = query_ref.shape[0] // bias_ref.shape[0]
    first_query = (place % (X_SIZE * CORES)) * rows
    last = (first_query + rows - 1) // KEY_BLOCK

    def step(index, carried):
        causal_visit((near, near_used), query_ref, plane, bias_ref, later, last - index, first_query)
        return carried

    lax.fori_loop(0, last + 1, step, 0)


def whole_plane(state, query_ref, plane, bias_ref, together=2):
    later = later_keys()
    blocks = plane.shape[0] // KEY_BLOCK

    def step(index, carried):
        for offset in range(together):
            block = blocks - 1 - offset - together * index
            causal_visit(state, query_ref, plane, bias_ref, later, block, None)
        return carried

    lax.fori_loop(0, blocks // together, step, 0)


def two_planes_kernel(distance, place_ref, bias_ref, query_ref, below, below_twin, above, above_twin,
                      near_in, near_used_in, far_in, counts_in, near, near_used, far, counts,
                      planes, found, found_used):
    place = place_ref[0]
    tally(counts, below, below_twin, above, above_twin)
    level = place // (X_SIZE * CORES)
    lay_out(below, below_twin, planes.at[0], place)
    lay_out(above, above_twin, planes.at[1], place)

    def visit(side, carried):
        found[...] = jnp.zeros_like(found)
        found_used[...] = jnp.zeros_like(found_used)
        whole_plane((found, found_used), query_ref, planes.at[side], bias_ref)

        @pl.when(side == 0)
        def _():
            near[...] += jnp.exp2(-near_used[...]) * found[...]
            near_used[...] += found_used[...]

        @pl.when(side == 1)
        def _():
            far[...] = found[...] + jnp.exp2(-found_used[...]) * far[...]

        return carried

    first = jnp.where(level >= distance, 0, 1)
    past = jnp.where(level + distance >= Z_SIZE, 2, 1)
    lax.fori_loop(first, past, visit, 0)


def last_plane_kernel(distance, place_ref, bias_ref, query_ref, below, below_twin,
                      near_in, near_used_in, far_in, counts_in, out_ref, most_ref, plane, near, near_used, counts):
    place = place_ref[0]
    counts[...] = counts_in[...]
    tally(counts, below, below_twin)
    rows = out_ref.shape[0]
    lane = lax.broadcasted_iota(jnp.int32, counts.shape, 1) % rows // (rows // 4)
    most = jnp.zeros((counts.shape[0], 1), jnp.float32)
    for member in range(4):
        named = jnp.sum(jnp.where(lane == member, counts[...], 0.0), axis=1, keepdims=True)
        most = jnp.maximum(most, named)
    most_ref[0] = jnp.max(most).astype(jnp.int32)
    near[...] = near_in[...]
    near_used[...] = near_used_in[...]

    @pl.when(place // (X_SIZE * CORES) >= distance)
    def _():
        lay_out(below, below_twin, plane, place)
        whole_plane((near, near_used), query_ref, plane, bias_ref, 1)

    rows = out_ref.shape[0]
    for head in range(bias_ref.shape[0]):
        at = slice(head * rows, (head + 1) * rows)
        output = near[at] + jnp.exp2(-near_used[at]) * far_in[at]
        scaled = output * lax.rsqrt(jnp.mean(output * output, axis=-1, keepdims=True) + epsilon)
        out_ref[:, head * HEAD : (head + 1) * HEAD] = scaled.astype(jnp.bfloat16)


def attention_call(kernel, name, planes, position, break_bias, stacked, key_values, state, rows):
    stack = stacked.shape[0]
    in_vmem = pl.BlockSpec(memory_space=pltpu.VMEM)
    in_smem = pl.BlockSpec(memory_space=pltpu.SMEM)
    plane = (Z_PLANE * rows, 2 * HEAD)
    running = pltpu.VMEM((stack, HEAD), jnp.float32)
    kept = jax.ShapeDtypeStruct((stack, HEAD), jnp.float32)
    counts = (Z_SIZE * Z_PLANE, rows * TOP)
    last = name == "attend_last"
    keys = planes * Z_PLANE * rows
    first_state = 3 + len(key_values)
    heads = jax.ShapeDtypeStruct((rows, stack // rows * HEAD), jnp.bfloat16)
    return pl.pallas_call(
        kernel,
        out_shape=(heads, jax.ShapeDtypeStruct((1,), jnp.int32))
        if last
        else (kept,) * 3 + (jax.ShapeDtypeStruct(counts, jnp.float32),),
        in_specs=[in_smem, in_smem] + [in_vmem] * (1 + len(key_values) + len(state)),
        out_specs=(in_vmem, in_smem) if last else (in_vmem,) * 4,
        scratch_shapes=[pltpu.VMEM(plane if planes == 1 else (planes, *plane), jnp.bfloat16)]
        + ([running, running] if state else [])
        + ([pltpu.VMEM(counts, jnp.float32)] if last else []),
        input_output_aliases={} if last or not state else {first_state + i: i for i in range(4)},
        cost_estimate=pl.CostEstimate(
            flops=2 * stack * keys * (2 * HEAD + KEY_BLOCK), transcendentals=3 * stack * keys, bytes_accessed=0
        ),
        compiler_params=pltpu.CompilerParams(vmem_limit_bytes=24 * 1024 * 1024),
    )(position, break_bias, stacked, *key_values, *state)


def moved(shard, step_z, step_x, swap):
    pairs = []
    for place in range(Z_SIZE * Z_PLANE):
        z, x, core = place // Z_PLANE, place // CORES % X_SIZE, place % CORES
        target = ((z + step_z) % Z_SIZE * X_SIZE + (x + step_x) % X_SIZE) * CORES + (core ^ swap)
        pairs.append((place, target))
    return lax.ppermute(shard, "sp", pairs)


def attend(queries, keys, values, break_bias, pick_ids, position):
    rows = queries.shape[0]
    heads = queries.shape[1] // HEAD
    stacked = jnp.concatenate([queries[:, h * HEAD : (h + 1) * HEAD] for h in range(heads)], axis=0)
    picks = pick_ids.T.astype(jnp.bfloat16).reshape(1, TOP * rows)
    picks = jnp.concatenate([picks, jnp.zeros((PICK_ROWS - 1, rows * TOP), jnp.bfloat16)], axis=0)
    block = jnp.concatenate([jnp.concatenate([keys, values], axis=1), picks], axis=0)
    own = jnp.stack([block] + [moved(block, 0, step, 0) for step in range(1, X_SIZE)])
    twin = moved(own, 0, 0, 1)
    common = (position, break_bias, stacked)
    below, above = own, own
    arrived = []
    for distance in range(1, Z_SIZE // 2 + 1):
        below = moved(below, 1, 0, 0)
        pieces = [below, moved(below, 0, 0, 1)]
        if distance < Z_SIZE // 2:
            above = moved(above, -1, 0, 0)
            pieces += [above, moved(above, 0, 0, 1)]
        arrived.append(pieces)
    state = attention_call(own_plane_kernel, "attend_0", 1, *common, (own, twin), (), rows)
    for distance in range(1, Z_SIZE // 2):
        kernel = functools.partial(two_planes_kernel, distance)
        name = f"attend_{distance}"
        state = attention_call(kernel, name, 2, *common, arrived[distance - 1], state, rows)
    kernel = functools.partial(last_plane_kernel, Z_SIZE // 2)
    return attention_call(kernel, "attend_last", 1, *common, arrived[-1], state, rows)


COLUMNS = 1024
PACKED = (48, 40)


def in_kernel(kernel, out_shapes, megabytes, flops, *operands, scratch=()):
    spec = pl.BlockSpec(memory_space=pltpu.VMEM)
    several = isinstance(out_shapes, tuple)
    return pl.pallas_call(
        kernel,
        out_shape=out_shapes,
        in_specs=[spec] * len(operands),
        out_specs=(spec,) * len(out_shapes) if several else spec,
        scratch_shapes=list(scratch),
        cost_estimate=pl.CostEstimate(flops=flops, transcendentals=0, bytes_accessed=0),
        compiler_params=pltpu.CompilerParams(vmem_limit_bytes=megabytes * 1024 * 1024),
    )(*operands)


def over_columns(width, step, carried, unrolled=False):
    if unrolled:
        for start in range(0, width, COLUMNS):
            carried = step(slice(start, start + COLUMNS), carried)
        return carried

    def at_column(index, carried):
        return step(pl.ds(pl.multiple_of(index * COLUMNS, COLUMNS), COLUMNS), carried)

    return lax.fori_loop(0, width // COLUMNS, at_column, carried)


def dispatch_kernel(mixed_ref, residual_ref, gain_ref, targets_ref, stream_ref, outgoing_ref):
    rows, width = residual_ref.shape
    experts, capacity = outgoing_ref.shape[:2]

    def add(at, total):
        mixed = mixed_ref[0, :, at].astype(jnp.float32)
        for member in range(1, mixed_ref.shape[0]):
            mixed = mixed + mixed_ref[member, :, at].astype(jnp.float32)
        stream = (residual_ref[:, at].astype(jnp.float32) + mixed).astype(jnp.bfloat16)
        stream_ref[:, at] = stream
        wide = stream.astype(jnp.float32)
        return total + jnp.sum(wide * wide, axis=1, keepdims=True)

    total = over_columns(width, add, jnp.zeros((rows, 1), jnp.float32), True)
    scale = lax.rsqrt(total / width + epsilon)
    slot = lax.broadcasted_iota(jnp.int32, (experts * capacity, rows), 0)
    chosen = (slot == targets_ref[0:1, :]) | (slot == targets_ref[1:2, :])
    chosen = chosen.astype(jnp.float32).astype(jnp.bfloat16)

    def send(at, carried):
        normed = (stream_ref[:, at].astype(jnp.float32) * scale * gain_ref[:, at]).astype(jnp.bfloat16)
        sent = jnp.dot(chosen, normed, preferred_element_type=jnp.float32).astype(jnp.bfloat16)
        outgoing_ref[:, :, at] = sent.reshape(experts, capacity, COLUMNS)
        return carried

    over_columns(width, send, 0, True)


def pack_kernel(arrived_ref, first_ref, second_ref, rest_ref, back_ref, entries):
    slots = arrived_ref.shape[0] * arrived_ref.shape[1]
    width = arrived_ref.shape[2]

    def read(at, largest):
        part = arrived_ref[:, :, at].reshape(slots, COLUMNS)
        entries[:, at] = part
        size = jnp.abs(part.astype(jnp.float32))
        for lane in range(0, COLUMNS, 128):
            largest = jnp.maximum(largest, size[:, lane : lane + 128])
        return largest

    largest = over_columns(width, read, jnp.zeros((slots, 128), jnp.float32))
    held = (jnp.max(largest, axis=1, keepdims=True) > 0).astype(jnp.float32)
    row = lax.broadcasted_iota(jnp.int32, (slots, slots), 0)
    column = lax.broadcasted_iota(jnp.int32, (slots, slots), 1)

    def product(left, right):
        left, right = left.astype(jnp.float32), right.astype(jnp.float32)
        return jnp.dot(
            left.astype(jnp.bfloat16), right.astype(jnp.bfloat16), preferred_element_type=jnp.float32
        )

    held_rows = jnp.broadcast_to(held, (slots, slots))
    held_columns = product(jnp.ones((slots, slots), jnp.float32), jnp.where(row == column, held_rows, 0.0))
    place_rows = product(column < row, held_rows)
    place_columns = product(held_columns, row < column)
    back = ((place_rows == column.astype(jnp.float32)) & (held_rows > 0)).astype(jnp.float32)
    back_ref[...] = back.astype(jnp.bfloat16)
    forth = ((place_columns == row.astype(jnp.float32)) & (held_columns > 0)).astype(jnp.float32)
    forth = forth.astype(jnp.bfloat16)
    half, both = first_ref.shape[0], first_ref.shape[0] + second_ref.shape[0]

    def write(at, carried):
        packed = jnp.dot(forth, entries[:, at], preferred_element_type=jnp.float32).astype(jnp.bfloat16)
        first_ref[:, at] = packed[:half]
        second_ref[:, at] = packed[half:both]
        rest_ref[:, at] = packed[both:]
        return carried

    over_columns(width, write, 0, True)


def expert_kernel(*refs):
    count = (len(refs) - 6) // 2
    inputs, outs = refs[:count], refs[count + 3 : -3]
    gate_ref, up_ref, down_ref = refs[count : count + 3]
    entries, gate, up = refs[-3:]
    width = inputs[0].shape[1]
    ends = list(itertools.accumulate(source.shape[0] for source in inputs))
    for source, end in zip(inputs, ends):
        entries[end - source.shape[0] : end] = source[...]
    gate[...] = jnp.zeros_like(gate)
    up[...] = jnp.zeros_like(up)

    def rise(index, carried):
        at = pl.ds(pl.multiple_of(index * COLUMNS, COLUMNS), COLUMNS)
        part = entries[:, at]
        gate[...] += jnp.dot(part, gate_ref[at, :], preferred_element_type=jnp.float32)
        up[...] += jnp.dot(part, up_ref[at, :], preferred_element_type=jnp.float32)
        return carried

    lax.fori_loop(0, width // COLUMNS, rise, 0)
    hidden = (gate[...] / (1.0 + jnp.exp(-gate[...])) * up[...]).astype(jnp.bfloat16)

    def fall(index, carried):
        at = pl.ds(pl.multiple_of(index * COLUMNS, COLUMNS), COLUMNS)
        share = jnp.dot(hidden, down_ref[:, at], preferred_element_type=jnp.float32).astype(jnp.bfloat16)
        for out, end in zip(outs, ends):
            out[:, at] = share[end - out.shape[0] : end]
        return carried

    lax.fori_loop(0, width // COLUMNS, fall, 0)


def run_experts(pieces, weights):
    shapes = tuple(jax.ShapeDtypeStruct(piece.shape, jnp.bfloat16) for piece in pieces)
    slots = sum(piece.shape[0] for piece in pieces)
    width, units = weights[0].shape
    flops = 6 * slots * width * units
    scratch = [pltpu.VMEM((slots, width), jnp.bfloat16)] + [pltpu.VMEM((slots, units), jnp.float32)] * 2
    return in_kernel(expert_kernel, shapes, 32, flops, *pieces, *weights, scratch=scratch)


def final_kernel(returned_ref, targets_ref, logits_ref, stream_ref, gain_ref, out_ref, blended):
    rows, width = stream_ref.shape
    slots = returned_ref.shape[0] * returned_ref.shape[1]
    slot = lax.broadcasted_iota(jnp.int32, (rows, slots), 1).astype(jnp.float32)
    diagonal = lax.broadcasted_iota(jnp.int32, (rows, rows), 0) == lax.broadcasted_iota(jnp.int32, (rows, rows), 1)

    def column(row):
        return jnp.sum(jnp.where(diagonal, row.astype(jnp.float32), 0.0), axis=1, keepdims=True)

    picks = [
        (slot == column(targets_ref[pick : pick + 1])).astype(jnp.float32).astype(jnp.bfloat16)
        for pick in range(TOP)
    ]
    logits = column(logits_ref[...])
    shares = (1.0 / (1.0 + jnp.exp(-logits)), 1.0 / (1.0 + jnp.exp(logits)))

    def mix(at, total):
        entries = returned_ref[:, :, at].reshape(slots, COLUMNS)
        both = shares[0] * jnp.dot(picks[0], entries, preferred_element_type=jnp.float32)
        both = both + shares[1] * jnp.dot(picks[1], entries, preferred_element_type=jnp.float32)
        blended[:, at] = both
        return total + jnp.sum(both * both, axis=1, keepdims=True)

    total = over_columns(width, mix, jnp.zeros((rows, 1), jnp.float32), True)
    scale = lax.rsqrt(total / width + epsilon)

    def add(at, carried):
        wide = stream_ref[:, at].astype(jnp.float32)
        out_ref[:, at] = (wide + blended[:, at] * scale * gain_ref[:, at]).astype(jnp.bfloat16)
        return carried

    over_columns(width, add, 0, True)


def along_tp(shard, step):
    size = lax.axis_size("tp")
    return lax.ppermute(shard, "tp", [(member, (member + step) % size) for member in range(size)])


def relay_kernel(own_up, far_up, own_down, far_down, up_ref, down_ref):
    for own, far, out in ((own_up, far_up, up_ref), (own_down, far_down, down_ref)):

        def step(index, carried):
            at = pl.ds(pl.multiple_of(index * COLUMNS, COLUMNS), COLUMNS)
            out[:, at] = (own[:, at].astype(jnp.float32) + far[:, at].astype(jnp.float32)).astype(jnp.bfloat16)
            return carried

        lax.fori_loop(0, out.shape[1] // COLUMNS, step, 0)


def unpack_kernel(back_ref, rest_ref, *refs):
    firsts, seconds, results_ref = refs[:3], refs[3:6], refs[6]
    width = firsts[0].shape[1]

    def step(at, carried):
        sums = []
        for parts in (firsts, seconds):
            total = parts[0][:, at].astype(jnp.float32)
            for part in parts[1:]:
                total = total + part[:, at].astype(jnp.float32)
            sums.append(total.astype(jnp.bfloat16))
        packed = jnp.concatenate(sums + [rest_ref[:, at]], axis=0)
        spread = jnp.dot(back_ref[...], packed, preferred_element_type=jnp.float32).astype(jnp.bfloat16)
        results_ref[:, :, at] = spread.reshape(results_ref.shape[0], results_ref.shape[1], COLUMNS)
        return carried

    over_columns(width, step, 0, True)


def rest_outputs(rest, weights):
    members = lax.axis_size("tp")
    copies = jnp.broadcast_to(rest[None], (members, *rest.shape))
    rows = lax.all_to_all(copies, "tp", split_axis=0, concat_axis=0, tiled=True).reshape(-1, rest.shape[1])
    (share,) = run_experts((rows,), weights)
    parts = lax.all_to_all(split_up(share, 0, members), "tp", split_axis=0, concat_axis=0, tiled=True)
    return jnp.sum(parts.astype(jnp.float32), axis=0).astype(jnp.bfloat16)


def expert_outputs(arrived, most, weights):
    experts, capacity, width = arrived.shape
    slots = experts * capacity
    half, other = (jax.ShapeDtypeStruct((count, width), jnp.bfloat16) for count in PACKED)
    rest_shape = jax.ShapeDtypeStruct((slots - sum(PACKED), width), jnp.bfloat16)
    square = jax.ShapeDtypeStruct((slots, slots), jnp.bfloat16)
    first, second, rest, back = in_kernel(
        pack_kernel, (half, other, rest_shape, square), 16, 2 * slots * slots * width, arrived,
        scratch=[pltpu.VMEM((slots, width), jnp.bfloat16)],
    )
    below_first = along_tp(first, 1)
    above_second = along_tp(second, -1)
    below_second = along_tp(second, 1)
    above_first = along_tp(first, -1)
    far_first = along_tp(below_first, 1)
    far_second = along_tp(above_second, -1)
    own = run_experts((first, second), weights)
    near = run_experts((below_first, below_second, above_first, above_second), weights)
    direct_up = along_tp(near[3], 1)
    direct_down = along_tp(near[0], -1)
    far = run_experts((far_first, far_second), weights)
    relay_up = along_tp(far[0], 1)
    relay_down = along_tp(far[1], -1)
    both_up, both_down = in_kernel(
        relay_kernel, (half, other), 8, 2 * sum(PACKED) * width, near[2], relay_up, near[1], relay_down
    )
    both_up = along_tp(both_up, 1)
    both_down = along_tp(both_down, -1)
    rest_out = lax.cond(most > sum(PACKED), lambda: rest_outputs(rest, weights), lambda: jnp.zeros_like(rest))
    return in_kernel(
        unpack_kernel, jax.ShapeDtypeStruct(arrived.shape, jnp.bfloat16), 16,
        2 * slots * slots * width, back, rest_out, own[0], both_up, direct_down, own[1], direct_up, both_down,
    )


def on_device(
    queries,
    keys,
    values,
    break_bias,
    residual,
    w_out,
    ffn_gain,
    pick_ids,
    pair_logit,
    w_gate,
    w_up,
    w_down,
    out_gain,
):
    position = lax.axis_index("sp")
    quarters = lax.axis_size("tp")
    quarter = lax.axis_index("tp")
    slice_rows = queries.shape[0] // quarters
    width = w_out.shape[1]
    experts = lax.axis_size("sp")
    capacity = max(2, (3 * slice_rows + experts - 1) // experts)
    routed = lax.dynamic_slice_in_dim(pick_ids.T, quarter * slice_rows, slice_rows, 1)
    flat_ids = routed.reshape(slice_rows * TOP)
    places = jnp.arange(slice_rows * TOP, dtype=jnp.int32)
    matches = (flat_ids[:, None] == flat_ids[None, :]) & (places[None, :] < places[:, None])
    ranks = jnp.sum(matches.astype(jnp.int32), axis=1)
    targets = (flat_ids * capacity + ranks).reshape(TOP, slice_rows)
    logits = lax.dynamic_slice_in_dim(pair_logit, quarter * slice_rows, slice_rows, 0)[None]

    place = position.reshape(1).astype(jnp.int32)
    head_out, most = attend(queries, keys, values, break_bias, pick_ids, place)
    head_out, targets, logits = lax.optimization_barrier((head_out, targets, logits))
    partial = jnp.dot(head_out, w_out, preferred_element_type=jnp.float32).astype(jnp.bfloat16)
    parts = split_up(partial, 0, quarters)
    mixed = lax.all_to_all(parts, "tp", split_axis=0, concat_axis=0, tiled=True)
    slots = jax.ShapeDtypeStruct((experts, capacity, width), jnp.bfloat16)
    rows = jax.ShapeDtypeStruct((slice_rows, width), jnp.bfloat16)
    dispatch_flops = 2 * experts * capacity * slice_rows * width
    stream, outgoing = in_kernel(
        dispatch_kernel, (rows, slots), 16, dispatch_flops,
        mixed, residual, ffn_gain[None], targets,
    )
    arrived = lax.all_to_all(outgoing, "sp", split_axis=0, concat_axis=0, tiled=True)
    results = expert_outputs(arrived, most[0], (w_gate[0], w_up[0], w_down[0]))
    returned = lax.all_to_all(results, "sp", split_axis=0, concat_axis=0, tiled=True)
    return in_kernel(
        final_kernel, rows, 16, 2 * dispatch_flops,
        returned, targets, logits, stream, out_gain[None],
        scratch=[pltpu.VMEM((slice_rows, width), jnp.float32)],
    )


def solution(mesh):
    placed = (
        P("sp", "tp"),
        P("sp", "tp"),
        P("sp", "tp"),
        P("tp"),
        P(("sp", "tp"), None),
        P("tp", None),
        P(),
        P("sp", None),
        P("sp"),
        P("sp", None, "tp"),
        P("sp", None, "tp"),
        P("sp", "tp", None),
        P(),
    )

    return jax.shard_map(on_device, mesh=mesh, in_specs=placed, out_specs=P(("sp", "tp"), None), check_vma=False)
```

```python
import functools
import itertools

import jax
import jax.numpy as jnp
from jax import lax
from jax.experimental import pallas as pl
from jax.experimental.pallas import tpu as pltpu
from jax.sharding import PartitionSpec as P


HEAD = 128
TOP = 2
Z_SIZE = 8
X_SIZE = 4
CORES = 2
Z_PLANE = X_SIZE * CORES

epsilon = 1e-06


def split_up(shard, dim, peers):
    before, after = (shard.shape[:dim], shard.shape[dim + 1 :])
    return jnp.moveaxis(shard.reshape(*before, peers, -1, *after), dim, 0)


LOG2E = 1.4426950408889634
KEY_BLOCK = 256
MOST = 100.0
PICK_ROWS = 8


def causal_visit(state, query_ref, kv_ref, bias_ref, later, block, first_query):
    outputs, used = state
    rows = query_ref.shape[0] // bias_ref.shape[0]
    heads = bias_ref.shape[0]
    factor = HEAD ** (-0.5) * LOG2E
    at_block = pl.ds(pl.multiple_of(block * KEY_BLOCK, KEY_BLOCK), KEY_BLOCK)
    keys = kv_ref[at_block, :HEAD]
    values = kv_ref[at_block, HEAD:]
    scores = lax.dot_general(
        query_ref[...], keys, (((1,), (1,)), ((), ())), preferred_element_type=jnp.float32
    )
    if first_query is not None:
        query_pos = first_query + lax.broadcasted_iota(jnp.int32, (rows, KEY_BLOCK), 0)
        key_pos = block * KEY_BLOCK + lax.broadcasted_iota(jnp.int32, (rows, KEY_BLOCK), 1)
        before = key_pos < query_pos
    breaks, leads = [], []
    for head in range(heads):
        z = scores[head * rows : (head + 1) * rows] * factor + bias_ref[head] * LOG2E
        softplus = jnp.maximum(jnp.log2(1.0 + jnp.exp2(jnp.minimum(z, MOST))), z)
        leads.append(z - softplus)
        breaks.append(softplus if first_query is None else jnp.where(before, softplus, 0.0))
    behind = jnp.dot(
        jnp.concatenate([b.astype(jnp.bfloat16) for b in breaks], axis=0),
        later,
        preferred_element_type=jnp.float32,
    )
    weights = []
    for head in range(heads):
        at = slice(head * rows, (head + 1) * rows)
        past = behind[at]
        gone = used[at]
        weight = jnp.exp2(leads[head] - past - jnp.concatenate([gone, gone], axis=1))
        if first_query is not None:
            weight = jnp.where(before, weight, 0.0)
        weights.append(weight.astype(jnp.bfloat16))
        used[at] = gone + jnp.broadcast_to(past[:, :1] + breaks[head][:, :1], gone.shape)
    outputs[...] += jnp.dot(
        jnp.concatenate(weights, axis=0), values, preferred_element_type=jnp.float32
    )


def later_keys():
    return (
        lax.broadcasted_iota(jnp.int32, (KEY_BLOCK, KEY_BLOCK), 0)
        > lax.broadcasted_iota(jnp.int32, (KEY_BLOCK, KEY_BLOCK), 1)
    ).astype(jnp.float32).astype(jnp.bfloat16)


def lay_out(own_ref, twin_ref, plane, place):
    lanes = (place // CORES) % X_SIZE
    core = place % CORES
    length = own_ref.shape[1] - PICK_ROWS
    for shift in range(X_SIZE):
        source = ((lanes + X_SIZE - shift) % X_SIZE) * CORES
        plane[pl.ds(pl.multiple_of((source + core) * length, length), length)] = own_ref[shift, :length]
        plane[pl.ds(pl.multiple_of((source + 1 - core) * length, length), length)] = twin_ref[shift, :length]


def tally(counts, *pieces):
    expert = lax.broadcasted_iota(jnp.int32, counts.shape, 0).astype(jnp.float32)
    found = counts[...]
    for piece in pieces:
        length = piece.shape[1] - PICK_ROWS
        for shift in range(X_SIZE):
            picks = piece[shift, length:].astype(jnp.float32)[0:1]
            found = found + (picks == expert).astype(jnp.float32)
    counts[...] = found


def own_plane_kernel(place_ref, bias_ref, query_ref, own_ref, twin_ref, near, near_used, far, counts, plane):
    place = place_ref[0]
    lay_out(own_ref, twin_ref, plane, place)
    for ref in (near, near_used, far, counts):
        ref[...] = jnp.zeros_like(ref)
    tally(counts, own_ref, twin_ref)
    later = later_keys()
    rows = query_ref.shape[0] // bias_ref.shape[0]
    first_query = (place % (X_SIZE * CORES)) * rows
    last = (first_query + rows - 1) // KEY_BLOCK

    def step(index, carried):
        causal_visit((near, near_used), query_ref, plane, bias_ref, later, last - index, first_query)
        return carried

    lax.fori_loop(0, last + 1, step, 0)


def whole_plane(state, query_ref, plane, bias_ref, together=2):
    later = later_keys()
    blocks = plane.shape[0] // KEY_BLOCK

    def step(index, carried):
        for offset in range(together):
            block = blocks - 1 - offset - together * index
            causal_visit(state, query_ref, plane, bias_ref, later, block, None)
        return carried

    lax.fori_loop(0, blocks // together, step, 0)


def two_planes_kernel(distance, place_ref, bias_ref, query_ref, below, below_twin, above, above_twin,
                      near_in, near_used_in, far_in, counts_in, near, near_used, far, counts,
                      planes, found, found_used):
    place = place_ref[0]
    tally(counts, below, below_twin, above, above_twin)
    level = place // (X_SIZE * CORES)
    lay_out(below, below_twin, planes.at[0], place)
    lay_out(above, above_twin, planes.at[1], place)

    def visit(side, carried):
        found[...] = jnp.zeros_like(found)
        found_used[...] = jnp.zeros_like(found_used)
        whole_plane((found, found_used), query_ref, planes.at[side], bias_ref)

        @pl.when(side == 0)
        def _():
            near[...] += jnp.exp2(-near_used[...]) * found[...]
            near_used[...] += found_used[...]

        @pl.when(side == 1)
        def _():
            far[...] = found[...] + jnp.exp2(-found_used[...]) * far[...]

        return carried

    first = jnp.where(level >= distance, 0, 1)
    past = jnp.where(level + distance >= Z_SIZE, 2, 1)
    lax.fori_loop(first, past, visit, 0)


def last_plane_kernel(distance, place_ref, bias_ref, query_ref, below, below_twin,
                      near_in, near_used_in, far_in, counts_in, out_ref, most_ref, plane, near, near_used, counts):
    place = place_ref[0]
    counts[...] = counts_in[...]
    tally(counts, below, below_twin)
    rows = out_ref.shape[0]
    lane = lax.broadcasted_iota(jnp.int32, counts.shape, 1) % rows // (rows // 4)
    most = jnp.zeros((counts.shape[0], 1), jnp.float32)
    for member in range(4):
        named = jnp.sum(jnp.where(lane == member, counts[...], 0.0), axis=1, keepdims=True)
        most = jnp.maximum(most, named)
    most_ref[0] = jnp.max(most).astype(jnp.int32)
    near[...] = near_in[...]
    near_used[...] = near_used_in[...]

    @pl.when(place // (X_SIZE * CORES) >= distance)
    def _():
        lay_out(below, below_twin, plane, place)
        whole_plane((near, near_used), query_ref, plane, bias_ref, 1)

    rows = out_ref.shape[0]
    for head in range(bias_ref.shape[0]):
        at = slice(head * rows, (head + 1) * rows)
        output = near[at] + jnp.exp2(-near_used[at]) * far_in[at]
        scaled = output * lax.rsqrt(jnp.mean(output * output, axis=-1, keepdims=True) + epsilon)
        out_ref[:, head * HEAD : (head + 1) * HEAD] = scaled.astype(jnp.bfloat16)


def attention_call(kernel, name, planes, position, break_bias, stacked, key_values, state, rows):
    stack = stacked.shape[0]
    in_vmem = pl.BlockSpec(memory_space=pltpu.VMEM)
    in_smem = pl.BlockSpec(memory_space=pltpu.SMEM)
    plane = (Z_PLANE * rows, 2 * HEAD)
    running = pltpu.VMEM((stack, HEAD), jnp.float32)
    kept = jax.ShapeDtypeStruct((stack, HEAD), jnp.float32)
    counts = (Z_SIZE * Z_PLANE, rows * TOP)
    last = name == "attend_last"
    keys = planes * Z_PLANE * rows
    first_state = 3 + len(key_values)
    heads = jax.ShapeDtypeStruct((rows, stack // rows * HEAD), jnp.bfloat16)
    return pl.pallas_call(
        kernel,
        out_shape=(heads, jax.ShapeDtypeStruct((1,), jnp.int32))
        if last
        else (kept,) * 3 + (jax.ShapeDtypeStruct(counts, jnp.float32),),
        in_specs=[in_smem, in_smem] + [in_vmem] * (1 + len(key_values) + len(state)),
        out_specs=(in_vmem, in_smem) if last else (in_vmem,) * 4,
        scratch_shapes=[pltpu.VMEM(plane if planes == 1 else (planes, *plane), jnp.bfloat16)]
        + ([running, running] if state else [])
        + ([pltpu.VMEM(counts, jnp.float32)] if last else []),
        input_output_aliases={} if last or not state else {first_state + i: i for i in range(4)},
        cost_estimate=pl.CostEstimate(
            flops=2 * stack * keys * (2 * HEAD + KEY_BLOCK), transcendentals=3 * stack * keys, bytes_accessed=0
        ),
        compiler_params=pltpu.CompilerParams(vmem_limit_bytes=8 * 1024 * 1024),
    )(position, break_bias, stacked, *key_values, *state)


def moved(shard, step_z, step_x, swap):
    pairs = []
    for place in range(Z_SIZE * Z_PLANE):
        z, x, core = place // Z_PLANE, place // CORES % X_SIZE, place % CORES
        target = ((z + step_z) % Z_SIZE * X_SIZE + (x + step_x) % X_SIZE) * CORES + (core ^ swap)
        pairs.append((place, target))
    return lax.ppermute(shard, "sp", pairs)


def attend(queries, keys, values, break_bias, pick_ids, position, routing):
    rows = queries.shape[0]
    heads = queries.shape[1] // HEAD
    stacked = jnp.concatenate([queries[:, h * HEAD : (h + 1) * HEAD] for h in range(heads)], axis=0)
    picks = pick_ids.T.astype(jnp.bfloat16).reshape(1, TOP * rows)
    picks = jnp.concatenate([picks, jnp.zeros((PICK_ROWS - 1, rows * TOP), jnp.bfloat16)], axis=0)
    block = jnp.concatenate([jnp.concatenate([keys, values], axis=1), picks], axis=0)
    own = jnp.stack([block] + [moved(block, 0, step, 0) for step in range(1, X_SIZE)])
    own, stacked, routing = lax.optimization_barrier((own, stacked, routing))
    twin = moved(own, 0, 0, 1)
    common = (position, break_bias, stacked)
    below, above = own, own
    arrived = []
    for distance in range(1, Z_SIZE // 2 + 1):
        below = moved(below, 1, 0, 0)
        pieces = [below, moved(below, 0, 0, 1)]
        if distance < Z_SIZE // 2:
            above = moved(above, -1, 0, 0)
            pieces += [above, moved(above, 0, 0, 1)]
        arrived.append(pieces)
    state = attention_call(own_plane_kernel, "attend_0", 1, *common, (own, twin), (), rows)
    for distance in range(1, Z_SIZE // 2):
        kernel = functools.partial(two_planes_kernel, distance)
        name = f"attend_{distance}"
        state = attention_call(kernel, name, 2, *common, arrived[distance - 1], state, rows)
    kernel = functools.partial(last_plane_kernel, Z_SIZE // 2)
    return *attention_call(kernel, "attend_last", 1, *common, arrived[-1], state, rows), routing


COLUMNS = 1024
PACKED = (48, 40)


def in_kernel(kernel, out_shapes, megabytes, flops, *operands, scratch=()):
    spec = pl.BlockSpec(memory_space=pltpu.VMEM)
    several = isinstance(out_shapes, tuple)
    return pl.pallas_call(
        kernel,
        out_shape=out_shapes,
        in_specs=[spec] * len(operands),
        out_specs=(spec,) * len(out_shapes) if several else spec,
        scratch_shapes=list(scratch),
        cost_estimate=pl.CostEstimate(flops=flops, transcendentals=0, bytes_accessed=0),
        compiler_params=pltpu.CompilerParams(vmem_limit_bytes=megabytes * 1024 * 1024),
    )(*operands)


def over_columns(width, step, carried, unrolled=False):
    if unrolled:
        for start in range(0, width, COLUMNS):
            carried = step(slice(start, start + COLUMNS), carried)
        return carried

    def at_column(index, carried):
        return step(pl.ds(pl.multiple_of(index * COLUMNS, COLUMNS), COLUMNS), carried)

    return lax.fori_loop(0, width // COLUMNS, at_column, carried)


def dispatch_kernel(mixed_ref, residual_ref, gain_ref, targets_ref, stream_ref, outgoing_ref):
    rows, width = residual_ref.shape
    experts, capacity = outgoing_ref.shape[:2]

    def add(at, total):
        mixed = mixed_ref[0, :, at].astype(jnp.float32)
        for member in range(1, mixed_ref.shape[0]):
            mixed = mixed + mixed_ref[member, :, at].astype(jnp.float32)
        stream = (residual_ref[:, at].astype(jnp.float32) + mixed).astype(jnp.bfloat16)
        stream_ref[:, at] = stream
        wide = stream.astype(jnp.float32)
        return total + jnp.sum(wide * wide, axis=1, keepdims=True)

    total = over_columns(width, add, jnp.zeros((rows, 1), jnp.float32), True)
    scale = lax.rsqrt(total / width + epsilon)
    slot = lax.broadcasted_iota(jnp.int32, (experts * capacity, rows), 0)
    chosen = (slot == targets_ref[0:1, :]) | (slot == targets_ref[1:2, :])
    chosen = chosen.astype(jnp.float32).astype(jnp.bfloat16)

    def send(at, carried):
        normed = (stream_ref[:, at].astype(jnp.float32) * scale * gain_ref[:, at]).astype(jnp.bfloat16)
        sent = jnp.dot(chosen, normed, preferred_element_type=jnp.float32).astype(jnp.bfloat16)
        outgoing_ref[:, :, at] = sent.reshape(experts, capacity, COLUMNS)
        return carried

    over_columns(width, send, 0, True)


def pack_kernel(arrived_ref, first_ref, second_ref, rest_ref, back_ref, entries):
    slots = arrived_ref.shape[0] * arrived_ref.shape[1]
    width = arrived_ref.shape[2]

    def read(at, largest):
        part = arrived_ref[:, :, at].reshape(slots, COLUMNS)
        entries[:, at] = part
        size = jnp.abs(part.astype(jnp.float32))
        for lane in range(0, COLUMNS, 128):
            largest = jnp.maximum(largest, size[:, lane : lane + 128])
        return largest

    largest = over_columns(width, read, jnp.zeros((slots, 128), jnp.float32))
    held = (jnp.max(largest, axis=1, keepdims=True) > 0).astype(jnp.float32)
    row = lax.broadcasted_iota(jnp.int32, (slots, slots), 0)
    column = lax.broadcasted_iota(jnp.int32, (slots, slots), 1)

    def product(left, right):
        left, right = left.astype(jnp.float32), right.astype(jnp.float32)
        return jnp.dot(
            left.astype(jnp.bfloat16), right.astype(jnp.bfloat16), preferred_element_type=jnp.float32
        )

    held_rows = jnp.broadcast_to(held, (slots, slots))
    held_columns = product(jnp.ones((slots, slots), jnp.float32), jnp.where(row == column, held_rows, 0.0))
    place_rows = product(column < row, held_rows)
    place_columns = product(held_columns, row < column)
    back = ((place_rows == column.astype(jnp.float32)) & (held_rows > 0)).astype(jnp.float32)
    back_ref[...] = back.astype(jnp.bfloat16)
    forth = ((place_columns == row.astype(jnp.float32)) & (held_columns > 0)).astype(jnp.float32)
    forth = forth.astype(jnp.bfloat16)
    half, both = first_ref.shape[0], first_ref.shape[0] + second_ref.shape[0]

    def write(at, carried):
        packed = jnp.dot(forth, entries[:, at], preferred_element_type=jnp.float32).astype(jnp.bfloat16)
        first_ref[:, at] = packed[:half]
        second_ref[:, at] = packed[half:both]
        rest_ref[:, at] = packed[both:]
        return carried

    over_columns(width, write, 0, True)


def expert_kernel(*refs):
    count = (len(refs) - 6) // 2
    inputs, outs = refs[:count], refs[count + 3 : -3]
    gate_ref, up_ref, down_ref = refs[count : count + 3]
    entries, gate, up = refs[-3:]
    width = inputs[0].shape[1]
    ends = list(itertools.accumulate(source.shape[0] for source in inputs))
    for source, end in zip(inputs, ends):
        entries[end - source.shape[0] : end] = source[...]
    gate[...] = jnp.zeros_like(gate)
    up[...] = jnp.zeros_like(up)

    def rise(index, carried):
        at = pl.ds(pl.multiple_of(index * COLUMNS, COLUMNS), COLUMNS)
        part = entries[:, at]
        gate[...] += jnp.dot(part, gate_ref[at, :], preferred_element_type=jnp.float32)
        up[...] += jnp.dot(part, up_ref[at, :], preferred_element_type=jnp.float32)
        return carried

    lax.fori_loop(0, width // COLUMNS, rise, 0)
    hidden = (gate[...] / (1.0 + jnp.exp(-gate[...])) * up[...]).astype(jnp.bfloat16)

    def fall(index, carried):
        at = pl.ds(pl.multiple_of(index * COLUMNS, COLUMNS), COLUMNS)
        share = jnp.dot(hidden, down_ref[:, at], preferred_element_type=jnp.float32).astype(jnp.bfloat16)
        for out, end in zip(outs, ends):
            out[:, at] = share[end - out.shape[0] : end]
        return carried

    lax.fori_loop(0, width // COLUMNS, fall, 0)


def run_experts(pieces, weights):
    shapes = tuple(jax.ShapeDtypeStruct(piece.shape, jnp.bfloat16) for piece in pieces)
    slots = sum(piece.shape[0] for piece in pieces)
    width, units = weights[0].shape
    flops = 6 * slots * width * units
    scratch = [pltpu.VMEM((slots, width), jnp.bfloat16)] + [pltpu.VMEM((slots, units), jnp.float32)] * 2
    return in_kernel(expert_kernel, shapes, 32, flops, *pieces, *weights, scratch=scratch)


def final_kernel(returned_ref, targets_ref, logits_ref, stream_ref, gain_ref, out_ref, blended):
    rows, width = stream_ref.shape
    slots = returned_ref.shape[0] * returned_ref.shape[1]
    slot = lax.broadcasted_iota(jnp.int32, (rows, slots), 1).astype(jnp.float32)
    diagonal = lax.broadcasted_iota(jnp.int32, (rows, rows), 0) == lax.broadcasted_iota(jnp.int32, (rows, rows), 1)

    def column(row):
        return jnp.sum(jnp.where(diagonal, row.astype(jnp.float32), 0.0), axis=1, keepdims=True)

    picks = [
        (slot == column(targets_ref[pick : pick + 1])).astype(jnp.float32).astype(jnp.bfloat16)
        for pick in range(TOP)
    ]
    logits = column(logits_ref[...])
    shares = (1.0 / (1.0 + jnp.exp(-logits)), 1.0 / (1.0 + jnp.exp(logits)))

    def mix(at, total):
        entries = returned_ref[:, :, at].reshape(slots, COLUMNS)
        both = shares[0] * jnp.dot(picks[0], entries, preferred_element_type=jnp.float32)
        both = both + shares[1] * jnp.dot(picks[1], entries, preferred_element_type=jnp.float32)
        blended[:, at] = both
        return total + jnp.sum(both * both, axis=1, keepdims=True)

    total = over_columns(width, mix, jnp.zeros((rows, 1), jnp.float32), True)
    scale = lax.rsqrt(total / width + epsilon)

    def add(at, carried):
        wide = stream_ref[:, at].astype(jnp.float32)
        out_ref[:, at] = (wide + blended[:, at] * scale * gain_ref[:, at]).astype(jnp.bfloat16)
        return carried

    over_columns(width, add, 0, True)


def along_tp(shard, step):
    size = lax.axis_size("tp")
    return lax.ppermute(shard, "tp", [(member, (member + step) % size) for member in range(size)])


def relay_kernel(own_up, far_up, own_down, far_down, up_ref, down_ref):
    for own, far, out in ((own_up, far_up, up_ref), (own_down, far_down, down_ref)):

        def step(index, carried):
            at = pl.ds(pl.multiple_of(index * COLUMNS, COLUMNS), COLUMNS)
            out[:, at] = (own[:, at].astype(jnp.float32) + far[:, at].astype(jnp.float32)).astype(jnp.bfloat16)
            return carried

        lax.fori_loop(0, out.shape[1] // COLUMNS, step, 0)


def unpack_kernel(back_ref, rest_ref, *refs):
    firsts, seconds, results_ref = refs[:3], refs[3:6], refs[6]
    width = firsts[0].shape[1]

    def step(at, carried):
        sums = []
        for parts in (firsts, seconds):
            total = parts[0][:, at].astype(jnp.float32)
            for part in parts[1:]:
                total = total + part[:, at].astype(jnp.float32)
            sums.append(total.astype(jnp.bfloat16))
        packed = jnp.concatenate(sums + [rest_ref[:, at]], axis=0)
        spread = jnp.dot(back_ref[...], packed, preferred_element_type=jnp.float32).astype(jnp.bfloat16)
        results_ref[:, :, at] = spread.reshape(results_ref.shape[0], results_ref.shape[1], COLUMNS)
        return carried

    over_columns(width, step, 0, True)


def rest_outputs(rest, weights):
    members = lax.axis_size("tp")
    copies = jnp.broadcast_to(rest[None], (members, *rest.shape))
    rows = lax.all_to_all(copies, "tp", split_axis=0, concat_axis=0, tiled=True).reshape(-1, rest.shape[1])
    (share,) = run_experts((rows,), weights)
    parts = lax.all_to_all(split_up(share, 0, members), "tp", split_axis=0, concat_axis=0, tiled=True)
    return jnp.sum(parts.astype(jnp.float32), axis=0).astype(jnp.bfloat16)


def expert_outputs(arrived, most, weights):
    experts, capacity, width = arrived.shape
    slots = experts * capacity
    half, other = (jax.ShapeDtypeStruct((count, width), jnp.bfloat16) for count in PACKED)
    rest_shape = jax.ShapeDtypeStruct((slots - sum(PACKED), width), jnp.bfloat16)
    square = jax.ShapeDtypeStruct((slots, slots), jnp.bfloat16)
    first, second, rest, back = in_kernel(
        pack_kernel, (half, other, rest_shape, square), 16, 2 * slots * slots * width, arrived,
        scratch=[pltpu.VMEM((slots, width), jnp.bfloat16)],
    )
    below_first = along_tp(first, 1)
    above_second = along_tp(second, -1)
    below_second = along_tp(second, 1)
    above_first = along_tp(first, -1)
    far_first = along_tp(below_first, 1)
    far_second = along_tp(above_second, -1)
    own = run_experts((first, second), weights)
    near = run_experts((below_first, below_second, above_first, above_second), weights)
    direct_up = along_tp(near[3], 1)
    direct_down = along_tp(near[0], -1)
    far = run_experts((far_first, far_second), weights)
    relay_up = along_tp(far[0], 1)
    relay_down = along_tp(far[1], -1)
    both_up, both_down = in_kernel(
        relay_kernel, (half, other), 8, 2 * sum(PACKED) * width, near[2], relay_up, near[1], relay_down
    )
    both_up = along_tp(both_up, 1)
    both_down = along_tp(both_down, -1)
    rest_out = lax.cond(most > sum(PACKED), lambda: rest_outputs(rest, weights), lambda: jnp.zeros_like(rest))
    return in_kernel(
        unpack_kernel, jax.ShapeDtypeStruct(arrived.shape, jnp.bfloat16), 16,
        2 * slots * slots * width, back, rest_out, own[0], both_up, direct_down, own[1], direct_up, both_down,
    )


def on_device(
    queries,
    keys,
    values,
    break_bias,
    residual,
    w_out,
    ffn_gain,
    pick_ids,
    pair_logit,
    w_gate,
    w_up,
    w_down,
    out_gain,
):
    position = lax.axis_index("sp")
    quarters = lax.axis_size("tp")
    quarter = lax.axis_index("tp")
    slice_rows = queries.shape[0] // quarters
    width = w_out.shape[1]
    experts = lax.axis_size("sp")
    capacity = max(2, (3 * slice_rows + experts - 1) // experts)
    routed = lax.dynamic_slice_in_dim(pick_ids.T, quarter * slice_rows, slice_rows, 1)
    flat_ids = routed.reshape(slice_rows * TOP)
    places = jnp.arange(slice_rows * TOP, dtype=jnp.int32)
    matches = (flat_ids[:, None] == flat_ids[None, :]) & (places[None, :] < places[:, None])
    ranks = jnp.sum(matches.astype(jnp.int32), axis=1)
    targets = (flat_ids * capacity + ranks).reshape(TOP, slice_rows)
    logits = lax.dynamic_slice_in_dim(pair_logit, quarter * slice_rows, slice_rows, 0)[None]

    place = position.reshape(1).astype(jnp.int32)
    routing = (targets, logits)
    head_out, most, routing = attend(queries, keys, values, break_bias, pick_ids, place, routing)
    targets, logits = routing
    partial = jnp.dot(head_out, w_out, preferred_element_type=jnp.float32).astype(jnp.bfloat16)
    parts = split_up(partial, 0, quarters)
    mixed = lax.all_to_all(parts, "tp", split_axis=0, concat_axis=0, tiled=True)
    slots = jax.ShapeDtypeStruct((experts, capacity, width), jnp.bfloat16)
    rows = jax.ShapeDtypeStruct((slice_rows, width), jnp.bfloat16)
    dispatch_flops = 2 * experts * capacity * slice_rows * width
    stream, outgoing = in_kernel(
        dispatch_kernel, (rows, slots), 16, dispatch_flops,
        mixed, residual, ffn_gain[None], targets,
    )
    arrived = lax.all_to_all(outgoing, "sp", split_axis=0, concat_axis=0, tiled=True)
    results = expert_outputs(arrived, most[0], (w_gate[0], w_up[0], w_down[0]))
    returned = lax.all_to_all(results, "sp", split_axis=0, concat_axis=0, tiled=True)
    return in_kernel(
        final_kernel, rows, 16, 2 * dispatch_flops,
        returned, targets, logits, stream, out_gain[None],
        scratch=[pltpu.VMEM((slice_rows, width), jnp.float32)],
    )


def solution(mesh):
    placed = (
        P("sp", "tp"),
        P("sp", "tp"),
        P("sp", "tp"),
        P("tp"),
        P(("sp", "tp"), None),
        P("tp", None),
        P(),
        P("sp", None),
        P("sp"),
        P("sp", None, "tp"),
        P("sp", None, "tp"),
        P("sp", "tp", None),
        P(),
    )

    return jax.shard_map(on_device, mesh=mesh, in_specs=placed, out_specs=P(("sp", "tp"), None), check_vma=False)
```

```python
import functools
import itertools

import jax
import jax.numpy as jnp
from jax import lax
from jax.experimental import pallas as pl
from jax.experimental.pallas import tpu as pltpu
from jax.sharding import PartitionSpec as P


HEAD = 128
TOP = 2
Z_SIZE = 8
X_SIZE = 4
CORES = 2
Z_PLANE = X_SIZE * CORES

epsilon = 1e-06


def split_up(shard, dim, peers):
    before, after = (shard.shape[:dim], shard.shape[dim + 1 :])
    return jnp.moveaxis(shard.reshape(*before, peers, -1, *after), dim, 0)


LOG2E = 1.4426950408889634
KEY_BLOCK = 256
MOST = 100.0
PICK_ROWS = 8
TOGETHER = 2


def causal_visit(state, query_ref, kv_ref, bias_ref, later, block, first_query):
    outputs, used = state
    rows = query_ref.shape[0] // bias_ref.shape[0]
    heads = bias_ref.shape[0]
    factor = HEAD ** (-0.5) * LOG2E
    at_block = pl.ds(pl.multiple_of(block * KEY_BLOCK, KEY_BLOCK), KEY_BLOCK)
    keys = kv_ref[at_block, :HEAD]
    values = kv_ref[at_block, HEAD:]
    scores = lax.dot_general(
        query_ref[...], keys, (((1,), (1,)), ((), ())), preferred_element_type=jnp.float32
    )
    if first_query is not None:
        query_pos = first_query + lax.broadcasted_iota(jnp.int32, (rows, KEY_BLOCK), 0)
        key_pos = block * KEY_BLOCK + lax.broadcasted_iota(jnp.int32, (rows, KEY_BLOCK), 1)
        before = key_pos < query_pos
    breaks, leads = [], []
    for head in range(heads):
        z = scores[head * rows : (head + 1) * rows] * factor + bias_ref[head] * LOG2E
        softplus = jnp.maximum(jnp.log2(1.0 + jnp.exp2(jnp.minimum(z, MOST))), z)
        leads.append(z - softplus)
        breaks.append(softplus if first_query is None else jnp.where(before, softplus, 0.0))
    behind = jnp.dot(
        jnp.concatenate([b.astype(jnp.bfloat16) for b in breaks], axis=0),
        later,
        preferred_element_type=jnp.float32,
    )
    weights = []
    for head in range(heads):
        at = slice(head * rows, (head + 1) * rows)
        past = behind[at]
        gone = used[at]
        weight = jnp.exp2(leads[head] - past - jnp.concatenate([gone, gone], axis=1))
        if first_query is not None:
            weight = jnp.where(before, weight, 0.0)
        weights.append(weight.astype(jnp.bfloat16))
        used[at] = gone + jnp.broadcast_to(past[:, :1] + breaks[head][:, :1], gone.shape)
    outputs[...] += jnp.dot(
        jnp.concatenate(weights, axis=0), values, preferred_element_type=jnp.float32
    )


def later_keys():
    return (
        lax.broadcasted_iota(jnp.int32, (KEY_BLOCK, KEY_BLOCK), 0)
        > lax.broadcasted_iota(jnp.int32, (KEY_BLOCK, KEY_BLOCK), 1)
    ).astype(jnp.float32).astype(jnp.bfloat16)


def lay_out(own_ref, twin_ref, plane, place):
    lanes = (place // CORES) % X_SIZE
    core = place % CORES
    length = own_ref.shape[1] - PICK_ROWS
    for shift in range(X_SIZE):
        source = ((lanes + X_SIZE - shift) % X_SIZE) * CORES
        plane[pl.ds(pl.multiple_of((source + core) * length, length), length)] = own_ref[shift, :length]
        plane[pl.ds(pl.multiple_of((source + 1 - core) * length, length), length)] = twin_ref[shift, :length]


def tally(counts, *pieces):
    expert = lax.broadcasted_iota(jnp.int32, counts.shape, 0).astype(jnp.float32)
    found = counts[...]
    for piece in pieces:
        length = piece.shape[1] - PICK_ROWS
        for shift in range(X_SIZE):
            picks = piece[shift, length:].astype(jnp.float32)[0:1]
            found = found + (picks == expert).astype(jnp.float32)
    counts[...] = found


def own_plane_kernel(place_ref, bias_ref, query_ref, own_ref, twin_ref, near, near_used, far, counts, plane):
    place = place_ref[0]
    lay_out(own_ref, twin_ref, plane, place)
    for ref in (near, near_used, far, counts):
        ref[...] = jnp.zeros_like(ref)
    tally(counts, own_ref, twin_ref)
    later = later_keys()
    rows = query_ref.shape[0] // bias_ref.shape[0]
    first_query = (place % (X_SIZE * CORES)) * rows
    last = (first_query + rows - 1) // KEY_BLOCK

    def step(index, carried):
        causal_visit((near, near_used), query_ref, plane, bias_ref, later, last - index, first_query)
        return carried

    lax.fori_loop(0, last + 1, step, 0)


def whole_plane(state, query_ref, plane, bias_ref):
    later = later_keys()
    blocks = plane.shape[0] // KEY_BLOCK

    def step(index, carried):
        for offset in range(TOGETHER):
            block = blocks - 1 - offset - TOGETHER * index
            causal_visit(state, query_ref, plane, bias_ref, later, block, None)
        return carried

    lax.fori_loop(0, blocks // TOGETHER, step, 0)


def two_planes_kernel(distance, place_ref, bias_ref, query_ref, below, below_twin, above, above_twin,
                      near_in, near_used_in, far_in, counts_in, near, near_used, far, counts,
                      planes, found, found_used):
    place = place_ref[0]
    tally(counts, below, below_twin, above, above_twin)
    level = place // (X_SIZE * CORES)
    lay_out(below, below_twin, planes.at[0], place)
    lay_out(above, above_twin, planes.at[1], place)

    def visit(side, carried):
        found[...] = jnp.zeros_like(found)
        found_used[...] = jnp.zeros_like(found_used)
        whole_plane((found, found_used), query_ref, planes.at[side], bias_ref)

        @pl.when(side == 0)
        def _():
            near[...] += jnp.exp2(-near_used[...]) * found[...]
            near_used[...] += found_used[...]

        @pl.when(side == 1)
        def _():
            far[...] = found[...] + jnp.exp2(-found_used[...]) * far[...]

        return carried

    first = jnp.where(level >= distance, 0, 1)
    past = jnp.where(level + distance >= Z_SIZE, 2, 1)
    lax.fori_loop(first, past, visit, 0)


def last_plane_kernel(distance, place_ref, bias_ref, query_ref, below, below_twin,
                      near_in, near_used_in, far_in, counts_in, out_ref, most_ref, plane, near, near_used, counts):
    place = place_ref[0]
    counts[...] = counts_in[...]
    tally(counts, below, below_twin)
    rows = out_ref.shape[0]
    lane = lax.broadcasted_iota(jnp.int32, counts.shape, 1) % rows // (rows // 4)
    most = jnp.zeros((counts.shape[0], 1), jnp.float32)
    for member in range(4):
        named = jnp.sum(jnp.where(lane == member, counts[...], 0.0), axis=1, keepdims=True)
        most = jnp.maximum(most, named)
    most_ref[0] = jnp.max(most).astype(jnp.int32)
    near[...] = near_in[...]
    near_used[...] = near_used_in[...]

    @pl.when(place // (X_SIZE * CORES) >= distance)
    def _():
        lay_out(below, below_twin, plane, place)
        whole_plane((near, near_used), query_ref, plane, bias_ref)

    rows = out_ref.shape[0]
    for head in range(bias_ref.shape[0]):
        at = slice(head * rows, (head + 1) * rows)
        output = near[at] + jnp.exp2(-near_used[at]) * far_in[at]
        scaled = output * lax.rsqrt(jnp.mean(output * output, axis=-1, keepdims=True) + epsilon)
        out_ref[:, head * HEAD : (head + 1) * HEAD] = scaled.astype(jnp.bfloat16)


def attention_call(kernel, name, planes, position, break_bias, stacked, key_values, state, rows):
    stack = stacked.shape[0]
    in_vmem = pl.BlockSpec(memory_space=pltpu.VMEM)
    in_smem = pl.BlockSpec(memory_space=pltpu.SMEM)
    plane = (Z_PLANE * rows, 2 * HEAD)
    running = pltpu.VMEM((stack, HEAD), jnp.float32)
    kept = jax.ShapeDtypeStruct((stack, HEAD), jnp.float32)
    counts = (Z_SIZE * Z_PLANE, rows * TOP)
    last = name == "attend_last"
    keys = planes * Z_PLANE * rows
    first_state = 3 + len(key_values)
    heads = jax.ShapeDtypeStruct((rows, stack // rows * HEAD), jnp.bfloat16)
    return pl.pallas_call(
        kernel,
        out_shape=(heads, jax.ShapeDtypeStruct((1,), jnp.int32))
        if last
        else (kept,) * 3 + (jax.ShapeDtypeStruct(counts, jnp.float32),),
        in_specs=[in_smem, in_smem] + [in_vmem] * (1 + len(key_values) + len(state)),
        out_specs=(in_vmem, in_smem) if last else (in_vmem,) * 4,
        scratch_shapes=[pltpu.VMEM(plane if planes == 1 else (planes, *plane), jnp.bfloat16)]
        + ([running, running] if state else [])
        + ([pltpu.VMEM(counts, jnp.float32)] if last else []),
        input_output_aliases={} if last or not state else {first_state + i: i for i in range(4)},
        cost_estimate=pl.CostEstimate(
            flops=2 * stack * keys * (2 * HEAD + KEY_BLOCK), transcendentals=3 * stack * keys, bytes_accessed=0
        ),
        compiler_params=pltpu.CompilerParams(vmem_limit_bytes=8 * 1024 * 1024),
    )(position, break_bias, stacked, *key_values, *state)


def moved(shard, step_z, step_x, swap):
    pairs = []
    for place in range(Z_SIZE * Z_PLANE):
        z, x, core = place // Z_PLANE, place // CORES % X_SIZE, place % CORES
        target = ((z + step_z) % Z_SIZE * X_SIZE + (x + step_x) % X_SIZE) * CORES + (core ^ swap)
        pairs.append((place, target))
    return lax.ppermute(shard, "sp", pairs)


def attend(queries, keys, values, break_bias, pick_ids, position, routing):
    rows = queries.shape[0]
    heads = queries.shape[1] // HEAD
    stacked = jnp.concatenate([queries[:, h * HEAD : (h + 1) * HEAD] for h in range(heads)], axis=0)
    picks = pick_ids.T.astype(jnp.bfloat16).reshape(1, TOP * rows)
    picks = jnp.concatenate([picks, jnp.zeros((PICK_ROWS - 1, rows * TOP), jnp.bfloat16)], axis=0)
    block = jnp.concatenate([jnp.concatenate([keys, values], axis=1), picks], axis=0)
    own = jnp.stack([block] + [moved(block, 0, step, 0) for step in range(1, X_SIZE)])
    own, stacked, routing = lax.optimization_barrier((own, stacked, routing))
    twin = moved(own, 0, 0, 1)
    common = (position, break_bias, stacked)
    below, above = own, own
    arrived = []
    for distance in range(1, Z_SIZE // 2 + 1):
        below = moved(below, 1, 0, 0)
        pieces = [below, moved(below, 0, 0, 1)]
        if distance < Z_SIZE // 2:
            above = moved(above, -1, 0, 0)
            pieces += [above, moved(above, 0, 0, 1)]
        arrived.append(pieces)
    state = attention_call(own_plane_kernel, "attend_0", 1, *common, (own, twin), (), rows)
    for distance in range(1, Z_SIZE // 2):
        kernel = functools.partial(two_planes_kernel, distance)
        name = f"attend_{distance}"
        state = attention_call(kernel, name, 2, *common, arrived[distance - 1], state, rows)
    kernel = functools.partial(last_plane_kernel, Z_SIZE // 2)
    return *attention_call(kernel, "attend_last", 1, *common, arrived[-1], state, rows), routing


COLUMNS = 1024
PACKED = (48, 40)


def in_kernel(kernel, out_shapes, megabytes, flops, *operands, scratch=()):
    spec = pl.BlockSpec(memory_space=pltpu.VMEM)
    several = isinstance(out_shapes, tuple)
    return pl.pallas_call(
        kernel,
        out_shape=out_shapes,
        in_specs=[spec] * len(operands),
        out_specs=(spec,) * len(out_shapes) if several else spec,
        scratch_shapes=list(scratch),
        cost_estimate=pl.CostEstimate(flops=flops, transcendentals=0, bytes_accessed=0),
        compiler_params=pltpu.CompilerParams(vmem_limit_bytes=megabytes * 1024 * 1024),
    )(*operands)


def over_columns(width, step, carried, unrolled=False):
    if unrolled:
        for start in range(0, width, COLUMNS):
            carried = step(slice(start, start + COLUMNS), carried)
        return carried

    def at_column(index, carried):
        return step(pl.ds(pl.multiple_of(index * COLUMNS, COLUMNS), COLUMNS), carried)

    return lax.fori_loop(0, width // COLUMNS, at_column, carried)


def dispatch_kernel(mixed_ref, residual_ref, gain_ref, targets_ref, stream_ref, outgoing_ref):
    rows, width = residual_ref.shape
    experts, capacity = outgoing_ref.shape[:2]

    def add(at, total):
        mixed = mixed_ref[0, :, at].astype(jnp.float32)
        for member in range(1, mixed_ref.shape[0]):
            mixed = mixed + mixed_ref[member, :, at].astype(jnp.float32)
        stream = (residual_ref[:, at].astype(jnp.float32) + mixed).astype(jnp.bfloat16)
        stream_ref[:, at] = stream
        wide = stream.astype(jnp.float32)
        return total + jnp.sum(wide * wide, axis=1, keepdims=True)

    total = over_columns(width, add, jnp.zeros((rows, 1), jnp.float32), True)
    scale = lax.rsqrt(total / width + epsilon)
    slot = lax.broadcasted_iota(jnp.int32, (experts * capacity, rows), 0)
    chosen = (slot == targets_ref[0:1, :]) | (slot == targets_ref[1:2, :])
    chosen = chosen.astype(jnp.float32).astype(jnp.bfloat16)

    def send(at, carried):
        normed = (stream_ref[:, at].astype(jnp.float32) * scale * gain_ref[:, at]).astype(jnp.bfloat16)
        sent = jnp.dot(chosen, normed, preferred_element_type=jnp.float32).astype(jnp.bfloat16)
        outgoing_ref[:, :, at] = sent.reshape(experts, capacity, COLUMNS)
        return carried

    over_columns(width, send, 0, True)


def pack_kernel(arrived_ref, first_ref, second_ref, rest_ref, back_ref, entries):
    slots = arrived_ref.shape[0] * arrived_ref.shape[1]
    width = arrived_ref.shape[2]

    def read(at, largest):
        part = arrived_ref[:, :, at].reshape(slots, COLUMNS)
        entries[:, at] = part
        size = jnp.abs(part.astype(jnp.float32))
        for lane in range(0, COLUMNS, 128):
            largest = jnp.maximum(largest, size[:, lane : lane + 128])
        return largest

    largest = over_columns(width, read, jnp.zeros((slots, 128), jnp.float32))
    held = (jnp.max(largest, axis=1, keepdims=True) > 0).astype(jnp.float32)
    row = lax.broadcasted_iota(jnp.int32, (slots, slots), 0)
    column = lax.broadcasted_iota(jnp.int32, (slots, slots), 1)

    def product(left, right):
        left, right = left.astype(jnp.float32), right.astype(jnp.float32)
        return jnp.dot(
            left.astype(jnp.bfloat16), right.astype(jnp.bfloat16), preferred_element_type=jnp.float32
        )

    held_rows = jnp.broadcast_to(held, (slots, slots))
    held_columns = product(jnp.ones((slots, slots), jnp.float32), jnp.where(row == column, held_rows, 0.0))
    place_rows = product(column < row, held_rows)
    place_columns = product(held_columns, row < column)
    back = ((place_rows == column.astype(jnp.float32)) & (held_rows > 0)).astype(jnp.float32)
    back_ref[...] = back.astype(jnp.bfloat16)
    forth = ((place_columns == row.astype(jnp.float32)) & (held_columns > 0)).astype(jnp.float32)
    forth = forth.astype(jnp.bfloat16)
    half, both = first_ref.shape[0], first_ref.shape[0] + second_ref.shape[0]

    def write(at, carried):
        packed = jnp.dot(forth, entries[:, at], preferred_element_type=jnp.float32).astype(jnp.bfloat16)
        first_ref[:, at] = packed[:half]
        second_ref[:, at] = packed[half:both]
        rest_ref[:, at] = packed[both:]
        return carried

    over_columns(width, write, 0, True)


def expert_kernel(*refs):
    count = (len(refs) - 6) // 2
    inputs, outs = refs[:count], refs[count + 3 : -3]
    gate_ref, up_ref, down_ref = refs[count : count + 3]
    entries, gate, up = refs[-3:]
    width = inputs[0].shape[1]
    ends = list(itertools.accumulate(source.shape[0] for source in inputs))
    for source, end in zip(inputs, ends):
        entries[end - source.shape[0] : end] = source[...]
    gate[...] = jnp.zeros_like(gate)
    up[...] = jnp.zeros_like(up)

    def rise(index, carried):
        at = pl.ds(pl.multiple_of(index * COLUMNS, COLUMNS), COLUMNS)
        part = entries[:, at]
        gate[...] += jnp.dot(part, gate_ref[at, :], preferred_element_type=jnp.float32)
        up[...] += jnp.dot(part, up_ref[at, :], preferred_element_type=jnp.float32)
        return carried

    lax.fori_loop(0, width // COLUMNS, rise, 0)
    hidden = (gate[...] / (1.0 + jnp.exp(-gate[...])) * up[...]).astype(jnp.bfloat16)

    def fall(index, carried):
        at = pl.ds(pl.multiple_of(index * COLUMNS, COLUMNS), COLUMNS)
        share = jnp.dot(hidden, down_ref[:, at], preferred_element_type=jnp.float32).astype(jnp.bfloat16)
        for out, end in zip(outs, ends):
            out[:, at] = share[end - out.shape[0] : end]
        return carried

    lax.fori_loop(0, width // COLUMNS, fall, 0)


def run_experts(pieces, weights):
    shapes = tuple(jax.ShapeDtypeStruct(piece.shape, jnp.bfloat16) for piece in pieces)
    slots = sum(piece.shape[0] for piece in pieces)
    width, units = weights[0].shape
    flops = 6 * slots * width * units
    scratch = [pltpu.VMEM((slots, width), jnp.bfloat16)] + [pltpu.VMEM((slots, units), jnp.float32)] * 2
    return in_kernel(expert_kernel, shapes, 32, flops, *pieces, *weights, scratch=scratch)


def final_kernel(returned_ref, targets_ref, logits_ref, stream_ref, gain_ref, out_ref, blended):
    rows, width = stream_ref.shape
    slots = returned_ref.shape[0] * returned_ref.shape[1]
    slot = lax.broadcasted_iota(jnp.int32, (rows, slots), 1).astype(jnp.float32)
    diagonal = lax.broadcasted_iota(jnp.int32, (rows, rows), 0) == lax.broadcasted_iota(jnp.int32, (rows, rows), 1)

    def column(row):
        return jnp.sum(jnp.where(diagonal, row.astype(jnp.float32), 0.0), axis=1, keepdims=True)

    picks = [
        (slot == column(targets_ref[pick : pick + 1])).astype(jnp.float32).astype(jnp.bfloat16)
        for pick in range(TOP)
    ]
    logits = column(logits_ref[...])
    shares = (1.0 / (1.0 + jnp.exp(-logits)), 1.0 / (1.0 + jnp.exp(logits)))

    def mix(at, total):
        entries = returned_ref[:, :, at].reshape(slots, COLUMNS)
        both = shares[0] * jnp.dot(picks[0], entries, preferred_element_type=jnp.float32)
        both = both + shares[1] * jnp.dot(picks[1], entries, preferred_element_type=jnp.float32)
        blended[:, at] = both
        return total + jnp.sum(both * both, axis=1, keepdims=True)

    total = over_columns(width, mix, jnp.zeros((rows, 1), jnp.float32), True)
    scale = lax.rsqrt(total / width + epsilon)

    def add(at, carried):
        wide = stream_ref[:, at].astype(jnp.float32)
        out_ref[:, at] = (wide + blended[:, at] * scale * gain_ref[:, at]).astype(jnp.bfloat16)
        return carried

    over_columns(width, add, 0, True)


def along_tp(shard, step):
    size = lax.axis_size("tp")
    return lax.ppermute(shard, "tp", [(member, (member + step) % size) for member in range(size)])


def relay_kernel(own_up, far_up, own_down, far_down, up_ref, down_ref):
    for own, far, out in ((own_up, far_up, up_ref), (own_down, far_down, down_ref)):

        def step(index, carried):
            at = pl.ds(pl.multiple_of(index * COLUMNS, COLUMNS), COLUMNS)
            out[:, at] = (own[:, at].astype(jnp.float32) + far[:, at].astype(jnp.float32)).astype(jnp.bfloat16)
            return carried

        lax.fori_loop(0, out.shape[1] // COLUMNS, step, 0)


def unpack_kernel(back_ref, rest_ref, *refs):
    firsts, seconds, results_ref = refs[:3], refs[3:6], refs[6]
    width = firsts[0].shape[1]

    def step(at, carried):
        sums = []
        for parts in (firsts, seconds):
            total = parts[0][:, at].astype(jnp.float32)
            for part in parts[1:]:
                total = total + part[:, at].astype(jnp.float32)
            sums.append(total.astype(jnp.bfloat16))
        packed = jnp.concatenate(sums + [rest_ref[:, at]], axis=0)
        spread = jnp.dot(back_ref[...], packed, preferred_element_type=jnp.float32).astype(jnp.bfloat16)
        results_ref[:, :, at] = spread.reshape(results_ref.shape[0], results_ref.shape[1], COLUMNS)
        return carried

    over_columns(width, step, 0, True)


def rest_outputs(rest, weights):
    members = lax.axis_size("tp")
    copies = jnp.broadcast_to(rest[None], (members, *rest.shape))
    rows = lax.all_to_all(copies, "tp", split_axis=0, concat_axis=0, tiled=True).reshape(-1, rest.shape[1])
    (share,) = run_experts((rows,), weights)
    parts = lax.all_to_all(split_up(share, 0, members), "tp", split_axis=0, concat_axis=0, tiled=True)
    return jnp.sum(parts.astype(jnp.float32), axis=0).astype(jnp.bfloat16)


def expert_outputs(arrived, most, weights):
    experts, capacity, width = arrived.shape
    slots = experts * capacity
    half, other = (jax.ShapeDtypeStruct((count, width), jnp.bfloat16) for count in PACKED)
    rest_shape = jax.ShapeDtypeStruct((slots - sum(PACKED), width), jnp.bfloat16)
    square = jax.ShapeDtypeStruct((slots, slots), jnp.bfloat16)
    first, second, rest, back = in_kernel(
        pack_kernel, (half, other, rest_shape, square), 16, 2 * slots * slots * width, arrived,
        scratch=[pltpu.VMEM((slots, width), jnp.bfloat16)],
    )
    below_first = along_tp(first, 1)
    above_second = along_tp(second, -1)
    below_second = along_tp(second, 1)
    above_first = along_tp(first, -1)
    far_first = along_tp(below_first, 1)
    far_second = along_tp(above_second, -1)
    own = run_experts((first, second), weights)
    near = run_experts((below_first, below_second, above_first, above_second), weights)
    direct_up = along_tp(near[3], 1)
    direct_down = along_tp(near[0], -1)
    far = run_experts((far_first, far_second), weights)
    relay_up = along_tp(far[0], 1)
    relay_down = along_tp(far[1], -1)
    both_up, both_down = in_kernel(
        relay_kernel, (half, other), 8, 2 * sum(PACKED) * width, near[2], relay_up, near[1], relay_down
    )
    both_up = along_tp(both_up, 1)
    both_down = along_tp(both_down, -1)
    rest_out = lax.cond(most > sum(PACKED), lambda: rest_outputs(rest, weights), lambda: jnp.zeros_like(rest))
    return in_kernel(
        unpack_kernel, jax.ShapeDtypeStruct(arrived.shape, jnp.bfloat16), 16,
        2 * slots * slots * width, back, rest_out, own[0], both_up, direct_down, own[1], direct_up, both_down,
    )


def on_device(
    queries,
    keys,
    values,
    break_bias,
    residual,
    w_out,
    ffn_gain,
    pick_ids,
    pair_logit,
    w_gate,
    w_up,
    w_down,
    out_gain,
):
    position = lax.axis_index("sp")
    quarters = lax.axis_size("tp")
    quarter = lax.axis_index("tp")
    slice_rows = queries.shape[0] // quarters
    width = w_out.shape[1]
    experts = lax.axis_size("sp")
    capacity = max(2, (3 * slice_rows + experts - 1) // experts)
    routed = lax.dynamic_slice_in_dim(pick_ids.T, quarter * slice_rows, slice_rows, 1)
    flat_ids = routed.reshape(slice_rows * TOP)
    places = jnp.arange(slice_rows * TOP, dtype=jnp.int32)
    matches = (flat_ids[:, None] == flat_ids[None, :]) & (places[None, :] < places[:, None])
    ranks = jnp.sum(matches.astype(jnp.int32), axis=1)
    targets = (flat_ids * capacity + ranks).reshape(TOP, slice_rows)
    logits = lax.dynamic_slice_in_dim(pair_logit, quarter * slice_rows, slice_rows, 0)[None]

    place = position.reshape(1).astype(jnp.int32)
    routing = (targets, logits)
    head_out, most, routing = attend(queries, keys, values, break_bias, pick_ids, place, routing)
    targets, logits = routing
    partial = jnp.dot(head_out, w_out, preferred_element_type=jnp.float32).astype(jnp.bfloat16)
    parts = split_up(partial, 0, quarters)
    mixed = lax.all_to_all(parts, "tp", split_axis=0, concat_axis=0, tiled=True)
    slots = jax.ShapeDtypeStruct((experts, capacity, width), jnp.bfloat16)
    rows = jax.ShapeDtypeStruct((slice_rows, width), jnp.bfloat16)
    dispatch_flops = 2 * experts * capacity * slice_rows * width
    stream, outgoing = in_kernel(
        dispatch_kernel, (rows, slots), 16, dispatch_flops,
        mixed, residual, ffn_gain[None], targets,
    )
    arrived = lax.all_to_all(outgoing, "sp", split_axis=0, concat_axis=0, tiled=True)
    results = expert_outputs(arrived, most[0], (w_gate[0], w_up[0], w_down[0]))
    returned = lax.all_to_all(results, "sp", split_axis=0, concat_axis=0, tiled=True)
    return in_kernel(
        final_kernel, rows, 16, 2 * dispatch_flops,
        returned, targets, logits, stream, out_gain[None],
        scratch=[pltpu.VMEM((slice_rows, width), jnp.float32)],
    )


def solution(mesh):
    placed = (
        P("sp", "tp"),
        P("sp", "tp"),
        P("sp", "tp"),
        P("tp"),
        P(("sp", "tp"), None),
        P("tp", None),
        P(),
        P("sp", None),
        P("sp"),
        P("sp", None, "tp"),
        P("sp", None, "tp"),
        P("sp", "tp", None),
        P(),
    )

    return jax.shard_map(on_device, mesh=mesh, in_specs=placed, out_specs=P(("sp", "tp"), None), check_vma=False)
```
